32 devices in a mesh: ep: 8 (over z, x), tp: 4 (over y, core).
Axes of the slice: x: 2, y: 2, z: 4, core: 2. Of those that a mesh axis runs over, the one named last changes fastest.
Arguments:
- queries: bfloat16 [4096, 1024], P('ep', 'tp'), may hold values from -6 to 6
- forget_forward_logits: bfloat16 [4096, 1024], P('ep', 'tp'), may hold values from -6 to 12
- forget_backward_logits: bfloat16 [4096, 1024], P('ep', 'tp'), may hold values from -6 to 12
- values: bfloat16 [4096, 1024], P('ep', 'tp'), may hold values from -6 to 6
- output_gate_logits: bfloat16 [4096, 1024], P('ep', 'tp'), may hold values from -6 to 6
- lower_bound_forward: float32 [1024], P('tp')
- lower_bound_backward: float32 [1024], P('tp')
- extra_log_decay: float32 [4096, 8], P('ep', 'tp'), may hold values from -2 to 0
- head_norm_scale: float32 [1024], P('tp'), may hold values from 0.1 to 1.9
- output_projection: bfloat16 [1024, 2048], P('tp'), may hold values from -0.1875 to 0.1875
- second_residual: bfloat16 [4096, 2048], P('ep'), may hold values from -6 to 6
- expert_norm_scale: float32 [2048], replicated, may hold values from 0.1 to 1.9
- routes: int32 [4096, 2], P('ep'), may hold values from 0 to 7, all different within a row; in each aligned block of 128 rows (0 to 127, 128 to 255, ...) at most 64 rows name the same one
- specialist_mixing_factor: float32 [4096, 2], P(('ep', 'tp')), may hold values from 0.1 to 1
- expert_gate_matrix: bfloat16 [8, 2048, 1024], P('ep', None, 'tp'), may hold values from -0.125 to 0.125
- expert_up_matrix: bfloat16 [8, 2048, 1024], P('ep', None, 'tp'), may hold values from -0.125 to 0.125
- expert_down_matrix: bfloat16 [8, 1024, 2048], P('ep', 'tp'), may hold values from -0.1875 to 0.1875
Outputs:
- mixer_output: bfloat16 [4096, 2048], P(('ep', 'tp'))
- routed_output: bfloat16 [4096, 2048], P(('ep', 'tp'))
The draws below stay inside these ranges and needn't reach their ends.
Inputs may be any that keep to these rules, and one draw needn't show every extreme that they name: `routes`: in each aligned block of 128 rows no expert is named by more than 64 rows; the 2 experts of a row differ.
All inputs are finite; a program needn't handle non-finite values.
Results may differ from the reference program's by a relative error of at most 0.014.
Values may be sent and summed in bfloat16 or wider, within the bound.
A program may use at most 128 MiB of HBM per device.

```python
import math
import jax
import jax.numpy as jnp
import numpy as np
from jax import lax

D = 2048
RECURRENT_HEADS = 8
DK = 128
DV = 128
FF = 1024
TOPK = 2
SPAN = 64
ROWS = 128
KEY_WIDTH = 1024
VAL_WIDTH = 1024
GROUP_WIDTH = 256
EXPERT_PART = 256
EXPERTS = 8
CAPQ = 64
TOKENS_A = 4096
TOKENS_B = 4096
N_EP = 8
N_TP = 4


def floor_common(key, salt):
    key = jax.random.fold_in(key, salt)
    key_order, key_slow, key_fast = jax.random.split(key, 3)
    ordering = jax.random.permutation(key_order, RECURRENT_HEADS)
    slow_heads = ordering < RECURRENT_HEADS // 2
    slow_rate = jax.random.uniform(key_slow, (RECURRENT_HEADS, DK), jnp.float32, 0.3, 2.0) / TOKENS_A
    fast_rate = jnp.exp(jax.random.uniform(key_fast, (RECURRENT_HEADS, DK), jnp.float32, math.log(0.025), math.log(0.1)))
    decay_rate = jnp.where(slow_heads[:, None], slow_rate, fast_rate)
    return (jnp.log1p(-decay_rate) - jnp.log(decay_rate)).reshape(RECURRENT_HEADS * DK).astype(jnp.float32)


def draw_lower_bound_forward(key, part):
    return floor_common(key, 11)


def draw_lower_bound_backward(key, part):
    return floor_common(key, 12)


def forget_common(key, salt):
    key = jax.random.fold_in(key, salt)
    key_base, key_run = jax.random.split(key, 2)
    base = jnp.clip(1.5 * jax.random.normal(key_base, (TOKENS_A, RECURRENT_HEADS, DK), jnp.float32), -6.0, 6.0)
    run_length = 4 * SPAN
    run_count = (TOKENS_A + run_length - 1) // run_length
    lifted = 6.0 * jax.random.randint(key_run, (run_count, RECURRENT_HEADS), 0, 2).astype(jnp.float32)
    position_block = jnp.arange(TOKENS_A, dtype=jnp.int32) // run_length
    offsets = lifted[position_block]
    return (base + offsets[:, :, None]).reshape(TOKENS_A, RECURRENT_HEADS * DK).astype(jnp.float32)


def draw_forget_forward_logits(key, part):
    return forget_common(key, 21).astype(jnp.bfloat16)


def draw_forget_backward_logits(key, part):
    return forget_common(key, 22).astype(jnp.bfloat16)


def draw_extra_log_decay(key, part):
    key_rate, key_place, key_depth = jax.random.split(key, 3)
    span_rows = TOKENS_A // EXPERTS
    factor = jnp.exp(jax.random.uniform(key_rate, (EXPERTS, RECURRENT_HEADS), jnp.float32, 0.0, math.log(3.0)))
    token_position = jnp.arange(TOKENS_A, dtype=jnp.int32)
    owner_block = token_position // span_rows
    stable_state = -0.2 / TOKENS_A * factor[owner_block]
    slot_positions = jax.random.randint(key_place, (2, RECURRENT_HEADS), 0, TOKENS_A)
    cumulative_decay = jnp.log(jax.random.uniform(key_depth, (2, RECURRENT_HEADS), jnp.float32, 0.55, 0.8))
    extra_decay_hits = token_position[:, None, None] == slot_positions[None, :, :]
    return (stable_state + jnp.sum(jnp.where(extra_decay_hits, cumulative_decay[None], 0.0), axis=1)).astype(jnp.float32)


def shard_levels(key, shape, cuts, low, high):
    level, own = 1.0, jax.random.fold_in(key, 6)
    for position, shards_of in cuts:
        draws = jnp.exp(jax.random.uniform(jax.random.fold_in(own, position), (shards_of,), jnp.float32, low / len(cuts), high / len(cuts)))
        level = level * jnp.repeat(draws, shape[position] // shards_of).reshape([-1 if axis == position else 1 for axis in range(len(shape))])
    return level


def deal_out(own_key, own, number, rows, count, top, most, lean):
    ranking = jax.random.permutation(own_key, count)
    crowded, common = load_shares(count, rows * top, most, lean, True), load_shares(count, rows * top, most, lean, False)
    places = jnp.arange(count)

    def named(sizes, offset_by):
        used = int((sizes > 0).sum())
        fixed = max(1, used // 4)
        passed = fixed + (places - fixed + offset_by * (used - fixed)) % max(1, count - fixed)
        return jnp.zeros((count,), jnp.int32).at[ranking[jnp.where(places < fixed, places, passed)]].set(jnp.asarray(sizes, jnp.int32))

    sizes = jnp.where(number % 4 == 0, named(crowded, number // 4), named(common, number - number // 4 - 1))
    mixed = jax.random.permutation(jax.random.fold_in(own, 3), count)
    source_of, receiver = mixed[0:count // 2 * 2:2], mixed[1:count // 2 * 2:2]
    slack = jnp.minimum(sizes[source_of] - 1, most - sizes[receiver]) // 2
    slack = jnp.where((source_of == ranking[0]) | (receiver == ranking[0]) | (sizes[receiver] == 0), 0, jnp.maximum(slack, 0))
    passed = jax.random.randint(jax.random.fold_in(own, 4), (count // 2,), 0, 1 << 20) % (slack + 1)
    sizes = sizes.at[source_of].add(-passed).at[receiver].add(passed)
    members = jnp.searchsorted(jnp.cumsum(sizes), jnp.arange(rows * top), side="right").astype(jnp.int32)
    table = members.reshape(top, rows).T
    table = table[jax.random.permutation(jax.random.fold_in(own, 1), rows)]
    offset_by = jax.random.randint(jax.random.fold_in(own, 2), (rows, 1), 0, top)
    return jnp.take_along_axis(table, (jnp.arange(top)[None, :] + offset_by) % top, axis=1)


def load_shares(count, total, bound, skew, full):
    weights = [(1 << 20) // math.isqrt(standing ** skew) + 1 for standing in range(1, count + 1)]
    largest = bound if full else min(bound, max(-(-total // count), total * weights[0] // sum(weights)))
    least = 1 if total - largest >= count - 1 else 0
    given, rest = [largest] + [least] * (count - 1), total - largest - least * (count - 1)
    while rest > 0:
        movable = [i for i in range(1, count) if given[i] < largest] or [i for i in range(1, count) if given[i] < bound]
        mass, remaining = sum([weights[i] for i in movable]), rest
        for i in movable:
            extra = min(bound - given[i], max(1, remaining * weights[i] // mass), rest)
            given[i] = given[i] + extra
            rest = rest - extra
    return np.array(given)


def noise(stream_key, shape, deviation, bound, shards=(), held_as=jnp.bfloat16):
    loudness = shard_levels(stream_key, shape, shards, -0.22, 0.18) if shards else 1.0
    entries = jax.random.normal(stream_key, shape, jnp.float32) * deviation * loudness
    return jnp.minimum(jnp.maximum(entries, -bound), bound).astype(held_as)


def setup_inputs(seed: int = 0) -> dict:
    arg_keys = jax.random.split(jax.random.key(seed), 18)
    queries = noise(arg_keys[0], (TOKENS_A, KEY_WIDTH), 1.0, 6.0, ((0, 8), (1, 4)))
    forget_forward_logits = draw_forget_forward_logits(jax.random.fold_in(arg_keys[17], 71), 0)
    forget_backward_logits = draw_forget_backward_logits(jax.random.fold_in(arg_keys[17], 71), 0)
    values = noise(arg_keys[3], (TOKENS_A, VAL_WIDTH), 1.0, 6.0, ((0, 8), (1, 4)))
    output_gate_logits = noise(arg_keys[4], (TOKENS_A, VAL_WIDTH), 1.0, 6.0, ((0, 8), (1, 4)))
    lower_bound_forward = draw_lower_bound_forward(jax.random.fold_in(arg_keys[17], 71), 0)
    lower_bound_backward = draw_lower_bound_backward(jax.random.fold_in(arg_keys[17], 71), 0)
    extra_log_decay = draw_extra_log_decay(jax.random.fold_in(arg_keys[17], 71), 0)
    head_norm_scale = jnp.clip(1.0 + 0.18 * jax.random.normal(arg_keys[8], (VAL_WIDTH,), jnp.float32), 0.1, 1.9)
    output_projection = noise(arg_keys[9], (VAL_WIDTH, D), VAL_WIDTH ** -0.5, 0.1875, ((0, 4),))
    second_residual = noise(arg_keys[10], (TOKENS_B, D), 1.0, 6.0, ((0, 8),))
    expert_norm_scale = jnp.clip(1.0 + 0.18 * jax.random.normal(arg_keys[11], (D,), jnp.float32), 0.1, 1.9)
    routes_keys = jax.random.split(jax.random.fold_in(arg_keys[12], 1), TOKENS_B // ROWS)
    routes_turns = jax.random.permutation(jax.random.fold_in(arg_keys[12], 3), TOKENS_B // ROWS)
    routes = jax.vmap(lambda own, number: deal_out(jax.random.fold_in(arg_keys[12], 2), own, number, ROWS, EXPERTS, TOPK, CAPQ, 2))(routes_keys, routes_turns).reshape((TOKENS_B, TOPK))
    specialist_mixing_factor = jnp.clip(0.1 + 0.9 * jax.random.uniform(arg_keys[13], (TOKENS_B, TOPK), jnp.float32) ** shard_levels(arg_keys[13], (TOKENS_B, TOPK), ((0, 32),), -0.2, 0.2), 0.1, 1.0)
    expert_gate_matrix = noise(arg_keys[14], (EXPERTS, D, FF), D ** -0.5, 0.125, ((0, 8), (2, 4)))
    expert_up_matrix = noise(arg_keys[15], (EXPERTS, D, FF), D ** -0.5, 0.125, ((0, 8), (2, 4)))
    expert_down_matrix = noise(arg_keys[16], (EXPERTS, FF, D), FF ** -0.5, 0.1875, ((0, 8), (1, 4)))
    return dict(queries=queries, forget_forward_logits=forget_forward_logits, forget_backward_logits=forget_backward_logits, values=values, output_gate_logits=output_gate_logits, lower_bound_forward=lower_bound_forward, lower_bound_backward=lower_bound_backward, extra_log_decay=extra_log_decay, head_norm_scale=head_norm_scale, output_projection=output_projection, second_residual=second_residual, expert_norm_scale=expert_norm_scale, routes=routes, specialist_mixing_factor=specialist_mixing_factor, expert_gate_matrix=expert_gate_matrix, expert_up_matrix=expert_up_matrix, expert_down_matrix=expert_down_matrix)


EPS = 1e-06
PRECISE_PRODUCT = lax.Precision.HIGHEST

def block_pass(feature, key_matrix_rows, value_rows, log_forget_decay):
    row_count, number_of_heads, channels = feature.shape
    blocks = row_count // SPAN
    lower_mask = jnp.tril(jnp.ones((SPAN, SPAN), bool))[:, :, None, None]

    def shaped(tensor):
        return tensor.reshape(blocks, SPAN, number_of_heads, tensor.shape[-1])

    def advance(progress, inputs):
        recurrent_memory, offset = progress
        query_tile_rows, address_piece_entries, content_piece_entries, decay_block = inputs
        progressive_summary = jnp.cumsum(decay_block, axis=0)
        spread_log = jnp.where(lower_mask, progressive_summary[:, None] - progressive_summary[None, :], -jnp.inf)
        scores = lax.optimization_barrier(jnp.sum(query_tile_rows[:, None] * address_piece_entries[None, :] * jnp.exp(spread_log), axis=-1))
        inner_part = jnp.einsum('tsh,shv->thv', scores, content_piece_entries, precision=PRECISE_PRODUCT)
        handed_summary = jnp.einsum('wbf,bfl->wbl', query_tile_rows * jnp.exp(progressive_summary), recurrent_memory, precision=PRECISE_PRODUCT)
        segment_fading_total = progressive_summary[-1]
        trained_portion = jnp.einsum('gkf,gkr->kfr', address_piece_entries * jnp.exp(segment_fading_total[None] - progressive_summary), content_piece_entries, precision=PRECISE_PRODUCT)
        recurrent_memory = jnp.exp(segment_fading_total)[:, :, None] * recurrent_memory + trained_portion
        return ((recurrent_memory, offset + segment_fading_total), (inner_part + handed_summary, query_tile_rows * jnp.exp(progressive_summary + offset)))
    initial = (jnp.zeros((number_of_heads, channels, value_rows.shape[-1]), jnp.float32), jnp.zeros((number_of_heads, channels), jnp.float32))
    (recurrent_memory, decay_total), (output_rows, query_decay_reach) = lax.scan(advance, initial, (shaped(feature), shaped(key_matrix_rows), shaped(value_rows), shaped(log_forget_decay)))
    return (output_rows.reshape(row_count, number_of_heads, -1), query_decay_reach.reshape(row_count, number_of_heads, channels), recurrent_memory, decay_total)

def forget_gate_terms(forget_gate_input, lower_bound_logit, extra_decay_rows, number_of_heads):
    row_count = forget_gate_input.shape[0]
    widened_values = forget_gate_input.astype(jnp.float32).reshape(row_count, number_of_heads, -1)
    lower_bound_share = jax.nn.sigmoid(lower_bound_logit).reshape(number_of_heads, -1)
    remaining_fraction = jax.nn.sigmoid(-lower_bound_logit).reshape(number_of_heads, -1)
    log_forget_decay = jnp.log(lower_bound_share + remaining_fraction * jax.nn.sigmoid(widened_values)) + extra_decay_rows[:, :, None]
    return (remaining_fraction * jax.nn.sigmoid(-widened_values), log_forget_decay)

def finish_heads(combined, head_norm_scale, output_gate_logits, number_of_heads):
    mean_square = lax.optimization_barrier(jnp.mean(combined * combined, axis=-1, keepdims=True))
    scaled = combined * lax.rsqrt(mean_square + EPS) * head_norm_scale.reshape(number_of_heads, -1)
    opened = scaled * jax.nn.silu(output_gate_logits.astype(jnp.float32)).reshape(combined.shape)
    return opened.astype(jnp.bfloat16).reshape(combined.shape[0], -1)

def normalize(tensor, gain):
    widened_values = tensor.astype(jnp.float32)
    return (widened_values * lax.rsqrt(lax.optimization_barrier(jnp.mean(widened_values * widened_values, axis=-1, keepdims=True)) + EPS) * gain).astype(jnp.bfloat16)

def reference(queries, forget_forward_logits, forget_backward_logits, values, output_gate_logits, lower_bound_forward, lower_bound_backward, extra_log_decay, head_norm_scale, output_projection, second_residual, expert_norm_scale, routes, specialist_mixing_factor, expert_gate_matrix, expert_up_matrix, expert_down_matrix):
    feature = jax.nn.silu(queries.astype(jnp.float32)).reshape(TOKENS_A, RECURRENT_HEADS, DK)
    value_rows = values.astype(jnp.float32).reshape(TOKENS_A, RECURRENT_HEADS, DV)
    combined = jnp.zeros(value_rows.shape, jnp.float32)
    for forget_gate_input, lower_bound_logit, reverse in ((forget_forward_logits, lower_bound_forward, False), (forget_backward_logits, lower_bound_backward, True)):
        key_matrix_rows, log_forget_decay = forget_gate_terms(forget_gate_input, lower_bound_logit, extra_log_decay, RECURRENT_HEADS)
        if reverse:
            output_rows = block_pass(jnp.flip(feature, 0), jnp.flip(key_matrix_rows, 0), jnp.flip(value_rows, 0), jnp.flip(log_forget_decay, 0))[0]
            output_rows = jnp.flip(output_rows, 0)
        else:
            output_rows = block_pass(feature, key_matrix_rows, value_rows, log_forget_decay)[0]
        combined = combined + output_rows
    mixer_hidden = finish_heads(combined, head_norm_scale, output_gate_logits, RECURRENT_HEADS)
    summed = jnp.zeros((TOKENS_A, D), jnp.float32)
    for group_index in range(N_TP):
        lower_edge = group_index * GROUP_WIDTH
        partial_value = jnp.dot(mixer_hidden[:, lower_edge:lower_edge + GROUP_WIDTH], output_projection[lower_edge:lower_edge + GROUP_WIDTH], preferred_element_type=jnp.float32)
        summed = summed + lax.optimization_barrier(partial_value.astype(jnp.bfloat16)).astype(jnp.float32)
    mixer_output = summed.astype(jnp.bfloat16)
    routed_normed = normalize(second_residual, expert_norm_scale)
    slot_total = N_EP * N_TP * CAPQ
    token_ids = jnp.arange(TOKENS_B, dtype=jnp.int32)

    def one_expert(accumulated, expert):
        chosen = routes == expert
        weight = lax.optimization_barrier(jnp.sum(jnp.where(chosen, specialist_mixing_factor, 0.0), axis=1))
        member = jnp.any(chosen, axis=1)
        token_position = (jnp.cumsum(member.astype(jnp.int32)) - 1).astype(jnp.int32)
        token_position = jnp.where(member, token_position, slot_total).astype(jnp.int32)
        slot_table = jnp.zeros((slot_total + 1,), jnp.int32).at[token_position].set(token_ids)[:slot_total]
        slot_weight = jnp.zeros((slot_total + 1,), jnp.float32).at[token_position].set(weight)[:slot_total]
        picked = routed_normed[slot_table]
        gated = jnp.dot(picked, expert_gate_matrix[expert], preferred_element_type=jnp.float32)
        lifted = jnp.dot(picked, expert_up_matrix[expert], preferred_element_type=jnp.float32)
        expert_hidden = (jax.nn.silu(gated) * lifted).astype(jnp.bfloat16)
        down_rows = expert_down_matrix[expert]
        result = jnp.zeros((slot_total, D), jnp.float32)
        for group_index in range(N_TP):
            lower_edge = group_index * EXPERT_PART
            partial_value = jnp.dot(expert_hidden[:, lower_edge:lower_edge + EXPERT_PART], down_rows[lower_edge:lower_edge + EXPERT_PART], preferred_element_type=jnp.float32)
            result = result + lax.optimization_barrier(partial_value.astype(jnp.bfloat16)).astype(jnp.float32)
        expert_result = lax.optimization_barrier(result.astype(jnp.bfloat16)).astype(jnp.float32)
        accumulated = accumulated.at[slot_table].add(slot_weight[:, None] * expert_result)
        return (accumulated, None)
    accumulated = lax.scan(one_expert, jnp.zeros((TOKENS_B, D), jnp.float32), jnp.arange(EXPERTS, dtype=jnp.int32))[0]
    routed_output = accumulated.astype(jnp.bfloat16)
    return (mixer_output, routed_output)
```

```python
import functools

import jax
import jax.numpy as jnp
from jax import lax
from jax.experimental import pallas as pl
from jax.experimental.pallas import tpu as pltpu
from jax.sharding import PartitionSpec as P

TOPK = 2
CHUNK = 128
LEAF = 16
DECAY_ROWS = 16
PIECES = 4
EPS = 1e-06
MESH = pl.DeviceIdType.MESH
F32 = jnp.float32
BF16 = jnp.bfloat16


def neighbours():
    place, count = lax.axis_index("tp"), lax.axis_size("tp")
    return place + 1 - 2 * lax.rem(place, 2), lax.rem(place + count // 2, count)


def greet(axis, n):
    me = lax.axis_index(axis)
    barrier = pltpu.get_barrier_semaphore()

    def one(step, carry):
        peer = lax.rem(me + step, n)
        pl.semaphore_signal(barrier, inc=1, device_id={axis: peer}, device_id_type=MESH)
        return carry

    lax.fori_loop(1, n, one, 0)


def dot_rows(a, b):
    return lax.dot_general(a, b, (((1,), (1,)), ((), ())), preferred_element_type=F32)


def gates(logits, bound, extra):
    shrink = jnp.exp(-logits)
    opened = 1.0 / (1.0 + shrink)
    floor_part = 1.0 / (1.0 + jnp.exp(-bound))
    complement = 1.0 / (1.0 + jnp.exp(bound))
    decay = jnp.log(floor_part + complement * opened) + extra
    return complement * (shrink * opened), decay


def referenced(total, size, place):
    blocks = total.reshape(CHUNK // size, size, total.shape[-1])
    anchor = jnp.broadcast_to(blocks[:, place : place + 1, :], blocks.shape)
    return total - anchor.reshape(total.shape)


def chunk_scores(feature, key, total, backward, rows, cols):
    scores = jnp.zeros((CHUNK, CHUNK), F32)
    size = CHUNK
    while size > LEAF:
        half = size // 2
        reach = jnp.exp(-jnp.abs(referenced(total, size, half if backward else half - 1)))
        part = dot_rows((feature * reach).astype(BF16), (key * reach).astype(BF16))
        late, early = (cols, rows) if backward else (rows, cols)
        mask = (rows // size == cols // size) & (late % size >= half) & (early % size < half)
        scores = scores + jnp.where(mask, part, 0.0)
        size = half
    spread = referenced(total, LEAF, LEAF // 2 if backward else LEAF // 2 - 1)
    part = dot_rows(
        (feature * jnp.exp(spread)).astype(BF16), (key * jnp.exp(-spread)).astype(BF16)
    )
    mask = (rows // LEAF == cols // LEAF) & ((rows <= cols) if backward else (rows >= cols))
    return scores + jnp.where(mask, part, 0.0)


def fused_kernel(
    n,
    quarters,
    q_any,
    ff_any,
    fb_any,
    v_any,
    og_any,
    lbf_ref,
    lbb_ref,
    extra_ref,
    scale_ref,
    proj_any,
    resid_any,
    gain_ref,
    routes_ref,
    mix_ref,
    gate_any,
    up_any,
    down_any,
    mixed_ref,
    routed_ref,
    q_ref,
    ff_ref,
    fb_ref,
    v_ref,
    og_ref,
    proj_ref,
    resid_ref,
    ranks_ref,
    shares_ref,
    chooser_ref,
    blend_ref,
    slots_ref,
    arrived_ref,
    gates_ref,
    ups_ref,
    downs_ref,
    active_ref,
    leaving_ref,
    returned_ref,
    local_ref,
    reach_ref,
    part_ref,
    fade_ref,
    state_out,
    state_in,
    hidden_ref,
    partial_ref,
    pieces_ref,
    load_sem,
    slot_send,
    slot_recv,
    state_send,
    state_recv,
    weight_send,
    weight_recv,
    back_send,
    back_recv,
    piece_send,
    piece_recv,
):
    me = lax.axis_index("ep")
    place = lax.axis_index("tp")
    group_rows, width = q_ref.shape
    row_count, width_model = resid_ref.shape
    chunks = group_rows // CHUNK
    heads = extra_ref.shape[0]
    channels = width // heads
    slot_total = slots_ref.shape[0]
    slot_count = slot_total // n
    pieces, _, span = leaving_ref.shape
    units = down_any.shape[1]
    beside, across = neighbours()

    first_row = pl.multiple_of(place * row_count, row_count)
    loads = [
        pltpu.make_async_copy(source, target, load_sem.at[i])
        for i, (source, target) in enumerate(
            (
                (resid_any.at[pl.ds(first_row, row_count)], resid_ref),
                (q_any, q_ref),
                (ff_any, ff_ref),
                (fb_any, fb_ref),
                (v_any, v_ref),
                (og_any, og_ref),
                (proj_any, proj_ref),
                (gate_any.at[0], gates_ref.at[3]),
                (up_any.at[0], ups_ref.at[3]),
            )
            + tuple(
                (
                    down_any.at[0, :, c * span : (c + 1) * span],
                    downs_ref.at[c, 3 * units : 4 * units],
                )
                for c in range(pieces)
            )
        )
    ]
    for load in loads:
        load.start()

    greet("ep", n)
    greet("tp", quarters)
    pl.semaphore_wait(pltpu.get_barrier_semaphore(), n + quarters - 2)

    def weight_copy(i, hop):
        if i < 2:
            own, held = ((gate_any.at[0], gates_ref), (up_any.at[0], ups_ref))[i]
            target, passed = held.at[hop], held.at[1]
        else:
            c = i - 2
            own = down_any.at[0, :, c * span : (c + 1) * span]
            target = downs_ref.at[c, hop * units : (hop + 1) * units]
            passed = downs_ref.at[c, units : 2 * units]
        return pltpu.make_async_remote_copy(
            src_ref=passed if hop == 2 else own,
            dst_ref=target,
            send_sem=weight_send.at[i, hop],
            recv_sem=weight_recv.at[i, hop],
            device_id={"tp": across if hop == 1 else beside},
            device_id_type=MESH,
        )

    for i in range(2 + pieces):
        weight_copy(i, 1).start()

    lanes = pl.ds(first_row, row_count)
    expert = lax.broadcasted_iota(jnp.int32, (n, row_count), 0)
    hits = jnp.zeros((n, row_count), F32)
    shares = jnp.zeros((n, row_count), F32)
    for k in range(TOPK):
        chosen = routes_ref[k : k + 1, lanes] == expert
        hits = jnp.where(chosen, 1.0, hits)
        shares = jnp.where(chosen, mix_ref[k : k + 1], shares)
    before = lax.broadcasted_iota(jnp.int32, (row_count, row_count), 0)
    after = lax.broadcasted_iota(jnp.int32, (row_count, row_count), 1)
    earlier = (before < after).astype(BF16)
    ranks = jnp.dot(hits.astype(BF16), earlier, preferred_element_type=F32)
    ranks_ref[...] = jnp.where(hits > 0.0, ranks, -1.0)
    shares_ref[...] = shares
    slot = lax.broadcasted_iota(jnp.int32, (slot_count, row_count), 0).astype(F32)
    picks, blends = [], []
    for e in range(n):
        match = slot == ranks_ref[e : e + 1]
        picks.append(jnp.where(match, 1.0, 0.0))
        blends.append(jnp.where(match, shares_ref[e : e + 1], 0.0))
    chooser_ref[...] = jnp.concatenate(picks, axis=0).astype(BF16)

    loads[0].wait()
    rows_wide = resid_ref[...].astype(F32)
    mean_square = jnp.mean(rows_wide * rows_wide, axis=-1, keepdims=True)
    own_rows = (rows_wide * lax.rsqrt(mean_square + EPS) * gain_ref[...]).astype(BF16)
    for g in range(slot_total // row_count):
        at = slice(g * row_count, (g + 1) * row_count)
        slots_ref[at] = jnp.dot(
            chooser_ref[at], own_rows, preferred_element_type=F32
        ).astype(BF16)

    def block(ref, index):
        return ref.at[pl.ds(pl.multiple_of(index * slot_count, slot_count), slot_count)]

    def slot_copy(target, source):
        return pltpu.make_async_remote_copy(
            src_ref=block(slots_ref, target),
            dst_ref=block(arrived_ref, source),
            send_sem=slot_send.at[target],
            recv_sem=slot_recv.at[source],
            device_id={"ep": target},
            device_id_type=MESH,
        )

    def back_copy(c, target, source):
        return pltpu.make_async_remote_copy(
            src_ref=block(leaving_ref.at[c], target),
            dst_ref=block(returned_ref.at[c], source),
            send_sem=back_send.at[c, target],
            recv_sem=back_recv.at[c, source],
            device_id={"ep": target},
            device_id_type=MESH,
        )

    def each_peer(act):
        def one(step, carry):
            act(lax.rem(me + step, n))
            return carry

        lax.fori_loop(1, n, one, 0)

    each_peer(lambda peer: slot_copy(peer, me).start())
    for i in range(2 + pieces):
        weight_copy(i, 0).start()
    here = pl.ds(pl.multiple_of(me * slot_count, slot_count), slot_count)
    arrived_ref[here] = slots_ref[here]
    blend = jnp.concatenate(blends, axis=0).T
    blend_high = blend.astype(BF16)
    blend_ref[0] = blend_high
    blend_ref[1] = (blend - blend_high.astype(F32)).astype(BF16)

    for load in loads[1:6]:
        load.wait()
    rows = lax.broadcasted_iota(jnp.int32, (CHUNK, CHUNK), 0)
    cols = lax.broadcasted_iota(jnp.int32, (CHUNK, CHUNK), 1)

    def local(c, carry):
        at = pl.ds(pl.multiple_of(c * CHUNK, CHUNK), CHUNK)
        for h in range(heads):
            lanes = slice(h * channels, (h + 1) * channels)
            queries = q_ref[at, lanes].astype(F32)
            feature = queries / (1.0 + jnp.exp(-queries))
            value_rows = v_ref[at, lanes]
            extra = jnp.broadcast_to(extra_ref[h : h + 1, at], (channels, CHUNK)).T
            scores = jnp.zeros((CHUNK, CHUNK), F32)
            for way, (logit_ref, bound_ref) in enumerate(((ff_ref, lbf_ref), (fb_ref, lbb_ref))):
                key, decay = gates(logit_ref[at, lanes].astype(F32), bound_ref[:, lanes], extra)
                order = (rows <= cols) if way else (rows >= cols)
                total = jnp.dot(
                    order.astype(F32),
                    decay,
                    preferred_element_type=F32,
                    precision=lax.Precision.HIGHEST,
                )
                edge = total[0:1] if way else total[CHUNK - 1 : CHUNK]
                scores = scores + chunk_scores(feature, key, total, way == 1, rows, cols)
                reach_ref[way, h, c] = (feature * jnp.exp(total)).astype(BF16)
                faded = (key * jnp.exp(edge - total)).astype(BF16)
                part_ref[way, h, c] = lax.dot_general(
                    value_rows, faded, (((0,), (0,)), ((), ())), preferred_element_type=F32
                )
                fade_ref[way, h, c] = jnp.broadcast_to(jnp.exp(edge), (8, channels))
            local_ref[h, c] = jnp.dot(
                scores.astype(BF16), value_rows, preferred_element_type=F32
            )
        return carry

    lax.fori_loop(0, chunks, local, 0)
    for way in range(2):
        for h in range(heads):
            state = jnp.zeros(part_ref.shape[3:], F32)
            fade = jnp.ones((1, channels), F32)
            for c in range(chunks)[:: -1 if way else 1]:
                step = fade_ref[way, h, c, 0:1]
                state = state * step + part_ref[way, h, c]
                fade = fade * step
            state_out[way, h, : state.shape[0]] = state.astype(BF16)
            state_out[way, h, state.shape[0] :] = jnp.broadcast_to(
                fade, (DECAY_ROWS, channels)
            ).astype(BF16)

    def state_copy(target, source):
        way = jnp.where(target > me, 0, 1)
        return pltpu.make_async_remote_copy(
            src_ref=state_out.at[way],
            dst_ref=state_in.at[source],
            send_sem=state_send.at[target],
            recv_sem=state_recv.at[source],
            device_id={"ep": target},
            device_id_type=MESH,
        )

    each_peer(lambda peer: state_copy(peer, me).start())

    def activate(i):
        arrived = arrived_ref[...]
        gated = jnp.dot(arrived, gates_ref[i], preferred_element_type=F32)
        lifted = jnp.dot(arrived, ups_ref[i], preferred_element_type=F32)
        active_ref[:, i * units : (i + 1) * units] = (
            gated / (1.0 + jnp.exp(-gated)) * lifted
        ).astype(BF16)

    for load in loads[6:]:
        load.wait()
    for i in range(2 + pieces):
        weight_copy(i, 0).wait_recv()
    weight_copy(0, 1).wait_recv()
    weight_copy(0, 2).start()
    each_peer(lambda peer: slot_copy(peer, peer).wait_recv())
    activate(3)
    activate(0)
    weight_copy(1, 1).wait_recv()
    weight_copy(1, 2).start()
    activate(1)
    weight_copy(0, 2).wait_recv()
    weight_copy(1, 2).wait_recv()
    activate(2)

    def results(c):
        weight_copy(2 + c, 1).wait_recv()
        weight_copy(2 + c, 2).start()
        weight_copy(2 + c, 2).wait_recv()
        leaving_ref[c] = jnp.dot(
            active_ref[...], downs_ref[c], preferred_element_type=F32
        ).astype(BF16)
        each_peer(lambda peer: back_copy(c, peer, me).start())
        returned_ref[c, here] = leaving_ref[c, here]

    def collect(c):
        each_peer(lambda peer: back_copy(c, peer, peer).wait_recv())
        came = returned_ref[c]
        total = jnp.dot(blend_ref[0], came, preferred_element_type=F32)
        total = total + jnp.dot(blend_ref[1], came, preferred_element_type=F32)
        routed_ref[:, c * span : (c + 1) * span] = total.astype(BF16)

    def finish_mixer():
        each_peer(lambda peer: state_copy(peer, peer).wait_recv())
        depth = part_ref.shape[3]
        for h in range(heads):
            for way in range(2):

                def one(hop, state, way=way, h=h):
                    source = n - 1 - hop if way else hop
                    step = state_in[source, h, depth : depth + DECAY_ROWS].astype(F32)[0:1]
                    return state * step + state_in[source, h, :depth].astype(F32)

                ahead = n - 1 - me if way else me
                state = lax.fori_loop(0, ahead, one, jnp.zeros(part_ref.shape[3:], F32))
                for c in range(chunks)[:: -1 if way else 1]:
                    local_ref[h, c] += dot_rows(reach_ref[way, h, c], state.astype(BF16))
                    state = state * fade_ref[way, h, c, 0:1] + part_ref[way, h, c]
            lanes = slice(h * channels, (h + 1) * channels)
            for c in range(chunks):
                at = slice(c * CHUNK, (c + 1) * CHUNK)
                combined = local_ref[h, c]
                mean_square = jnp.mean(combined * combined, axis=-1, keepdims=True)
                gate = og_ref[at, lanes].astype(F32)
                opened = combined * lax.rsqrt(mean_square + EPS) * scale_ref[:, lanes]
                hidden_ref[at, lanes] = (opened * (gate / (1.0 + jnp.exp(-gate)))).astype(BF16)

    def piece_copy(target, source):
        return pltpu.make_async_remote_copy(
            src_ref=partial_ref.at[target],
            dst_ref=pieces_ref.at[source],
            send_sem=piece_send.at[target],
            recv_sem=piece_recv.at[source],
            device_id={"tp": target},
            device_id_type=MESH,
        )

    def each_part(act):
        def one(step, carry):
            act(lax.rem(place + step, quarters))
            return carry

        lax.fori_loop(1, quarters, one, 0)

    def project():
        for part in range(quarters):
            at = slice(part * row_count, (part + 1) * row_count)
            partial_ref[part] = jnp.dot(
                hidden_ref[at], proj_ref[...], preferred_element_type=F32
            ).astype(BF16)
        each_part(lambda peer: piece_copy(peer, place).start())
        pieces_ref[place] = partial_ref[place]

    def gather_mixed():
        each_part(lambda peer: piece_copy(peer, peer).wait_recv())
        total = pieces_ref[0].astype(F32)
        for part in range(1, quarters):
            total = total + pieces_ref[part].astype(F32)
        mixed_ref[...] = total.astype(BF16)

    results(0)
    finish_mixer()
    results(1)
    project()
    for c in range(2, pieces):
        results(c)
    for c in range(pieces - 1):
        collect(c)
    gather_mixed()
    collect(pieces - 1)

    each_peer(lambda peer: slot_copy(peer, peer).wait_send())
    each_peer(lambda peer: state_copy(peer, peer).wait_send())
    for c in range(pieces):
        each_peer(lambda peer, c=c: back_copy(c, peer, peer).wait_send())
    each_part(lambda peer: piece_copy(peer, peer).wait_send())
    for i in range(2 + pieces):
        for hop in range(3):
            weight_copy(i, hop).wait_send()


def shards(
    queries,
    forget_forward_logits,
    forget_backward_logits,
    values,
    output_gate_logits,
    lower_bound_forward,
    lower_bound_backward,
    extra_log_decay,
    head_norm_scale,
    output_projection,
    second_residual,
    expert_norm_scale,
    routes,
    specialist_mixing_factor,
    expert_gate_matrix,
    expert_up_matrix,
    expert_down_matrix,
):
    group_rows, width_model = second_residual.shape
    quarters = lax.axis_size("tp")
    n = lax.axis_size("ep")
    row_count = group_rows // quarters
    slot_count = 2 * TOPK * row_count // n
    slot_total = n * slot_count
    width = queries.shape[1]
    heads = extra_log_decay.shape[1]
    channels = width // heads
    depth = values.shape[1] // heads
    chunks = group_rows // CHUNK
    units = expert_down_matrix.shape[1]
    span = width_model // PIECES
    vmem = pl.BlockSpec(memory_space=pltpu.VMEM)
    anywhere = pl.BlockSpec(memory_space=pl.ANY)
    state = (heads, depth + DECAY_ROWS, channels)
    block = (group_rows, width)
    out = jax.ShapeDtypeStruct((row_count, width_model), BF16)
    dma = pltpu.SemaphoreType.DMA
    return pl.pallas_call(
        functools.partial(fused_kernel, n, quarters),
        out_shape=(out, out),
        in_specs=[anywhere] * 5
        + [vmem] * 4
        + [anywhere] * 2
        + [vmem] * 3
        + [anywhere] * 3,
        out_specs=(vmem, vmem),
        scratch_shapes=[pltpu.VMEM(block, BF16)] * 5
        + [
            pltpu.VMEM((width, width_model), BF16),
            pltpu.VMEM((row_count, width_model), BF16),
            pltpu.VMEM((n, row_count), F32),
            pltpu.VMEM((n, row_count), F32),
            pltpu.VMEM((slot_total, row_count), BF16),
            pltpu.VMEM((2, row_count, slot_total), BF16),
            pltpu.VMEM((slot_total, width_model), BF16),
            pltpu.VMEM((slot_total, width_model), BF16),
            pltpu.VMEM((quarters,) + expert_gate_matrix.shape[1:], BF16),
            pltpu.VMEM((quarters,) + expert_up_matrix.shape[1:], BF16),
            pltpu.VMEM((PIECES, quarters * units, span), BF16),
            pltpu.VMEM((slot_total, quarters * units), BF16),
            pltpu.VMEM((PIECES, slot_total, span), BF16),
            pltpu.VMEM((PIECES, slot_total, span), BF16),
            pltpu.VMEM((heads, chunks, CHUNK, depth), F32),
            pltpu.VMEM((2, heads, chunks, CHUNK, channels), BF16),
            pltpu.VMEM((2, heads, chunks, depth, channels), F32),
            pltpu.VMEM((2, heads, chunks, 8, channels), F32),
            pltpu.VMEM((2,) + state, BF16),
            pltpu.VMEM((n,) + state, BF16),
            pltpu.VMEM(block, BF16),
            pltpu.VMEM((quarters, row_count, width_model), BF16),
            pltpu.VMEM((quarters, row_count, width_model), BF16),
            dma((9 + PIECES,)),
            dma((n,)),
            dma((n,)),
            dma((n,)),
            dma((n,)),
            dma((2 + PIECES, 3)),
            dma((2 + PIECES, 3)),
            dma((PIECES, n)),
            dma((PIECES, n)),
            dma((quarters,)),
            dma((quarters,)),
        ],
        compiler_params=pltpu.CompilerParams(
            collective_id=0, has_side_effects=True, vmem_limit_bytes=60 * 2**20
        ),
        cost_estimate=pl.CostEstimate(
            flops=4 * 10**10, bytes_accessed=30 * 2**20, transcendentals=0
        ),
        name="mix_and_route",
    )(
        queries,
        forget_forward_logits,
        forget_backward_logits,
        values,
        output_gate_logits,
        lower_bound_forward.reshape(1, -1),
        lower_bound_backward.reshape(1, -1),
        extra_log_decay.T,
        head_norm_scale.reshape(1, -1),
        output_projection,
        second_residual,
        expert_norm_scale.reshape(1, -1),
        routes.T,
        specialist_mixing_factor.T,
        expert_gate_matrix,
        expert_up_matrix,
        expert_down_matrix,
    )


def solution(mesh):
    in_specs = (
        P("ep", "tp"),
        P("ep", "tp"),
        P("ep", "tp"),
        P("ep", "tp"),
        P("ep", "tp"),
        P("tp"),
        P("tp"),
        P("ep", "tp"),
        P("tp"),
        P("tp", None),
        P("ep", None),
        P(),
        P("ep", None),
        P(("ep", "tp"), None),
        P("ep", None, "tp"),
        P("ep", None, "tp"),
        P("ep", "tp", None),
    )
    out_specs = (P(("ep", "tp"), None), P(("ep", "tp"), None))
    return jax.shard_map(shards, mesh=mesh, in_specs=in_specs, out_specs=out_specs, check_vma=False)
```

```python
import functools

import jax
import jax.numpy as jnp
from jax import lax
from jax.experimental import pallas as pl
from jax.experimental.pallas import tpu as pltpu
from jax.sharding import PartitionSpec as P

TOPK = 2
CHUNK = 128
LEAF = 16
DECAY_ROWS = 16
PIECES = 8
PLANES = 4
EPS = 1e-06
MESH = pl.DeviceIdType.MESH
F32 = jnp.float32
BF16 = jnp.bfloat16


def neighbours():
    place, count = lax.axis_index("tp"), lax.axis_size("tp")
    return place + 1 - 2 * lax.rem(place, 2), lax.rem(place + count // 2, count)


def greet(axis, n):
    me = lax.axis_index(axis)
    barrier = pltpu.get_barrier_semaphore()

    def one(step, carry):
        peer = lax.rem(me + step, n)
        pl.semaphore_signal(barrier, inc=1, device_id={axis: peer}, device_id_type=MESH)
        return carry

    lax.fori_loop(1, n, one, 0)


def dot_rows(a, b):
    return lax.dot_general(a, b, (((1,), (1,)), ((), ())), preferred_element_type=F32)


def gates(logits, bound, extra):
    shrink = jnp.exp(-logits)
    opened = 1.0 / (1.0 + shrink)
    floor_part = 1.0 / (1.0 + jnp.exp(-bound))
    complement = 1.0 / (1.0 + jnp.exp(bound))
    decay = jnp.log(floor_part + complement * opened) + extra
    return complement * (shrink * opened), decay


def referenced(total, size, place):
    blocks = total.reshape(CHUNK // size, size, total.shape[-1])
    anchor = jnp.broadcast_to(blocks[:, place : place + 1, :], blocks.shape)
    return total - anchor.reshape(total.shape)


def chunk_scores(feature, key, total, backward, rows, cols):
    scores = jnp.zeros((CHUNK, CHUNK), F32)
    size = CHUNK
    while size > LEAF:
        half = size // 2
        reach = jnp.exp(-jnp.abs(referenced(total, size, half if backward else half - 1)))
        part = dot_rows((feature * reach).astype(BF16), (key * reach).astype(BF16))
        late, early = (cols, rows) if backward else (rows, cols)
        mask = (rows // size == cols // size) & (late % size >= half) & (early % size < half)
        scores = scores + jnp.where(mask, part, 0.0)
        size = half
    spread = referenced(total, LEAF, LEAF // 2 if backward else LEAF // 2 - 1)
    part = dot_rows(
        (feature * jnp.exp(spread)).astype(BF16), (key * jnp.exp(-spread)).astype(BF16)
    )
    mask = (rows // LEAF == cols // LEAF) & ((rows <= cols) if backward else (rows >= cols))
    return scores + jnp.where(mask, part, 0.0)


def fused_kernel(
    n,
    quarters,
    q_any,
    ff_any,
    fb_any,
    v_any,
    og_any,
    lbf_ref,
    lbb_ref,
    extra_ref,
    scale_ref,
    proj_any,
    resid_any,
    gain_ref,
    routes_ref,
    mix_ref,
    gate_any,
    up_any,
    down_any,
    mixed_ref,
    routed_ref,
    q_ref,
    ff_ref,
    fb_ref,
    v_ref,
    og_ref,
    proj_ref,
    resid_ref,
    meta_ref,
    meta_in,
    rows_ref,
    rows_in,
    chooser_ref,
    blend_ref,
    merge_blend,
    slots_ref,
    arrived_ref,
    passed_ref,
    gates_ref,
    ups_ref,
    downs_ref,
    active_ref,
    leaving_ref,
    returned_ref,
    merge_in,
    merged_ref,
    merged_in,
    total_ref,
    local_ref,
    reach_ref,
    part_ref,
    fade_ref,
    state_out,
    state_in,
    hidden_ref,
    partial_ref,
    summed_ref,
    pieces_ref,
    load_sem,
    rows_sem,
    pass_send,
    merge_send,
    merge_recv,
    merged_send,
    merged_recv,
    slot_send,
    slot_recv,
    state_send,
    state_recv,
    weight_send,
    weight_recv,
    back_send,
    back_recv,
    piece_send,
    piece_recv,
):
    me = lax.axis_index("ep")
    place = lax.axis_index("tp")
    group_rows, width = q_ref.shape
    row_count, width_model = resid_ref.shape
    chunks = group_rows // CHUNK
    heads = extra_ref.shape[0]
    channels = width // heads
    slot_total = slots_ref.shape[0]
    slot_count = slot_total // n
    pieces, _, span = leaving_ref.shape
    units = down_any.shape[1]
    beside, across = neighbours()

    half = n // 2
    side = half * slot_count
    relayed = half == PLANES
    base = me // half * half
    other = half - base
    partner = lax.rem(me + half, n)
    plane = me // 2
    at_end = (plane == 0) | (plane == n // 2 - 1)

    def when_end(act):
        if relayed:
            pl.when(at_end)(act)

    def when_middle(act):
        if relayed:
            pl.when(jnp.logical_not(at_end))(act)
        else:
            act()

    def when_passing(act):
        if relayed:
            pl.when(jnp.logical_not(at_end))(act)

    first_row = pl.multiple_of(place * row_count, row_count)
    loads = [
        pltpu.make_async_copy(source, target, load_sem.at[i])
        for i, (source, target) in enumerate(
            (
                (resid_any.at[pl.ds(first_row, row_count)], resid_ref),
                (q_any, q_ref),
                (ff_any, ff_ref),
                (fb_any, fb_ref),
                (v_any, v_ref),
                (og_any, og_ref),
                (proj_any, proj_ref),
                (gate_any.at[0], gates_ref.at[3]),
                (up_any.at[0], ups_ref.at[3]),
            )
            + tuple(
                (
                    down_any.at[0, :, c * span : (c + 1) * span],
                    downs_ref.at[c, 3 * units : 4 * units],
                )
                for c in range(pieces)
            )
        )
    ]
    for load in loads:
        load.start()

    greet("ep", n)
    greet("tp", quarters)
    pl.semaphore_wait(pltpu.get_barrier_semaphore(), n + quarters - 2)

    def weight_copy(i, hop):
        if i < 2:
            own, held = ((gate_any.at[0], gates_ref), (up_any.at[0], ups_ref))[i]
            target, passed = held.at[hop], held.at[1]
        else:
            c = i - 2
            own = down_any.at[0, :, c * span : (c + 1) * span]
            target = downs_ref.at[c, hop * units : (hop + 1) * units]
            passed = downs_ref.at[c, units : 2 * units]
        return pltpu.make_async_remote_copy(
            src_ref=passed if hop == 2 else own,
            dst_ref=target,
            send_sem=weight_send.at[i, hop],
            recv_sem=weight_recv.at[i, hop],
            device_id={"tp": across if hop == 1 else beside},
            device_id_type=MESH,
        )

    for i in range(2 + pieces):
        weight_copy(i, 1).start()

    lanes = pl.ds(first_row, row_count)
    expert = lax.broadcasted_iota(jnp.int32, (n, row_count), 0)
    hits = jnp.zeros((n, row_count), F32)
    shares = jnp.zeros((n, row_count), F32)
    for k in range(TOPK):
        chosen = routes_ref[k : k + 1, lanes] == expert
        hits = jnp.where(chosen, 1.0, hits)
        shares = jnp.where(chosen, mix_ref[k : k + 1], shares)
    before = lax.broadcasted_iota(jnp.int32, (row_count, row_count), 0)
    after = lax.broadcasted_iota(jnp.int32, (row_count, row_count), 1)
    earlier = (before < after).astype(BF16)
    ranks = jnp.dot(hits.astype(BF16), earlier, preferred_element_type=F32)
    meta_ref[0] = jnp.where(hits > 0.0, ranks, -1.0)
    meta_ref[1] = shares
    slot = lax.broadcasted_iota(jnp.int32, (slot_count, row_count), 0).astype(F32)

    def selection(ref, first, count, weighted):
        parts = []
        for j in range(count):
            match = slot == ref[0, pl.ds(first + j, 1)]
            parts.append(jnp.where(match, ref[1, pl.ds(first + j, 1)] if weighted else 1.0, 0.0))
        return jnp.concatenate(parts, axis=0)

    def split(weights):
        high = weights.astype(BF16)
        return high, (weights - high.astype(F32)).astype(BF16)

    loads[0].wait()
    rows_wide = resid_ref[...].astype(F32)
    mean_square = jnp.mean(rows_wide * rows_wide, axis=-1, keepdims=True)
    rows_ref[...] = (rows_wide * lax.rsqrt(mean_square + EPS) * gain_ref[...]).astype(BF16)

    def rows_copy(i):
        return pltpu.make_async_remote_copy(
            src_ref=(rows_ref, meta_ref)[i],
            dst_ref=(rows_in, meta_in)[i],
            send_sem=rows_sem.at[0, i],
            recv_sem=rows_sem.at[1, i],
            device_id={"ep": partner},
            device_id_type=MESH,
        )

    @when_end
    def _():
        rows_copy(1).start()
        rows_copy(0).start()

    chooser_ref[...] = selection(meta_ref, 0, n, False).astype(BF16)
    for g in range(slot_total // row_count):
        at = slice(g * row_count, (g + 1) * row_count)
        slots_ref[at] = jnp.dot(
            chooser_ref[at], rows_ref[...], preferred_element_type=F32
        ).astype(BF16)

    def block(ref, index):
        return ref.at[pl.ds(pl.multiple_of(index * slot_count, slot_count), slot_count)]

    def slot_copy(target, source):
        return pltpu.make_async_remote_copy(
            src_ref=block(slots_ref, target),
            dst_ref=block(arrived_ref, source),
            send_sem=slot_send.at[target],
            recv_sem=slot_recv.at[source],
            device_id={"ep": target},
            device_id_type=MESH,
        )

    def back_copy(c, target, source):
        return pltpu.make_async_remote_copy(
            src_ref=block(leaving_ref.at[c], target),
            dst_ref=block(returned_ref.at[c], source),
            send_sem=back_send.at[c, target],
            recv_sem=back_recv.at[c, source],
            device_id={"ep": target},
            device_id_type=MESH,
        )

    def each_peer(act):
        def one(step, carry):
            act(lax.rem(me + step, n))
            return carry

        lax.fori_loop(1, n, one, 0)

    def each_near(act):
        def one(step, carry):
            act(base + lax.rem(me - base + step, half))
            return carry

        lax.fori_loop(1, half, one, 0)

    def each_far(act):
        def one(step, carry):
            act(other + lax.rem(me - base + step, half))
            return carry

        lax.fori_loop(0, half, one, 0)

    when_middle(lambda: each_far(lambda peer: slot_copy(peer, me).start()))
    each_near(lambda peer: slot_copy(peer, me).start())
    for i in range(2 + pieces):
        weight_copy(i, 0).start()
    here = pl.ds(pl.multiple_of(me * slot_count, slot_count), slot_count)
    arrived_ref[here] = slots_ref[here]
    for h in range(2):
        blend_ref[h, 0], blend_ref[h, 1] = split(selection(meta_ref, h * half, half, True).T)

    for load in loads[1:6]:
        load.wait()
    rows = lax.broadcasted_iota(jnp.int32, (CHUNK, CHUNK), 0)
    cols = lax.broadcasted_iota(jnp.int32, (CHUNK, CHUNK), 1)

    def local(c, carry):
        at = pl.ds(pl.multiple_of(c * CHUNK, CHUNK), CHUNK)
        for h in range(heads):
            lanes = slice(h * channels, (h + 1) * channels)
            queries = q_ref[at, lanes].astype(F32)
            feature = queries / (1.0 + jnp.exp(-queries))
            value_rows = v_ref[at, lanes]
            extra = jnp.broadcast_to(extra_ref[h : h + 1, at], (channels, CHUNK)).T
            scores = jnp.zeros((CHUNK, CHUNK), F32)
            for way, (logit_ref, bound_ref) in enumerate(((ff_ref, lbf_ref), (fb_ref, lbb_ref))):
                key, decay = gates(logit_ref[at, lanes].astype(F32), bound_ref[:, lanes], extra)
                order = (rows <= cols) if way else (rows >= cols)
                total = jnp.dot(
                    order.astype(F32),
                    decay,
                    preferred_element_type=F32,
                    precision=lax.Precision.HIGHEST,
                )
                edge = total[0:1] if way else total[CHUNK - 1 : CHUNK]
                scores = scores + chunk_scores(feature, key, total, way == 1, rows, cols)
                reach_ref[way, h, c] = (feature * jnp.exp(total)).astype(BF16)
                faded = (key * jnp.exp(edge - total)).astype(BF16)
                part_ref[way, h, c] = lax.dot_general(
                    value_rows, faded, (((0,), (0,)), ((), ())), preferred_element_type=F32
                )
                fade_ref[way, h, c] = jnp.broadcast_to(jnp.exp(edge), (8, channels))
            local_ref[h, c] = jnp.dot(
                scores.astype(BF16), value_rows, preferred_element_type=F32
            )
        return carry

    lax.fori_loop(0, chunks, local, 0)
    for way in range(2):
        for h in range(heads):
            state = jnp.zeros(part_ref.shape[3:], F32)
            fade = jnp.ones((1, channels), F32)
            for c in range(chunks)[:: -1 if way else 1]:
                step = fade_ref[way, h, c, 0:1]
                state = state * step + part_ref[way, h, c]
                fade = fade * step
            state_out[way, h, : state.shape[0]] = state.astype(BF16)
            state_out[way, h, state.shape[0] :] = jnp.broadcast_to(
                fade, (DECAY_ROWS, channels)
            ).astype(BF16)

    def state_copy(target, source):
        way = jnp.where(target > me, 0, 1)
        return pltpu.make_async_remote_copy(
            src_ref=state_out.at[way],
            dst_ref=state_in.at[source],
            send_sem=state_send.at[target],
            recv_sem=state_recv.at[source],
            device_id={"ep": target},
            device_id_type=MESH,
        )

    each_peer(lambda peer: state_copy(peer, me).start())

    def activate(i):
        arrived = arrived_ref[...]
        gated = jnp.dot(arrived, gates_ref[i], preferred_element_type=F32)
        lifted = jnp.dot(arrived, ups_ref[i], preferred_element_type=F32)
        active_ref[:, i * units : (i + 1) * units] = (
            gated / (1.0 + jnp.exp(-gated)) * lifted
        ).astype(BF16)

    for load in loads[6:]:
        load.wait()
    for i in range(2 + pieces):
        weight_copy(i, 0).wait_recv()
    weight_copy(0, 1).wait_recv()
    weight_copy(0, 2).start()

    def pass_copy(target):
        return pltpu.make_async_remote_copy(
            src_ref=block(passed_ref, target - base),
            dst_ref=block(arrived_ref, partner),
            send_sem=pass_send.at[target - base],
            recv_sem=slot_recv.at[partner],
            device_id={"ep": target},
            device_id_type=MESH,
        )

    @when_passing
    def _():
        rows_copy(1).wait_recv()
        rows_copy(0).wait_recv()
        chosen = selection(meta_in, base, half, False).astype(BF16)
        passed_ref[...] = jnp.dot(chosen, rows_in[...], preferred_element_type=F32).astype(BF16)
        each_near(lambda peer: pass_copy(peer).start())
        arrived_ref[pl.ds(pl.multiple_of(partner * slot_count, slot_count), slot_count)] = (
            passed_ref[pl.ds(pl.multiple_of((me - base) * slot_count, slot_count), slot_count)]
        )
        merge_blend[0], merge_blend[1] = split(selection(meta_in, base, half, True).T)

    each_near(lambda peer: slot_copy(peer, peer).wait_recv())

    def far_slots(peer):
        if relayed:
            pl.when(at_end | (peer != partner))(lambda: slot_copy(peer, peer).wait_recv())
        else:
            slot_copy(peer, peer).wait_recv()

    each_far(far_slots)
    activate(3)
    activate(0)
    weight_copy(1, 1).wait_recv()
    weight_copy(1, 2).start()
    activate(1)
    weight_copy(0, 2).wait_recv()
    weight_copy(1, 2).wait_recv()
    activate(2)

    mine = pl.ds(pl.multiple_of((me - base) * slot_count, slot_count), slot_count)

    def merge_copy(c, dest, source):
        return pltpu.make_async_remote_copy(
            src_ref=block(leaving_ref.at[c], dest),
            dst_ref=block(merge_in.at[c], source - base),
            send_sem=merge_send.at[c, dest],
            recv_sem=merge_recv.at[c, source],
            device_id={"ep": lax.rem(dest + half, n)},
            device_id_type=MESH,
        )

    def far_back(c, peer, act):
        if not relayed:
            getattr(back_copy(c, peer, me), act)()
            return
        far_plane = peer // 2
        far_end = (far_plane == 0) | (far_plane == n // 2 - 1)

        @pl.when(far_end & (peer != partner))
        def _():
            getattr(merge_copy(c, peer, me), act)()

        @pl.when(jnp.logical_not(far_end))
        def _():
            getattr(back_copy(c, peer, me), act)()

    def merged_copy(c):
        return pltpu.make_async_remote_copy(
            src_ref=merged_ref.at[c],
            dst_ref=merged_in.at[c],
            send_sem=merged_send.at[c],
            recv_sem=merged_recv.at[c],
            device_id={"ep": partner},
            device_id_type=MESH,
        )

    def blended(weights, values):
        total = jnp.dot(weights[0], values, preferred_element_type=F32)
        return total + jnp.dot(weights[1], values, preferred_element_type=F32)

    def merge(c):
        @when_passing
        def _():
            each_near(lambda peer: merge_copy(c, partner, peer).wait_recv())
            merged_ref[c] = blended(merge_blend, merge_in[c]).astype(BF16)
            merged_copy(c).start()

    def results(c):
        weight_copy(2 + c, 1).wait_recv()
        weight_copy(2 + c, 2).start()
        weight_copy(2 + c, 2).wait_recv()
        leaving_ref[c] = jnp.dot(
            active_ref[...], downs_ref[c], preferred_element_type=F32
        ).astype(BF16)
        each_far(lambda peer: far_back(c, peer, "start"))
        each_near(lambda peer: back_copy(c, peer, me).start())
        returned_ref[c, here] = leaving_ref[c, here]

        @when_passing
        def _():
            merge_in[c, mine] = leaving_ref[
                c, pl.ds(pl.multiple_of(partner * slot_count, slot_count), slot_count)
            ]

    def collect(c):
        each_near(lambda peer: back_copy(c, peer, peer).wait_recv())
        near = returned_ref[c, pl.ds(pl.multiple_of(base * slot_count, side), side)]
        total_ref[...] = blended(blend_ref.at[base // half], near)

        @when_middle
        def _():
            each_far(lambda peer: back_copy(c, peer, peer).wait_recv())
            far = returned_ref[c, pl.ds(pl.multiple_of(other * slot_count, side), side)]
            total_ref[...] += blended(blend_ref.at[other // half], far)

        @when_end
        def _():
            merged_copy(c).wait_recv()
            total_ref[...] += merged_in[c].astype(F32)

        routed_ref[:, c * span : (c + 1) * span] = total_ref[...].astype(BF16)

    def finish_mixer():
        each_peer(lambda peer: state_copy(peer, peer).wait_recv())
        depth = part_ref.shape[3]
        for h in range(heads):
            for way in range(2):

                def one(hop, state, way=way, h=h):
                    source = n - 1 - hop if way else hop
                    step = state_in[source, h, depth : depth + DECAY_ROWS].astype(F32)[0:1]
                    return state * step + state_in[source, h, :depth].astype(F32)

                ahead = n - 1 - me if way else me
                state = lax.fori_loop(0, ahead, one, jnp.zeros(part_ref.shape[3:], F32))
                for c in range(chunks)[:: -1 if way else 1]:
                    local_ref[h, c] += dot_rows(reach_ref[way, h, c], state.astype(BF16))
                    state = state * fade_ref[way, h, c, 0:1] + part_ref[way, h, c]
            lanes = slice(h * channels, (h + 1) * channels)
            for c in range(chunks):
                at = slice(c * CHUNK, (c + 1) * CHUNK)
                combined = local_ref[h, c]
                mean_square = jnp.mean(combined * combined, axis=-1, keepdims=True)
                gate = og_ref[at, lanes].astype(F32)
                opened = combined * lax.rsqrt(mean_square + EPS) * scale_ref[:, lanes]
                hidden_ref[at, lanes] = (opened * (gate / (1.0 + jnp.exp(-gate)))).astype(BF16)

    diagonal = lax.rem(beside + quarters // 2, quarters)

    def piece_copy(i):
        return pltpu.make_async_remote_copy(
            src_ref=(partial_ref.at[0], partial_ref.at[1], summed_ref)[i],
            dst_ref=pieces_ref.at[i],
            send_sem=piece_send.at[i],
            recv_sem=piece_recv.at[i],
            device_id={"tp": across if i == 2 else beside},
            device_id_type=MESH,
        )

    def project():
        for i, part in enumerate((diagonal, beside, across, place)):
            at = pl.ds(pl.multiple_of(part * row_count, row_count), row_count)
            partial_ref[i] = jnp.dot(
                hidden_ref[at], proj_ref[...], preferred_element_type=F32
            ).astype(BF16)
            if i < 2:
                piece_copy(i).start()

    def cross():
        piece_copy(0).wait_recv()
        summed_ref[...] = (partial_ref[2].astype(F32) + pieces_ref[0].astype(F32)).astype(BF16)
        piece_copy(2).start()

    def gather_mixed():
        piece_copy(1).wait_recv()
        piece_copy(2).wait_recv()
        total = partial_ref[3].astype(F32) + pieces_ref[1].astype(F32)
        mixed_ref[...] = (total + pieces_ref[2].astype(F32)).astype(BF16)

    results(0)
    results(1)
    finish_mixer()
    results(2)
    project()
    merge(0)
    results(3)
    cross()
    merge(1)
    for c in range(4, pieces):
        results(c)
        merge(c - 2)
    collect(0)
    merge(pieces - 2)
    collect(1)
    merge(pieces - 1)
    for c in range(2, pieces - 1):
        collect(c)
    gather_mixed()
    collect(pieces - 1)

    @when_end
    def _():
        rows_copy(0).wait_send()
        rows_copy(1).wait_send()

    when_middle(lambda: each_far(lambda peer: slot_copy(peer, me).wait_send()))
    each_near(lambda peer: slot_copy(peer, me).wait_send())
    when_passing(lambda: each_near(lambda peer: pass_copy(peer).wait_send()))
    each_peer(lambda peer: state_copy(peer, peer).wait_send())

    def leave(c, carry):
        each_far(lambda peer: far_back(c, peer, "wait_send"))
        each_near(lambda peer: back_copy(c, peer, me).wait_send())
        when_passing(lambda: merged_copy(c).wait_send())
        return carry

    lax.fori_loop(0, pieces, leave, 0)
    for i in range(3):
        piece_copy(i).wait_send()
    for i in range(2 + pieces):
        for hop in range(3):
            weight_copy(i, hop).wait_send()


def shards(
    queries,
    forget_forward_logits,
    forget_backward_logits,
    values,
    output_gate_logits,
    lower_bound_forward,
    lower_bound_backward,
    extra_log_decay,
    head_norm_scale,
    output_projection,
    second_residual,
    expert_norm_scale,
    routes,
    specialist_mixing_factor,
    expert_gate_matrix,
    expert_up_matrix,
    expert_down_matrix,
):
    group_rows, width_model = second_residual.shape
    quarters = lax.axis_size("tp")
    n = lax.axis_size("ep")
    row_count = group_rows // quarters
    slot_count = 2 * TOPK * row_count // n
    slot_total = n * slot_count
    width = queries.shape[1]
    heads = extra_log_decay.shape[1]
    channels = width // heads
    depth = values.shape[1] // heads
    chunks = group_rows // CHUNK
    units = expert_down_matrix.shape[1]
    span = width_model // PIECES
    vmem = pl.BlockSpec(memory_space=pltpu.VMEM)
    anywhere = pl.BlockSpec(memory_space=pl.ANY)
    state = (heads, depth + DECAY_ROWS, channels)
    block = (group_rows, width)
    out = jax.ShapeDtypeStruct((row_count, width_model), BF16)
    dma = pltpu.SemaphoreType.DMA
    return pl.pallas_call(
        functools.partial(fused_kernel, n, quarters),
        out_shape=(out, out),
        in_specs=[anywhere] * 5
        + [vmem] * 4
        + [anywhere] * 2
        + [vmem] * 3
        + [anywhere] * 3,
        out_specs=(vmem, vmem),
        scratch_shapes=[pltpu.VMEM(block, BF16)] * 5
        + [
            pltpu.VMEM((width, width_model), BF16),
            pltpu.VMEM((row_count, width_model), BF16),
            pltpu.VMEM((2, n, row_count), F32),
            pltpu.VMEM((2, n, row_count), F32),
            pltpu.VMEM((row_count, width_model), BF16),
            pltpu.VMEM((row_count, width_model), BF16),
            pltpu.VMEM((slot_total, row_count), BF16),
            pltpu.VMEM((2, 2, row_count, slot_total // 2), BF16),
            pltpu.VMEM((2, row_count, slot_total // 2), BF16),
            pltpu.VMEM((slot_total, width_model), BF16),
            pltpu.VMEM((slot_total, width_model), BF16),
            pltpu.VMEM((slot_total // 2, width_model), BF16),
            pltpu.VMEM((quarters,) + expert_gate_matrix.shape[1:], BF16),
            pltpu.VMEM((quarters,) + expert_up_matrix.shape[1:], BF16),
            pltpu.VMEM((PIECES, quarters * units, span), BF16),
            pltpu.VMEM((slot_total, quarters * units), BF16),
            pltpu.VMEM((PIECES, slot_total, span), BF16),
            pltpu.VMEM((PIECES, slot_total, span), BF16),
            pltpu.VMEM((PIECES, slot_total // 2, span), BF16),
            pltpu.VMEM((PIECES, row_count, span), BF16),
            pltpu.VMEM((PIECES, row_count, span), BF16),
            pltpu.VMEM((row_count, span), F32),
            pltpu.VMEM((heads, chunks, CHUNK, depth), F32),
            pltpu.VMEM((2, heads, chunks, CHUNK, channels), BF16),
            pltpu.VMEM((2, heads, chunks, depth, channels), F32),
            pltpu.VMEM((2, heads, chunks, 8, channels), F32),
            pltpu.VMEM((2,) + state, BF16),
            pltpu.VMEM((n,) + state, BF16),
            pltpu.VMEM(block, BF16),
            pltpu.VMEM((4, row_count, width_model), BF16),
            pltpu.VMEM((row_count, width_model), BF16),
            pltpu.VMEM((3, row_count, width_model), BF16),
            dma((9 + PIECES,)),
            dma((2, 2)),
            dma((n // 2,)),
            dma((PIECES, n)),
            dma((PIECES, n)),
            dma((PIECES,)),
            dma((PIECES,)),
            dma((n,)),
            dma((n,)),
            dma((n,)),
            dma((n,)),
            dma((2 + PIECES, 3)),
            dma((2 + PIECES, 3)),
            dma((PIECES, n)),
            dma((PIECES, n)),
            dma((3,)),
            dma((3,)),
        ],
        compiler_params=pltpu.CompilerParams(
            collective_id=0, has_side_effects=True, vmem_limit_bytes=48 * 2**20
        ),
        cost_estimate=pl.CostEstimate(
            flops=4 * 10**10, bytes_accessed=30 * 2**20, transcendentals=0
        ),
        name="mix_and_route",
    )(
        *(
            pltpu.with_memory_space_constraint(operand, pltpu.HBM)
            for operand in (
                queries,
                forget_forward_logits,
                forget_backward_logits,
                values,
                output_gate_logits,
                lower_bound_forward.reshape(1, -1),
                lower_bound_backward.reshape(1, -1),
                extra_log_decay.T,
                head_norm_scale.reshape(1, -1),
                output_projection,
                second_residual,
                expert_norm_scale.reshape(1, -1),
                routes.T,
                specialist_mixing_factor.T,
                expert_gate_matrix,
                expert_up_matrix,
                expert_down_matrix,
            )
        )
    )


def solution(mesh):
    in_specs = (
        P("ep", "tp"),
        P("ep", "tp"),
        P("ep", "tp"),
        P("ep", "tp"),
        P("ep", "tp"),
        P("tp"),
        P("tp"),
        P("ep", "tp"),
        P("tp"),
        P("tp", None),
        P("ep", None),
        P(),
        P("ep", None),
        P(("ep", "tp"), None),
        P("ep", None, "tp"),
        P("ep", None, "tp"),
        P("ep", "tp", None),
    )
    out_specs = (P(("ep", "tp"), None), P(("ep", "tp"), None))
    return jax.shard_map(shards, mesh=mesh, in_specs=in_specs, out_specs=out_specs, check_vma=False)
```

```python
import functools

import jax
import jax.numpy as jnp
from jax import lax
from jax.experimental import pallas as pl
from jax.experimental.pallas import tpu as pltpu
from jax.sharding import PartitionSpec as P

TOPK = 2
CHUNK = 128
LEAF = 16
DECAY_ROWS = 16
PIECES = 8
PLANES = 4
EPS = 1e-06
MESH = pl.DeviceIdType.MESH
F32 = jnp.float32
BF16 = jnp.bfloat16


def neighbours():
    place, count = lax.axis_index("tp"), lax.axis_size("tp")
    return place + 1 - 2 * lax.rem(place, 2), lax.rem(place + count // 2, count)


def greet(axis, n):
    me = lax.axis_index(axis)
    barrier = pltpu.get_barrier_semaphore()

    def one(step, carry):
        peer = lax.rem(me + step, n)
        pl.semaphore_signal(barrier, inc=1, device_id={axis: peer}, device_id_type=MESH)
        return carry

    lax.fori_loop(1, n, one, 0)


def dot_rows(a, b):
    return lax.dot_general(a, b, (((1,), (1,)), ((), ())), preferred_element_type=F32)


def gates(logits, bound, extra):
    shrink = jnp.exp(-logits)
    opened = 1.0 / (1.0 + shrink)
    floor_part = 1.0 / (1.0 + jnp.exp(-bound))
    complement = 1.0 / (1.0 + jnp.exp(bound))
    decay = jnp.log(floor_part + complement * opened) + extra
    return complement * (shrink * opened), decay


def referenced(total, size, place):
    blocks = total.reshape(CHUNK // size, size, total.shape[-1])
    anchor = jnp.broadcast_to(blocks[:, place : place + 1, :], blocks.shape)
    return total - anchor.reshape(total.shape)


def chunk_scores(feature, key, total, backward, rows, cols):
    scores = jnp.zeros((CHUNK, CHUNK), F32)
    size = CHUNK
    while size > LEAF:
        half = size // 2
        reach = jnp.exp(-jnp.abs(referenced(total, size, half if backward else half - 1)))
        part = dot_rows((feature * reach).astype(BF16), (key * reach).astype(BF16))
        late, early = (cols, rows) if backward else (rows, cols)
        mask = (rows // size == cols // size) & (late % size >= half) & (early % size < half)
        scores = scores + jnp.where(mask, part, 0.0)
        size = half
    spread = referenced(total, LEAF, LEAF // 2 if backward else LEAF // 2 - 1)
    part = dot_rows(
        (feature * jnp.exp(spread)).astype(BF16), (key * jnp.exp(-spread)).astype(BF16)
    )
    mask = (rows // LEAF == cols // LEAF) & ((rows <= cols) if backward else (rows >= cols))
    return scores + jnp.where(mask, part, 0.0)


def fused_kernel(
    n,
    quarters,
    q_any,
    ff_any,
    fb_any,
    v_any,
    og_any,
    lbf_ref,
    lbb_ref,
    extra_ref,
    scale_ref,
    proj_any,
    resid_any,
    gain_ref,
    routes_ref,
    mix_ref,
    gate_any,
    up_any,
    down_any,
    mixed_ref,
    routed_ref,
    q_ref,
    ff_ref,
    fb_ref,
    v_ref,
    og_ref,
    proj_ref,
    resid_ref,
    meta_ref,
    meta_in,
    rows_ref,
    rows_in,
    chooser_ref,
    blend_ref,
    merge_blend,
    slots_ref,
    arrived_ref,
    passed_ref,
    gates_ref,
    ups_ref,
    downs_ref,
    gated_ref,
    active_ref,
    leaving_ref,
    returned_ref,
    merge_in,
    merged_ref,
    merged_in,
    total_ref,
    local_ref,
    reach_ref,
    part_ref,
    fade_ref,
    state_out,
    state_in,
    hidden_ref,
    partial_ref,
    summed_ref,
    pieces_ref,
    load_sem,
    rows_sem,
    pass_send,
    merge_recv,
    merged_send,
    merged_recv,
    slot_send,
    slot_recv,
    state_send,
    state_recv,
    weight_send,
    weight_recv,
    back_send,
    back_recv,
    piece_send,
    piece_recv,
):
    me = lax.axis_index("ep")
    place = lax.axis_index("tp")
    group_rows, width = q_ref.shape
    row_count, width_model = resid_ref.shape
    chunks = group_rows // CHUNK
    heads = extra_ref.shape[0]
    channels = width // heads
    slot_total = slots_ref.shape[0]
    slot_count = slot_total // n
    pieces, _, span = leaving_ref.shape
    units = down_any.shape[1]
    beside, across = neighbours()

    half = n // 2
    side = half * slot_count
    relayed = half == PLANES
    base = me // half * half
    other = half - base
    partner = lax.rem(me + half, n)
    plane = me // 2
    at_end = (plane == 0) | (plane == n // 2 - 1)

    def when_end(act):
        if relayed:
            pl.when(at_end)(act)

    def when_middle(act):
        if relayed:
            pl.when(jnp.logical_not(at_end))(act)
        else:
            act()

    def when_passing(act):
        if relayed:
            pl.when(jnp.logical_not(at_end))(act)

    greet("ep", n)
    greet("tp", quarters)
    first_row = pl.multiple_of(place * row_count, row_count)
    loads = [
        pltpu.make_async_copy(source, target, load_sem.at[i])
        for i, (source, target) in enumerate(
            (
                (resid_any.at[pl.ds(first_row, row_count)], resid_ref),
                (q_any, q_ref),
                (ff_any, ff_ref),
                (fb_any, fb_ref),
                (v_any, v_ref),
                (og_any, og_ref),
                (proj_any, proj_ref),
                (gate_any.at[0], gates_ref.at[3]),
                (up_any.at[0], ups_ref.at[3]),
            )
        )
    ]
    down_loads = [
        pltpu.make_async_copy(
            down_any.at[0, :, c * span : (c + 1) * span],
            downs_ref.at[c, 3 * units : 4 * units],
            load_sem.at[9],
        )
        for c in range(pieces)
    ]
    for load in loads + down_loads:
        load.start()

    pl.semaphore_wait(pltpu.get_barrier_semaphore(), n + quarters - 2)

    def weight_copy(i, hop):
        if i < 2:
            own, held = ((gate_any.at[0], gates_ref), (up_any.at[0], ups_ref))[i]
            target, passed = held.at[hop], held.at[1]
        else:
            c = i - 2
            own = down_any.at[0, :, c * span : (c + 1) * span]
            target = downs_ref.at[c, hop * units : (hop + 1) * units]
            passed = downs_ref.at[c, units : 2 * units]
        return pltpu.make_async_remote_copy(
            src_ref=passed if hop == 2 else own,
            dst_ref=target,
            send_sem=weight_send.at[min(i, 2), hop],
            recv_sem=weight_recv.at[min(i, 2) if hop == 0 else i, hop],
            device_id={"tp": across if hop == 1 else beside},
            device_id_type=MESH,
        )

    for i in range(2 + pieces):
        weight_copy(i, 1).start()

    lanes = pl.ds(first_row, row_count)
    expert = lax.broadcasted_iota(jnp.int32, (n, row_count), 0)
    hits = jnp.zeros((n, row_count), F32)
    shares = jnp.zeros((n, row_count), F32)
    for k in range(TOPK):
        chosen = routes_ref[k : k + 1, lanes] == expert
        hits = jnp.where(chosen, 1.0, hits)
        shares = jnp.where(chosen, mix_ref[k : k + 1], shares)
    before = lax.broadcasted_iota(jnp.int32, (row_count, row_count), 0)
    after = lax.broadcasted_iota(jnp.int32, (row_count, row_count), 1)
    earlier = (before < after).astype(BF16)
    ranks = jnp.dot(hits.astype(BF16), earlier, preferred_element_type=F32)
    meta_ref[0] = jnp.where(hits > 0.0, ranks, -1.0)
    meta_ref[1] = shares
    slot = lax.broadcasted_iota(jnp.int32, (slot_count, row_count), 0).astype(F32)

    def selection(ref, first, count, weighted):
        parts = []
        for j in range(count):
            match = slot == ref[0, pl.ds(first + j, 1)]
            parts.append(jnp.where(match, ref[1, pl.ds(first + j, 1)] if weighted else 1.0, 0.0))
        return jnp.concatenate(parts, axis=0)

    def split(weights):
        high = weights.astype(BF16)
        return high, (weights - high.astype(F32)).astype(BF16)

    loads[0].wait()
    rows_wide = resid_ref[...].astype(F32)
    mean_square = jnp.mean(rows_wide * rows_wide, axis=-1, keepdims=True)
    rows_ref[...] = (rows_wide * lax.rsqrt(mean_square + EPS) * gain_ref[...]).astype(BF16)

    def rows_copy(i):
        return pltpu.make_async_remote_copy(
            src_ref=(rows_ref, meta_ref)[i],
            dst_ref=(rows_in, meta_in)[i],
            send_sem=rows_sem.at[0, i],
            recv_sem=rows_sem.at[1, i],
            device_id={"ep": partner},
            device_id_type=MESH,
        )

    @when_end
    def _():
        rows_copy(1).start()
        rows_copy(0).start()

    chooser_ref[...] = selection(meta_ref, 0, n, False).astype(BF16)
    for g in range(slot_total // row_count):
        at = slice(g * row_count, (g + 1) * row_count)
        slots_ref[at] = jnp.dot(
            chooser_ref[at], rows_ref[...], preferred_element_type=F32
        ).astype(BF16)

    def block(ref, index):
        return ref.at[pl.ds(pl.multiple_of(index * slot_count, slot_count), slot_count)]

    def slot_copy(target, far):
        return pltpu.make_async_remote_copy(
            src_ref=block(slots_ref, target),
            dst_ref=block(arrived_ref, me),
            send_sem=slot_send,
            recv_sem=slot_recv.at[far],
            device_id={"ep": target},
            device_id_type=MESH,
        )

    def settle(ref, semaphore):
        return pltpu.make_async_remote_copy(
            src_ref=ref,
            dst_ref=ref,
            send_sem=semaphore,
            recv_sem=semaphore,
            device_id={"ep": partner},
            device_id_type=MESH,
        )

    def back_copy(c, target, far):
        return pltpu.make_async_remote_copy(
            src_ref=block(leaving_ref.at[c], target),
            dst_ref=block(returned_ref.at[c], me),
            send_sem=back_send,
            recv_sem=back_recv.at[c, far],
            device_id={"ep": target},
            device_id_type=MESH,
        )

    def each_peer(act):
        def one(step, carry):
            act(lax.rem(me + step, n))
            return carry

        lax.fori_loop(1, n, one, 0)

    def each_near(act):
        def one(step, carry):
            act(base + lax.rem(me - base + step, half))
            return carry

        lax.fori_loop(1, half, one, 0)

    def each_far(act):
        def one(step, carry):
            act(other + lax.rem(me - base + step, half))
            return carry

        lax.fori_loop(0, half, one, 0)

    when_middle(lambda: each_far(lambda peer: slot_copy(peer, 1).start()))
    each_near(lambda peer: slot_copy(peer, 0).start())
    for i in range(2 + pieces):
        weight_copy(i, 0).start()
    here = pl.ds(pl.multiple_of(me * slot_count, slot_count), slot_count)
    arrived_ref[here] = slots_ref[here]
    for h in range(2):
        blend_ref[h, 0], blend_ref[h, 1] = split(selection(meta_ref, h * half, half, True).T)

    for load in loads[1:6]:
        load.wait()
    rows = lax.broadcasted_iota(jnp.int32, (CHUNK, CHUNK), 0)
    cols = lax.broadcasted_iota(jnp.int32, (CHUNK, CHUNK), 1)

    def local(c, carry):
        at = pl.ds(pl.multiple_of(c * CHUNK, CHUNK), CHUNK)
        for h in range(heads):
            lanes = slice(h * channels, (h + 1) * channels)
            queries = q_ref[at, lanes].astype(F32)
            feature = queries / (1.0 + jnp.exp(-queries))
            value_rows = v_ref[at, lanes]
            extra = jnp.broadcast_to(extra_ref[h : h + 1, at], (channels, CHUNK)).T
            scores = jnp.zeros((CHUNK, CHUNK), F32)
            for way, (logit_ref, bound_ref) in enumerate(((ff_ref, lbf_ref), (fb_ref, lbb_ref))):
                key, decay = gates(logit_ref[at, lanes].astype(F32), bound_ref[:, lanes], extra)
                order = (rows <= cols) if way else (rows >= cols)
                total = jnp.dot(
                    order.astype(F32),
                    decay,
                    preferred_element_type=F32,
                    precision=lax.Precision.HIGHEST,
                )
                edge = total[0:1] if way else total[CHUNK - 1 : CHUNK]
                scores = scores + chunk_scores(feature, key, total, way == 1, rows, cols)
                reach_ref[way, h, c] = (feature * jnp.exp(total)).astype(BF16)
                faded = (key * jnp.exp(edge - total)).astype(BF16)
                part_ref[way, h, c] = lax.dot_general(
                    value_rows, faded, (((0,), (0,)), ((), ())), preferred_element_type=F32
                )
                fade_ref[way, h, c] = jnp.broadcast_to(jnp.exp(edge), (8, channels))
            local_ref[h, c] = jnp.dot(
                scores.astype(BF16), value_rows, preferred_element_type=F32
            )
        return carry

    lax.fori_loop(0, chunks, local, 0)
    for way in range(2):
        for h in range(heads):
            state = jnp.zeros(part_ref.shape[3:], F32)
            fade = jnp.ones((1, channels), F32)
            for c in range(chunks)[:: -1 if way else 1]:
                step = fade_ref[way, h, c, 0:1]
                state = state * step + part_ref[way, h, c]
                fade = fade * step
            state_out[way, h, : state.shape[0]] = state.astype(BF16)
            state_out[way, h, state.shape[0] :] = jnp.broadcast_to(
                fade, (DECAY_ROWS, channels)
            ).astype(BF16)

    def state_copy(target):
        way = jnp.where(target > me, 0, 1)
        return pltpu.make_async_remote_copy(
            src_ref=state_out.at[way],
            dst_ref=state_in.at[me],
            send_sem=state_send,
            recv_sem=state_recv,
            device_id={"ep": target},
            device_id_type=MESH,
        )

    each_peer(lambda peer: state_copy(peer).start())

    def pass_copy(target):
        return pltpu.make_async_remote_copy(
            src_ref=block(passed_ref, target - base),
            dst_ref=block(arrived_ref, partner),
            send_sem=pass_send,
            recv_sem=slot_recv.at[1],
            device_id={"ep": target},
            device_id_type=MESH,
        )

    @when_passing
    def _():
        rows_copy(1).wait_recv()
        rows_copy(0).wait_recv()
        chosen = selection(meta_in, base, half, False).astype(BF16)
        passed_ref[...] = jnp.dot(chosen, rows_in[...], preferred_element_type=F32).astype(BF16)
        each_near(lambda peer: pass_copy(peer).start())
        arrived_ref[pl.ds(pl.multiple_of(partner * slot_count, slot_count), slot_count)] = (
            passed_ref[pl.ds(pl.multiple_of((me - base) * slot_count, slot_count), slot_count)]
        )
        merge_blend[0], merge_blend[1] = split(selection(meta_in, base, half, True).T)

    near_rows = pl.ds(pl.multiple_of(base * slot_count, side), side)
    far_rows = pl.ds(pl.multiple_of(other * slot_count, side), side)

    def open_gate(i, at):
        gated = jnp.dot(arrived_ref[at], gates_ref[i], preferred_element_type=F32)
        gated_ref[at, i * units : (i + 1) * units] = gated / (1.0 + jnp.exp(-gated))

    def activate(i, at):
        lifted = jnp.dot(arrived_ref[at], ups_ref[i], preferred_element_type=F32)
        columns = slice(i * units, (i + 1) * units)
        active_ref[at, columns] = (gated_ref[at, columns] * lifted).astype(BF16)

    for load in loads[6:]:
        load.wait()
    settle(downs_ref.at[:, 3 * units : 4 * units], load_sem.at[9]).wait_recv()
    weight_copy(0, 0).wait_recv()
    weight_copy(1, 0).wait_recv()
    settle(downs_ref.at[:, :units], weight_recv.at[2, 0]).wait_recv()
    settle(arrived_ref.at[: (half - 1) * slot_count], slot_recv.at[0]).wait_recv()
    for i in (3, 0):
        open_gate(i, near_rows)
        activate(i, near_rows)
    weight_copy(0, 1).wait_recv()
    weight_copy(0, 2).start()
    open_gate(1, near_rows)
    weight_copy(0, 2).wait_recv()
    open_gate(2, near_rows)

    @when_end
    def _():
        settle(arrived_ref.at[: half * slot_count], slot_recv.at[1]).wait_recv()

    @when_middle
    def _():
        blocks = half - 1 if relayed else half
        settle(arrived_ref.at[: blocks * slot_count], slot_recv.at[1]).wait_recv()

    for i in (3, 0):
        open_gate(i, far_rows)
        activate(i, far_rows)
    open_gate(1, far_rows)
    open_gate(2, far_rows)
    weight_copy(1, 1).wait_recv()
    weight_copy(1, 2).start()
    activate(1, slice(None))
    weight_copy(1, 2).wait_recv()
    activate(2, slice(None))

    mine = pl.ds(pl.multiple_of((me - base) * slot_count, slot_count), slot_count)

    def merge_copy(c, dest):
        return pltpu.make_async_remote_copy(
            src_ref=block(leaving_ref.at[c], dest),
            dst_ref=block(merge_in.at[c], me - base),
            send_sem=back_send,
            recv_sem=merge_recv.at[c],
            device_id={"ep": lax.rem(dest + half, n)},
            device_id_type=MESH,
        )

    def ends(peer):
        return (peer // 2 == 0) | (peer // 2 == n // 2 - 1)

    def merged_copy(c):
        return pltpu.make_async_remote_copy(
            src_ref=merged_ref.at[c],
            dst_ref=merged_in.at[c],
            send_sem=merged_send,
            recv_sem=merged_recv.at[c],
            device_id={"ep": partner},
            device_id_type=MESH,
        )

    def blended(weights, values):
        total = jnp.dot(weights[0], values, preferred_element_type=F32)
        return total + jnp.dot(weights[1], values, preferred_element_type=F32)

    def merge(c):
        @when_passing
        def _():
            settle(merge_in.at[c, : (half - 1) * slot_count], merge_recv.at[c]).wait_recv()
            merged_ref[c] = blended(merge_blend, merge_in[c]).astype(BF16)
            merged_copy(c).start()

    def results(c):
        weight_copy(2 + c, 1).wait_recv()
        weight_copy(2 + c, 2).start()
        weight_copy(2 + c, 2).wait_recv()
        leaving_ref[c] = jnp.dot(
            active_ref[...], downs_ref[c], preferred_element_type=F32
        ).astype(BF16)

        @when_passing
        def _():
            merge_in[c, mine] = leaving_ref[
                c, pl.ds(pl.multiple_of(partner * slot_count, slot_count), slot_count)
            ]

        if relayed:

            @each_far
            def _(peer):
                pl.when(ends(peer) & (peer != partner))(lambda: merge_copy(c, peer).start())

    def direct(c):
        @each_far
        def _(peer):
            if relayed:
                pl.when(jnp.logical_not(ends(peer)))(lambda: back_copy(c, peer, 1).start())
            else:
                back_copy(c, peer, 1).start()

        each_near(lambda peer: back_copy(c, peer, 0).start())
        returned_ref[c, here] = leaving_ref[c, here]

    def collect(c):
        settle(returned_ref.at[c, : (half - 1) * slot_count], back_recv.at[c, 0]).wait_recv()
        total_ref[...] = blended(blend_ref.at[base // half], returned_ref[c, near_rows])

        @when_middle
        def _():
            settle(returned_ref.at[c, : half * slot_count], back_recv.at[c, 1]).wait_recv()
            total_ref[...] += blended(blend_ref.at[other // half], returned_ref[c, far_rows])

        @when_end
        def _():
            merged_copy(c).wait_recv()
            total_ref[...] += merged_in[c].astype(F32)

        routed_ref[:, c * span : (c + 1) * span] = total_ref[...].astype(BF16)

    def finish_mixer():
        settle(state_in.at[: n - 1], state_recv).wait_recv()
        depth = part_ref.shape[3]
        for h in range(heads):
            for way in range(2):

                def one(hop, state, way=way, h=h):
                    source = n - 1 - hop if way else hop
                    step = state_in[source, h, depth : depth + DECAY_ROWS].astype(F32)[0:1]
                    return state * step + state_in[source, h, :depth].astype(F32)

                ahead = n - 1 - me if way else me
                state = lax.fori_loop(0, ahead, one, jnp.zeros(part_ref.shape[3:], F32))
                for c in range(chunks)[:: -1 if way else 1]:
                    local_ref[h, c] += dot_rows(reach_ref[way, h, c], state.astype(BF16))
                    state = state * fade_ref[way, h, c, 0:1] + part_ref[way, h, c]
            lanes = slice(h * channels, (h + 1) * channels)
            for c in range(chunks):
                at = slice(c * CHUNK, (c + 1) * CHUNK)
                combined = local_ref[h, c]
                mean_square = jnp.mean(combined * combined, axis=-1, keepdims=True)
                gate = og_ref[at, lanes].astype(F32)
                opened = combined * lax.rsqrt(mean_square + EPS) * scale_ref[:, lanes]
                hidden_ref[at, lanes] = (opened * (gate / (1.0 + jnp.exp(-gate)))).astype(BF16)

    diagonal = lax.rem(beside + quarters // 2, quarters)

    def piece_copy(i):
        return pltpu.make_async_remote_copy(
            src_ref=(partial_ref.at[0], partial_ref.at[1], summed_ref)[i],
            dst_ref=pieces_ref.at[i],
            send_sem=piece_send.at[i],
            recv_sem=piece_recv.at[i],
            device_id={"tp": across if i == 2 else beside},
            device_id_type=MESH,
        )

    def project():
        for i, part in enumerate((diagonal, beside, across, place)):
            at = pl.ds(pl.multiple_of(part * row_count, row_count), row_count)
            partial_ref[i] = jnp.dot(
                hidden_ref[at], proj_ref[...], preferred_element_type=F32
            ).astype(BF16)
            if i < 2:
                piece_copy(i).start()

    def cross():
        piece_copy(0).wait_recv()
        summed_ref[...] = (partial_ref[2].astype(F32) + pieces_ref[0].astype(F32)).astype(BF16)
        piece_copy(2).start()

    def gather_mixed():
        piece_copy(1).wait_recv()
        piece_copy(2).wait_recv()
        total = partial_ref[3].astype(F32) + pieces_ref[1].astype(F32)
        mixed_ref[...] = (total + pieces_ref[2].astype(F32)).astype(BF16)

    results(0)
    direct(0)
    results(1)
    finish_mixer()
    for c in range(2, pieces):
        results(c)
        merge(c - 2)
        direct(c - 1)
        if c == 2:
            project()
        if c == 3:
            cross()
    collect(0)
    collect(1)
    merge(pieces - 2)
    collect(2)
    merge(pieces - 1)
    direct(pieces - 1)
    for c in range(3, pieces - 1):
        collect(c)
    gather_mixed()
    collect(pieces - 1)

    @when_end
    def _():
        rows_copy(0).wait_send()
        rows_copy(1).wait_send()
        settle(slots_ref.at[: (half - 1) * slot_count], slot_send).wait_send()
        settle(leaving_ref.at[:, : (n - 1) * slot_count], back_send).wait_send()

    @when_middle
    def _():
        blocks = n - 2 if relayed else n - 1
        settle(slots_ref.at[: (n - 1) * slot_count], slot_send).wait_send()
        settle(leaving_ref.at[:, : blocks * slot_count], back_send).wait_send()

    @when_passing
    def _():
        settle(passed_ref.at[: (half - 1) * slot_count], pass_send).wait_send()
        settle(merged_ref, merged_send).wait_send()

    settle(state_in.at[: n - 1], state_send).wait_send()
    for i in range(3):
        piece_copy(i).wait_send()
    for hop in range(3):
        settle(gates_ref.at[0], weight_send.at[0, hop]).wait_send()
        settle(ups_ref.at[0], weight_send.at[1, hop]).wait_send()
        settle(downs_ref.at[:, :units], weight_send.at[2, hop]).wait_send()


def shards(
    queries,
    forget_forward_logits,
    forget_backward_logits,
    values,
    output_gate_logits,
    lower_bound_forward,
    lower_bound_backward,
    extra_log_decay,
    head_norm_scale,
    output_projection,
    second_residual,
    expert_norm_scale,
    routes,
    specialist_mixing_factor,
    expert_gate_matrix,
    expert_up_matrix,
    expert_down_matrix,
):
    group_rows, width_model = second_residual.shape
    quarters = lax.axis_size("tp")
    n = lax.axis_size("ep")
    row_count = group_rows // quarters
    slot_count = 2 * TOPK * row_count // n
    slot_total = n * slot_count
    width = queries.shape[1]
    heads = extra_log_decay.shape[1]
    channels = width // heads
    depth = values.shape[1] // heads
    chunks = group_rows // CHUNK
    units = expert_down_matrix.shape[1]
    span = width_model // PIECES
    vmem = pl.BlockSpec(memory_space=pltpu.VMEM)
    anywhere = pl.BlockSpec(memory_space=pl.ANY)
    state = (heads, depth + DECAY_ROWS, channels)
    block = (group_rows, width)
    out = jax.ShapeDtypeStruct((row_count, width_model), BF16)
    dma = pltpu.SemaphoreType.DMA
    return pl.pallas_call(
        functools.partial(fused_kernel, n, quarters),
        out_shape=(out, out),
        in_specs=[anywhere] * 5
        + [vmem] * 4
        + [anywhere] * 2
        + [vmem] * 3
        + [anywhere] * 3,
        out_specs=(vmem, vmem),
        scratch_shapes=[pltpu.VMEM(block, BF16)] * 5
        + [
            pltpu.VMEM((width, width_model), BF16),
            pltpu.VMEM((row_count, width_model), BF16),
            pltpu.VMEM((2, n, row_count), F32),
            pltpu.VMEM((2, n, row_count), F32),
            pltpu.VMEM((row_count, width_model), BF16),
            pltpu.VMEM((row_count, width_model), BF16),
            pltpu.VMEM((slot_total, row_count), BF16),
            pltpu.VMEM((2, 2, row_count, slot_total // 2), BF16),
            pltpu.VMEM((2, row_count, slot_total // 2), BF16),
            pltpu.VMEM((slot_total, width_model), BF16),
            pltpu.VMEM((slot_total, width_model), BF16),
            pltpu.VMEM((slot_total // 2, width_model), BF16),
            pltpu.VMEM((quarters,) + expert_gate_matrix.shape[1:], BF16),
            pltpu.VMEM((quarters,) + expert_up_matrix.shape[1:], BF16),
            pltpu.VMEM((PIECES, quarters * units, span), BF16),
            pltpu.VMEM((slot_total, quarters * units), F32),
            pltpu.VMEM((slot_total, quarters * units), BF16),
            pltpu.VMEM((PIECES, slot_total, span), BF16),
            pltpu.VMEM((PIECES, slot_total, span), BF16),
            pltpu.VMEM((PIECES, slot_total // 2, span), BF16),
            pltpu.VMEM((PIECES, row_count, span), BF16),
            pltpu.VMEM((PIECES, row_count, span), BF16),
            pltpu.VMEM((row_count, span), F32),
            pltpu.VMEM((heads, chunks, CHUNK, depth), F32),
            pltpu.VMEM((2, heads, chunks, CHUNK, channels), BF16),
            pltpu.VMEM((2, heads, chunks, depth, channels), F32),
            pltpu.VMEM((2, heads, chunks, 8, channels), F32),
            pltpu.VMEM((2,) + state, BF16),
            pltpu.VMEM((n,) + state, BF16),
            pltpu.VMEM(block, BF16),
            pltpu.VMEM((4, row_count, width_model), BF16),
            pltpu.VMEM((row_count, width_model), BF16),
            pltpu.VMEM((3, row_count, width_model), BF16),
            dma((10,)),
            dma((2, 2)),
            dma(()),
            dma((PIECES,)),
            dma(()),
            dma((PIECES,)),
            dma(()),
            dma((2,)),
            dma(()),
            dma(()),
            dma((3, 3)),
            dma((2 + PIECES, 3)),
            dma(()),
            dma((PIECES, 2)),
            dma((3,)),
            dma((3,)),
        ],
        compiler_params=pltpu.CompilerParams(
            collective_id=0, has_side_effects=True, vmem_limit_bytes=48 * 2**20
        ),
        cost_estimate=pl.CostEstimate(
            flops=4 * 10**10, bytes_accessed=30 * 2**20, transcendentals=0
        ),
        name="mix_and_route",
    )(
        *(
            pltpu.with_memory_space_constraint(operand, pltpu.HBM)
            for operand in (
                queries,
                forget_forward_logits,
                forget_backward_logits,
                values,
                output_gate_logits,
                lower_bound_forward.reshape(1, -1),
                lower_bound_backward.reshape(1, -1),
                extra_log_decay.T,
                head_norm_scale.reshape(1, -1),
                output_projection,
                second_residual,
                expert_norm_scale.reshape(1, -1),
                routes.T,
                specialist_mixing_factor.T,
                expert_gate_matrix,
                expert_up_matrix,
                expert_down_matrix,
            )
        )
    )


def solution(mesh):
    in_specs = (
        P("ep", "tp"),
        P("ep", "tp"),
        P("ep", "tp"),
        P("ep", "tp"),
        P("ep", "tp"),
        P("tp"),
        P("tp"),
        P("ep", "tp"),
        P("tp"),
        P("tp", None),
        P("ep", None),
        P(),
        P("ep", None),
        P(("ep", "tp"), None),
        P("ep", None, "tp"),
        P("ep", None, "tp"),
        P("ep", "tp", None),
    )
    out_specs = (P(("ep", "tp"), None), P(("ep", "tp"), None))
    return jax.shard_map(shards, mesh=mesh, in_specs=in_specs, out_specs=out_specs, check_vma=False)
```

```python
import functools

import jax
import jax.numpy as jnp
from jax import lax
from jax.experimental import pallas as pl
from jax.experimental.pallas import tpu as pltpu
from jax.sharding import PartitionSpec as P

TOPK = 2
CHUNK = 128
LEAF = 16
DECAY_ROWS = 16
SPANS = 16
PIECES = SPANS // 2 + 1
PLANES = 4
EPS = 1e-06
MESH = pl.DeviceIdType.MESH
F32 = jnp.float32
BF16 = jnp.bfloat16


def neighbours():
    place, count = lax.axis_index("tp"), lax.axis_size("tp")
    return place + 1 - 2 * lax.rem(place, 2), lax.rem(place + count // 2, count)


def greet(axis, n):
    me = lax.axis_index(axis)
    barrier = pltpu.get_barrier_semaphore()

    def one(step, carry):
        peer = lax.rem(me + step, n)
        pl.semaphore_signal(barrier, inc=1, device_id={axis: peer}, device_id_type=MESH)
        return carry

    lax.fori_loop(1, n, one, 0)


def dot_rows(a, b):
    return lax.dot_general(a, b, (((1,), (1,)), ((), ())), preferred_element_type=F32)


def gates(logits, bound, extra):
    shrink = jnp.exp(-logits)
    opened = 1.0 / (1.0 + shrink)
    floor_part = 1.0 / (1.0 + jnp.exp(-bound))
    complement = 1.0 / (1.0 + jnp.exp(bound))
    decay = jnp.log(floor_part + complement * opened) + extra
    return complement * (shrink * opened), decay


def referenced(total, size, place):
    blocks = total.reshape(CHUNK // size, size, total.shape[-1])
    anchor = jnp.broadcast_to(blocks[:, place : place + 1, :], blocks.shape)
    return total - anchor.reshape(total.shape)


def chunk_scores(feature, key, total, backward, rows, cols):
    scores = jnp.zeros((CHUNK, CHUNK), F32)
    size = CHUNK
    while size > LEAF:
        half = size // 2
        reach = jnp.exp(-jnp.abs(referenced(total, size, half if backward else half - 1)))
        part = dot_rows((feature * reach).astype(BF16), (key * reach).astype(BF16))
        late, early = (cols, rows) if backward else (rows, cols)
        mask = (rows // size == cols // size) & (late % size >= half) & (early % size < half)
        scores = scores + jnp.where(mask, part, 0.0)
        size = half
    spread = referenced(total, LEAF, LEAF // 2 if backward else LEAF // 2 - 1)
    part = dot_rows(
        (feature * jnp.exp(spread)).astype(BF16), (key * jnp.exp(-spread)).astype(BF16)
    )
    mask = (rows // LEAF == cols // LEAF) & ((rows <= cols) if backward else (rows >= cols))
    return scores + jnp.where(mask, part, 0.0)


def fused_kernel(
    n,
    quarters,
    q_any,
    ff_any,
    fb_any,
    v_any,
    og_any,
    lbf_ref,
    lbb_ref,
    extra_ref,
    scale_ref,
    proj_any,
    resid_any,
    gain_ref,
    routes_ref,
    mix_ref,
    gate_any,
    up_any,
    down_any,
    mixed_ref,
    routed_ref,
    q_ref,
    ff_ref,
    fb_ref,
    v_ref,
    og_ref,
    proj_ref,
    resid_ref,
    meta_ref,
    meta_in,
    rows_ref,
    rows_in,
    chooser_ref,
    blend_ref,
    merge_blend,
    slots_ref,
    arrived_ref,
    passed_ref,
    gates_ref,
    ups_ref,
    downs_ref_narrow,
    downs_ref_wide,
    gated_ref,
    active_ref,
    lifted_ref,
    leaving_ref_narrow,
    leaving_ref_wide,
    returned_ref_narrow,
    returned_ref_wide,
    merge_in_narrow,
    merge_in_wide,
    merged_ref_narrow,
    merged_ref_wide,
    merged_in_narrow,
    merged_in_wide,
    total_ref,
    local_ref,
    reach_ref,
    part_ref,
    fade_ref,
    state_out,
    state_in,
    hidden_ref,
    partial_ref,
    summed_ref,
    pieces_ref,
    load_sem,
    rows_sem,
    pass_send,
    merge_recv,
    merged_send,
    merged_recv,
    slot_send,
    slot_recv,
    state_send,
    state_recv,
    weight_send,
    weight_recv,
    far_send,
    near_send,
    back_recv,
    piece_send,
    piece_recv,
):
    me = lax.axis_index("ep")
    place = lax.axis_index("tp")
    group_rows, width = q_ref.shape
    row_count, width_model = resid_ref.shape
    chunks = group_rows // CHUNK
    heads = extra_ref.shape[0]
    channels = width // heads
    slot_total = slots_ref.shape[0]
    slot_count = slot_total // n
    units = down_any.shape[1]
    depth_half = width_model // 2

    pieces, span = PIECES, width_model // SPANS

    def piece(refs, c):
        narrow, wide = refs
        return narrow.at[c // (pieces - 1)] if is_narrow(c) else wide.at[c - 1]

    def is_narrow(c):
        return c in (0, pieces - 1)

    def far_group(c):
        return 1 if is_narrow(c) else 2 if c == pieces - 2 else 0

    def columns(c):
        first = max(0, (2 * c - 1) * span)
        return slice(first, first + (span if is_narrow(c) else 2 * span))

    downs_refs = downs_ref_narrow, downs_ref_wide
    leaving_refs = leaving_ref_narrow, leaving_ref_wide
    returned_refs = returned_ref_narrow, returned_ref_wide
    merge_refs = merge_in_narrow, merge_in_wide
    merged_refs = merged_ref_narrow, merged_ref_wide
    merged_in_refs = merged_in_narrow, merged_in_wide
    beside, across = neighbours()

    half = n // 2
    side = half * slot_count
    relayed = half == PLANES
    base = me // half * half
    other = half - base
    partner = lax.rem(me + half, n)
    plane = me // 2
    at_end = (plane == 0) | (plane == n // 2 - 1)

    def when_end(act):
        if relayed:
            pl.when(at_end)(act)

    def when_middle(act):
        if relayed:
            pl.when(jnp.logical_not(at_end))(act)
        else:
            act()

    def when_passing(act):
        if relayed:
            pl.when(jnp.logical_not(at_end))(act)

    greet("ep", n)
    greet("tp", quarters)
    first_row = pl.multiple_of(place * row_count, row_count)
    loads = [
        pltpu.make_async_copy(source, target, load_sem.at[i])
        for i, (source, target) in enumerate(
            (
                (gate_any.at[0], gates_ref.at[3]),
                (up_any.at[0], ups_ref.at[3]),
                (resid_any.at[pl.ds(first_row, row_count)], resid_ref),
                (q_any, q_ref),
                (ff_any, ff_ref),
                (fb_any, fb_ref),
                (v_any, v_ref),
                (og_any, og_ref),
                (proj_any, proj_ref),
            )
        )
    ]
    down_loads = [
        pltpu.make_async_copy(
            down_any.at[0, :, columns(c)],
            piece(downs_refs, c).at[3 * units : 4 * units],
            load_sem.at[9 if is_narrow(c) else 10],
        )
        for c in range(pieces)
    ]
    for load in loads[:2] + down_loads + loads[2:]:
        load.start()

    pl.semaphore_wait(pltpu.get_barrier_semaphore(), n + quarters - 2)

    def weight_copy(i, hop):
        kind = min(i, 1)
        if i == 0:
            held = lambda slot: gates_ref.at[slot]
        elif i < 3:
            at = slice((i - 1) * depth_half, i * depth_half)
            held = lambda slot: ups_ref.at[slot, at]
        else:
            kind = 2 if is_narrow(i - 3) else 3
            held = lambda slot: piece(downs_refs, i - 3).at[slot * units : (slot + 1) * units]
        return pltpu.make_async_remote_copy(
            src_ref=held(1 if hop == 2 else 3),
            dst_ref=held(hop),
            send_sem=weight_send.at[kind, hop],
            recv_sem=weight_recv.at[kind if hop == 0 else i, hop],
            device_id={"tp": across if hop == 1 else beside},
            device_id_type=MESH,
        )

    loads[0].wait()
    weight_copy(0, 1).start()
    loads[1].wait()
    for i in (1, 2):
        weight_copy(i, 1).start()
    for kind in range(2):
        own_part = downs_refs[kind].at[:, 3 * units : 4 * units]
        pltpu.make_async_copy(own_part, own_part, load_sem.at[9 + kind]).wait()
    for c in range(pieces):
        weight_copy(3 + c, 1).start()

    lanes = pl.ds(first_row, row_count)
    expert = lax.broadcasted_iota(jnp.int32, (n, row_count), 0)
    hits = jnp.zeros((n, row_count), F32)
    shares = jnp.zeros((n, row_count), F32)
    for k in range(TOPK):
        chosen = routes_ref[k : k + 1, lanes] == expert
        hits = jnp.where(chosen, 1.0, hits)
        shares = jnp.where(chosen, mix_ref[k : k + 1], shares)
    before = lax.broadcasted_iota(jnp.int32, (row_count, row_count), 0)
    after = lax.broadcasted_iota(jnp.int32, (row_count, row_count), 1)
    earlier = (before < after).astype(BF16)
    ranks = jnp.dot(hits.astype(BF16), earlier, preferred_element_type=F32)
    meta_ref[0] = jnp.where(hits > 0.0, ranks, -1.0)
    meta_ref[1] = shares
    slot = lax.broadcasted_iota(jnp.int32, (slot_count, row_count), 0).astype(F32)

    def selection(ref, first, count, weighted):
        parts = []
        for j in range(count):
            match = slot == ref[0, pl.ds(first + j, 1)]
            parts.append(jnp.where(match, ref[1, pl.ds(first + j, 1)] if weighted else 1.0, 0.0))
        return jnp.concatenate(parts, axis=0)

    def split(weights):
        high = weights.astype(BF16)
        return high, (weights - high.astype(F32)).astype(BF16)

    loads[2].wait()
    rows_wide = resid_ref[...].astype(F32)
    mean_square = jnp.mean(rows_wide * rows_wide, axis=-1, keepdims=True)
    rows_ref[...] = (rows_wide * lax.rsqrt(mean_square + EPS) * gain_ref[...]).astype(BF16)

    def rows_copy(i):
        return pltpu.make_async_remote_copy(
            src_ref=(rows_ref, meta_ref)[i],
            dst_ref=(rows_in, meta_in)[i],
            send_sem=rows_sem.at[0, i],
            recv_sem=rows_sem.at[1, i],
            device_id={"ep": partner},
            device_id_type=MESH,
        )

    @when_end
    def _():
        rows_copy(1).start()
        rows_copy(0).start()

    chooser_ref[...] = selection(meta_ref, 0, n, False).astype(BF16)
    for g in range(slot_total // row_count):
        at = slice(g * row_count, (g + 1) * row_count)
        slots_ref[at] = jnp.dot(
            chooser_ref[at], rows_ref[...], preferred_element_type=F32
        ).astype(BF16)

    def block(ref, index):
        return ref.at[pl.ds(pl.multiple_of(index * slot_count, slot_count), slot_count)]

    def slot_copy(target, far):
        return pltpu.make_async_remote_copy(
            src_ref=block(slots_ref, target),
            dst_ref=block(arrived_ref, me),
            send_sem=slot_send,
            recv_sem=slot_recv.at[far],
            device_id={"ep": target},
            device_id_type=MESH,
        )

    def settle(ref, semaphore):
        return pltpu.make_async_remote_copy(
            src_ref=ref,
            dst_ref=ref,
            send_sem=semaphore,
            recv_sem=semaphore,
            device_id={"ep": partner},
            device_id_type=MESH,
        )

    def back_copy(c, target, far):
        return pltpu.make_async_remote_copy(
            src_ref=block(piece(leaving_refs, c), target),
            dst_ref=block(piece(returned_refs, c), me),
            send_sem=far_send.at[far_group(c)] if far else near_send.at[int(is_narrow(c))],
            recv_sem=back_recv.at[c, far],
            device_id={"ep": target},
            device_id_type=MESH,
        )

    def each_peer(act):
        def one(step, carry):
            act(lax.rem(me + step, n))
            return carry

        lax.fori_loop(1, n, one, 0)

    def each_near(act):
        def one(step, carry):
            act(base + lax.rem(me - base + step, half))
            return carry

        lax.fori_loop(1, half, one, 0)

    def each_far(act):
        def one(step, carry):
            act(other + lax.rem(me - base + step, half))
            return carry

        lax.fori_loop(0, half, one, 0)

    when_middle(lambda: each_far(lambda peer: slot_copy(peer, 1).start()))
    each_near(lambda peer: slot_copy(peer, 0).start())
    for i in range(3 + pieces):
        weight_copy(i, 0).start()
    here = pl.ds(pl.multiple_of(me * slot_count, slot_count), slot_count)
    arrived_ref[here] = slots_ref[here]
    for h in range(2):
        blend_ref[h, 0], blend_ref[h, 1] = split(selection(meta_ref, h * half, half, True).T)

    for load in loads[3:]:
        load.wait()
    rows = lax.broadcasted_iota(jnp.int32, (CHUNK, CHUNK), 0)
    cols = lax.broadcasted_iota(jnp.int32, (CHUNK, CHUNK), 1)

    def local(c, carry):
        at = pl.ds(pl.multiple_of(c * CHUNK, CHUNK), CHUNK)
        for h in range(heads):
            lanes = slice(h * channels, (h + 1) * channels)
            queries = q_ref[at, lanes].astype(F32)
            feature = queries / (1.0 + jnp.exp(-queries))
            value_rows = v_ref[at, lanes]
            extra = jnp.broadcast_to(extra_ref[h : h + 1, at], (channels, CHUNK)).T
            scores = jnp.zeros((CHUNK, CHUNK), F32)
            for way, (logit_ref, bound_ref) in enumerate(((ff_ref, lbf_ref), (fb_ref, lbb_ref))):
                key, decay = gates(logit_ref[at, lanes].astype(F32), bound_ref[:, lanes], extra)
                order = (rows <= cols) if way else (rows >= cols)
                total = jnp.dot(
                    order.astype(F32),
                    decay,
                    preferred_element_type=F32,
                    precision=lax.Precision.HIGHEST,
                )
                edge = total[0:1] if way else total[CHUNK - 1 : CHUNK]
                scores = scores + chunk_scores(feature, key, total, way == 1, rows, cols)
                reach_ref[way, h, c] = (feature * jnp.exp(total)).astype(BF16)
                faded = (key * jnp.exp(edge - total)).astype(BF16)
                part_ref[way, h, c] = lax.dot_general(
                    value_rows, faded, (((0,), (0,)), ((), ())), preferred_element_type=F32
                )
                fade_ref[way, h, c] = jnp.broadcast_to(jnp.exp(edge), (8, channels))
            local_ref[h, c] = jnp.dot(
                scores.astype(BF16), value_rows, preferred_element_type=F32
            )
        return carry

    lax.fori_loop(0, chunks, local, 0)
    for way in range(2):
        for h in range(heads):
            state = jnp.zeros(part_ref.shape[3:], F32)
            fade = jnp.ones((1, channels), F32)
            for c in range(chunks)[:: -1 if way else 1]:
                step = fade_ref[way, h, c, 0:1]
                state = state * step + part_ref[way, h, c]
                fade = fade * step
            state_out[way, h, : state.shape[0]] = state.astype(BF16)
            state_out[way, h, state.shape[0] :] = jnp.broadcast_to(
                fade, (DECAY_ROWS, channels)
            ).astype(BF16)

    def state_copy(target):
        way = jnp.where(target > me, 0, 1)
        return pltpu.make_async_remote_copy(
            src_ref=state_out.at[way],
            dst_ref=state_in.at[me],
            send_sem=state_send,
            recv_sem=state_recv,
            device_id={"ep": target},
            device_id_type=MESH,
        )

    each_peer(lambda peer: state_copy(peer).start())

    def pass_copy(target):
        return pltpu.make_async_remote_copy(
            src_ref=block(passed_ref, target - base),
            dst_ref=block(arrived_ref, partner),
            send_sem=pass_send,
            recv_sem=slot_recv.at[1],
            device_id={"ep": target},
            device_id_type=MESH,
        )

    @when_passing
    def _():
        rows_copy(1).wait_recv()
        rows_copy(0).wait_recv()
        chosen = selection(meta_in, base, half, False).astype(BF16)
        passed_ref[...] = jnp.dot(chosen, rows_in[...], preferred_element_type=F32).astype(BF16)
        each_near(lambda peer: pass_copy(peer).start())
        arrived_ref[pl.ds(pl.multiple_of(partner * slot_count, slot_count), slot_count)] = (
            passed_ref[pl.ds(pl.multiple_of((me - base) * slot_count, slot_count), slot_count)]
        )
        merge_blend[0], merge_blend[1] = split(selection(meta_in, base, half, True).T)

    near_rows = pl.ds(pl.multiple_of(base * slot_count, side), side)
    far_rows = pl.ds(pl.multiple_of(other * slot_count, side), side)

    def open_gate(i, at):
        gated = jnp.dot(arrived_ref[at], gates_ref[i], preferred_element_type=F32)
        gated_ref[at, i * units : (i + 1) * units] = gated / (1.0 + jnp.exp(-gated))

    def lift(i, part, at):
        rows_of = slice(part * depth_half, (part + 1) * depth_half)
        return jnp.dot(arrived_ref[at, rows_of], ups_ref[i, rows_of], preferred_element_type=F32)

    def activate(i, at, lifted):
        hidden = slice(i * units, (i + 1) * units)
        active_ref[at, hidden] = (gated_ref[at, hidden] * lifted).astype(BF16)

    def activate_whole(i, at):
        activate(i, at, jnp.dot(arrived_ref[at], ups_ref[i], preferred_element_type=F32))

    def finish_mixer():
        settle(state_in.at[: n - 1], state_recv).wait_recv()
        depth = part_ref.shape[3]
        for h in range(heads):
            for way in range(2):

                def one(hop, state, way=way, h=h):
                    source = n - 1 - hop if way else hop
                    step = state_in[source, h, depth : depth + DECAY_ROWS].astype(F32)[0:1]
                    return state * step + state_in[source, h, :depth].astype(F32)

                ahead = n - 1 - me if way else me
                state = lax.fori_loop(0, ahead, one, jnp.zeros(part_ref.shape[3:], F32))
                for c in range(chunks)[:: -1 if way else 1]:
                    local_ref[h, c] += dot_rows(reach_ref[way, h, c], state.astype(BF16))
                    state = state * fade_ref[way, h, c, 0:1] + part_ref[way, h, c]
            lanes = slice(h * channels, (h + 1) * channels)
            for c in range(chunks):
                at = slice(c * CHUNK, (c + 1) * CHUNK)
                combined = local_ref[h, c]
                mean_square = jnp.mean(combined * combined, axis=-1, keepdims=True)
                gate = og_ref[at, lanes].astype(F32)
                opened = combined * lax.rsqrt(mean_square + EPS) * scale_ref[:, lanes]
                hidden_ref[at, lanes] = (opened * (gate / (1.0 + jnp.exp(-gate)))).astype(BF16)

    every = slice(None)
    for kind in range(2):
        settle(downs_refs[kind].at[:, :units], weight_recv.at[2 + kind, 0]).wait_recv()
    weight_copy(0, 0).wait_recv()
    settle(ups_ref.at[0], weight_recv.at[1, 0]).wait_recv()
    settle(arrived_ref.at[: (half - 1) * slot_count], slot_recv.at[0]).wait_recv()
    for i in (3, 0):
        open_gate(i, near_rows)
        activate_whole(i, near_rows)
    weight_copy(0, 1).wait_recv()
    weight_copy(0, 2).start()
    open_gate(1, near_rows)
    weight_copy(0, 2).wait_recv()
    open_gate(2, near_rows)
    weight_copy(1, 1).wait_recv()
    weight_copy(1, 2).start()

    @when_end
    def _():
        settle(arrived_ref.at[: half * slot_count], slot_recv.at[1]).wait_recv()

    @when_middle
    def _():
        blocks = half - 1 if relayed else half
        settle(arrived_ref.at[: blocks * slot_count], slot_recv.at[1]).wait_recv()

    for i in (3, 0):
        open_gate(i, far_rows)
        activate_whole(i, far_rows)
    open_gate(1, far_rows)
    open_gate(2, far_rows)
    lifted_ref[0] = lift(1, 0, every)
    weight_copy(1, 2).wait_recv()
    lifted_ref[1] = lift(2, 0, every)
    weight_copy(2, 1).wait_recv()
    weight_copy(2, 2).start()
    activate(1, every, lifted_ref[0] + lift(1, 1, every))
    weight_copy(3, 1).wait_recv()
    weight_copy(3, 2).start()
    weight_copy(2, 2).wait_recv()
    activate(2, every, lifted_ref[1] + lift(2, 1, every))

    mine = pl.ds(pl.multiple_of((me - base) * slot_count, slot_count), slot_count)

    def merge_copy(c, dest):
        return pltpu.make_async_remote_copy(
            src_ref=block(piece(leaving_refs, c), dest),
            dst_ref=block(piece(merge_refs, c), me - base),
            send_sem=far_send.at[far_group(c)],
            recv_sem=merge_recv.at[c],
            device_id={"ep": lax.rem(dest + half, n)},
            device_id_type=MESH,
        )

    def ends(peer):
        return (peer // 2 == 0) | (peer // 2 == n // 2 - 1)

    def merged_copy(c):
        return pltpu.make_async_remote_copy(
            src_ref=piece(merged_refs, c),
            dst_ref=piece(merged_in_refs, c),
            send_sem=merged_send.at[int(is_narrow(c))],
            recv_sem=merged_recv.at[c],
            device_id={"ep": partner},
            device_id_type=MESH,
        )

    def blended(weights, values):
        total = jnp.dot(weights[0], values, preferred_element_type=F32)
        return total + jnp.dot(weights[1], values, preferred_element_type=F32)

    def merge(c):
        @when_passing
        def _():
            ready = piece(merge_refs, c).at[: (half - 1) * slot_count]
            settle(ready, merge_recv.at[c]).wait_recv()
            piece(merged_refs, c)[...] = blended(merge_blend, piece(merge_refs, c)[...]).astype(BF16)
            merged_copy(c).start()

    def results(c):
        if c > 0:
            weight_copy(3 + c, 1).wait_recv()
            weight_copy(3 + c, 2).start()
        weight_copy(3 + c, 2).wait_recv()
        leaving = piece(leaving_refs, c)
        leaving[...] = jnp.dot(
            active_ref[...], piece(downs_refs, c)[...], preferred_element_type=F32
        ).astype(BF16)

        @when_passing
        def _():
            piece(merge_refs, c)[mine] = leaving[
                pl.ds(pl.multiple_of(partner * slot_count, slot_count), slot_count)
            ]

        if relayed:

            @each_far
            def _(peer):
                pl.when(ends(peer) & (peer != partner))(lambda: merge_copy(c, peer).start())

        @each_far
        def _(peer):
            if relayed:
                pl.when(jnp.logical_not(ends(peer)))(lambda: back_copy(c, peer, 1).start())
            else:
                back_copy(c, peer, 1).start()

    def near(c):
        each_near(lambda peer: back_copy(c, peer, 0).start())
        piece(returned_refs, c)[here] = piece(leaving_refs, c)[here]

    def collect(c):
        returned = piece(returned_refs, c)
        total = total_ref.at[:, : returned.shape[1]]
        settle(returned.at[: (half - 1) * slot_count], back_recv.at[c, 0]).wait_recv()
        total[...] = blended(blend_ref.at[base // half], returned[near_rows])

        @when_middle
        def _():
            settle(returned.at[: half * slot_count], back_recv.at[c, 1]).wait_recv()
            total[...] += blended(blend_ref.at[other // half], returned[far_rows])

        @when_end
        def _():
            merged_copy(c).wait_recv()
            total[...] += piece(merged_in_refs, c)[...].astype(F32)

        routed_ref[:, columns(c)] = total[...].astype(BF16)

    diagonal = lax.rem(beside + quarters // 2, quarters)

    def piece_copy(i):
        return pltpu.make_async_remote_copy(
            src_ref=(partial_ref.at[0], partial_ref.at[1], summed_ref)[i],
            dst_ref=pieces_ref.at[i],
            send_sem=piece_send.at[i],
            recv_sem=piece_recv.at[i],
            device_id={"tp": across if i == 2 else beside},
            device_id_type=MESH,
        )

    def project():
        for i, part in enumerate((diagonal, beside, across, place)):
            at = pl.ds(pl.multiple_of(part * row_count, row_count), row_count)
            partial_ref[i] = jnp.dot(
                hidden_ref[at], proj_ref[...], preferred_element_type=F32
            ).astype(BF16)
            if i < 2:
                piece_copy(i).start()

    def cross():
        piece_copy(0).wait_recv()
        summed_ref[...] = (partial_ref[2].astype(F32) + pieces_ref[0].astype(F32)).astype(BF16)
        piece_copy(2).start()

    def gather_mixed():
        piece_copy(1).wait_recv()
        piece_copy(2).wait_recv()
        total = partial_ref[3].astype(F32) + pieces_ref[1].astype(F32)
        mixed_ref[...] = (total + pieces_ref[2].astype(F32)).astype(BF16)

    for c in range(pieces):
        results(c)
        if c == 0:
            near(0)
        else:
            when_middle(lambda: near(c))
        if c == 4:
            when_end(lambda: near(1))
        if c == 1:
            finish_mixer()
        if c > 1:
            merge(c - 2)
        if c == 2:
            project()
        if c == 4:
            cross()

    def far_sent(group, blocks):
        narrow, wide = leaving_refs
        sent = (wide.at[: pieces - 3], narrow, wide.at[:1])[group]
        settle(sent.at[:, : blocks * slot_count], far_send.at[group]).wait_send()

    @when_end
    def _():
        far_sent(2, half)
        for c in range(2, pieces):
            near(c)

    merge(pieces - 2)
    merge(pieces - 1)
    for c in range(pieces):
        if c == pieces // 2:
            gather_mixed()
        collect(c)

    @when_end
    def _():
        rows_copy(0).wait_send()
        rows_copy(1).wait_send()
        settle(slots_ref.at[: (half - 1) * slot_count], slot_send).wait_send()
        for group in range(2):
            far_sent(group, half)

    @when_middle
    def _():
        settle(slots_ref.at[: (n - 1) * slot_count], slot_send).wait_send()
        for group in range(3):
            far_sent(group, half - 1 if relayed else half)

    @when_passing
    def _():
        settle(passed_ref.at[: (half - 1) * slot_count], pass_send).wait_send()
        for kind in range(2):
            settle(merged_refs[kind], merged_send.at[1 - kind]).wait_send()

    for kind in range(2):
        sent = leaving_refs[kind].at[:, : (half - 1) * slot_count]
        settle(sent, near_send.at[1 - kind]).wait_send()
    settle(state_in.at[: n - 1], state_send).wait_send()
    for i in range(3):
        piece_copy(i).wait_send()
    for hop in range(3):
        settle(gates_ref.at[0], weight_send.at[0, hop]).wait_send()
        settle(ups_ref.at[0], weight_send.at[1, hop]).wait_send()
        for kind in range(2):
            settle(downs_refs[kind].at[:, :units], weight_send.at[2 + kind, hop]).wait_send()


def shards(
    queries,
    forget_forward_logits,
    forget_backward_logits,
    values,
    output_gate_logits,
    lower_bound_forward,
    lower_bound_backward,
    extra_log_decay,
    head_norm_scale,
    output_projection,
    second_residual,
    expert_norm_scale,
    routes,
    specialist_mixing_factor,
    expert_gate_matrix,
    expert_up_matrix,
    expert_down_matrix,
):
    group_rows, width_model = second_residual.shape
    quarters = lax.axis_size("tp")
    n = lax.axis_size("ep")
    row_count = group_rows // quarters
    slot_count = 2 * TOPK * row_count // n
    slot_total = n * slot_count
    width = queries.shape[1]
    heads = extra_log_decay.shape[1]
    channels = width // heads
    depth = values.shape[1] // heads
    chunks = group_rows // CHUNK
    units = expert_down_matrix.shape[1]
    span = width_model // SPANS
    vmem = pl.BlockSpec(memory_space=pltpu.VMEM)
    anywhere = pl.BlockSpec(memory_space=pl.ANY)
    state = (heads, depth + DECAY_ROWS, channels)
    block = (group_rows, width)
    out = jax.ShapeDtypeStruct((row_count, width_model), BF16)

    def narrow_and_wide(height):
        return [
            pltpu.VMEM((2, height, span), BF16),
            pltpu.VMEM((PIECES - 2, height, 2 * span), BF16),
        ]

    dma = pltpu.SemaphoreType.DMA
    return pl.pallas_call(
        functools.partial(fused_kernel, n, quarters),
        out_shape=(out, out),
        in_specs=[anywhere] * 5
        + [vmem] * 4
        + [anywhere] * 2
        + [vmem] * 3
        + [anywhere] * 3,
        out_specs=(vmem, vmem),
        scratch_shapes=[pltpu.VMEM(block, BF16)] * 5
        + [
            pltpu.VMEM((width, width_model), BF16),
            pltpu.VMEM((row_count, width_model), BF16),
            pltpu.VMEM((2, n, row_count), F32),
            pltpu.VMEM((2, n, row_count), F32),
            pltpu.VMEM((row_count, width_model), BF16),
            pltpu.VMEM((row_count, width_model), BF16),
            pltpu.VMEM((slot_total, row_count), BF16),
            pltpu.VMEM((2, 2, row_count, slot_total // 2), BF16),
            pltpu.VMEM((2, row_count, slot_total // 2), BF16),
            pltpu.VMEM((slot_total, width_model), BF16),
            pltpu.VMEM((slot_total, width_model), BF16),
            pltpu.VMEM((slot_total // 2, width_model), BF16),
            pltpu.VMEM((quarters,) + expert_gate_matrix.shape[1:], BF16),
            pltpu.VMEM((quarters,) + expert_up_matrix.shape[1:], BF16),
            *narrow_and_wide(quarters * units),
            pltpu.VMEM((slot_total, quarters * units), F32),
            pltpu.VMEM((slot_total, quarters * units), BF16),
            pltpu.VMEM((2, slot_total, units), F32),
            *narrow_and_wide(slot_total),
            *narrow_and_wide(slot_total),
            *narrow_and_wide(slot_total // 2),
            *narrow_and_wide(row_count),
            *narrow_and_wide(row_count),
            pltpu.VMEM((row_count, 2 * span), F32),
            pltpu.VMEM((heads, chunks, CHUNK, depth), F32),
            pltpu.VMEM((2, heads, chunks, CHUNK, channels), BF16),
            pltpu.VMEM((2, heads, chunks, depth, channels), F32),
            pltpu.VMEM((2, heads, chunks, 8, channels), F32),
            pltpu.VMEM((2,) + state, BF16),
            pltpu.VMEM((n,) + state, BF16),
            pltpu.VMEM(block, BF16),
            pltpu.VMEM((4, row_count, width_model), BF16),
            pltpu.VMEM((row_count, width_model), BF16),
            pltpu.VMEM((3, row_count, width_model), BF16),
            dma((11,)),
            dma((2, 2)),
            dma(()),
            dma((PIECES,)),
            dma((2,)),
            dma((PIECES,)),
            dma(()),
            dma((2,)),
            dma(()),
            dma(()),
            dma((4, 3)),
            dma((3 + PIECES, 3)),
            dma((3,)),
            dma((2,)),
            dma((PIECES, 2)),
            dma((3,)),
            dma((3,)),
        ],
        compiler_params=pltpu.CompilerParams(
            collective_id=0, has_side_effects=True, vmem_limit_bytes=48 * 2**20
        ),
        cost_estimate=pl.CostEstimate(
            flops=4 * 10**10, bytes_accessed=30 * 2**20, transcendentals=0
        ),
        name="mix_and_route",
    )(
        *(
            pltpu.with_memory_space_constraint(operand, pltpu.HBM)
            for operand in (
                queries,
                forget_forward_logits,
                forget_backward_logits,
                values,
                output_gate_logits,
                lower_bound_forward.reshape(1, -1),
                lower_bound_backward.reshape(1, -1),
                extra_log_decay.T,
                head_norm_scale.reshape(1, -1),
                output_projection,
                second_residual,
                expert_norm_scale.reshape(1, -1),
                routes.T,
                specialist_mixing_factor.T,
                expert_gate_matrix,
                expert_up_matrix,
                expert_down_matrix,
            )
        )
    )


def solution(mesh):
    in_specs = (
        P("ep", "tp"),
        P("ep", "tp"),
        P("ep", "tp"),
        P("ep", "tp"),
        P("ep", "tp"),
        P("tp"),
        P("tp"),
        P("ep", "tp"),
        P("tp"),
        P("tp", None),
        P("ep", None),
        P(),
        P("ep", None),
        P(("ep", "tp"), None),
        P("ep", None, "tp"),
        P("ep", None, "tp"),
        P("ep", "tp", None),
    )
    out_specs = (P(("ep", "tp"), None), P(("ep", "tp"), None))
    return jax.shard_map(shards, mesh=mesh, in_specs=in_specs, out_specs=out_specs, check_vma=False)
```

```python
import functools

import jax
import jax.numpy as jnp
from jax import lax
from jax.experimental import pallas as pl
from jax.experimental.pallas import tpu as pltpu
from jax.sharding import PartitionSpec as P

TOPK = 2
CHUNK = 128
LEAF = 16
DECAY_ROWS = 16
SPANS = 16
PIECES = SPANS // 2 + 1
PLANES = 4
EPS = 1e-06
MESH = pl.DeviceIdType.MESH
F32 = jnp.float32
BF16 = jnp.bfloat16


def neighbours():
    place, count = lax.axis_index("tp"), lax.axis_size("tp")
    return place + 1 - 2 * lax.rem(place, 2), lax.rem(place + count // 2, count)


def greet(axis, n):
    me = lax.axis_index(axis)
    barrier = pltpu.get_barrier_semaphore()

    def one(step, carry):
        peer = lax.rem(me + step, n)
        pl.semaphore_signal(barrier, inc=1, device_id={axis: peer}, device_id_type=MESH)
        return carry

    lax.fori_loop(1, n, one, 0)


def dot_rows(a, b):
    return lax.dot_general(a, b, (((1,), (1,)), ((), ())), preferred_element_type=F32)


def gates(logits, bound, extra):
    shrink = jnp.exp(-logits)
    opened = 1.0 / (1.0 + shrink)
    floor_part = 1.0 / (1.0 + jnp.exp(-bound))
    complement = 1.0 / (1.0 + jnp.exp(bound))
    decay = jnp.log(floor_part + complement * opened) + extra
    return complement * (shrink * opened), decay


def referenced(total, size, place):
    blocks = total.reshape(CHUNK // size, size, total.shape[-1])
    anchor = jnp.broadcast_to(blocks[:, place : place + 1, :], blocks.shape)
    return total - anchor.reshape(total.shape)


def chunk_scores(feature, key, total, backward, rows, cols):
    scores = jnp.zeros((CHUNK, CHUNK), F32)
    size = CHUNK
    while size > LEAF:
        half = size // 2
        reach = jnp.exp(-jnp.abs(referenced(total, size, half if backward else half - 1)))
        part = dot_rows((feature * reach).astype(BF16), (key * reach).astype(BF16))
        late, early = (cols, rows) if backward else (rows, cols)
        mask = (rows // size == cols // size) & (late % size >= half) & (early % size < half)
        scores = scores + jnp.where(mask, part, 0.0)
        size = half
    spread = referenced(total, LEAF, LEAF // 2 if backward else LEAF // 2 - 1)
    part = dot_rows(
        (feature * jnp.exp(spread)).astype(BF16), (key * jnp.exp(-spread)).astype(BF16)
    )
    mask = (rows // LEAF == cols // LEAF) & ((rows <= cols) if backward else (rows >= cols))
    return scores + jnp.where(mask, part, 0.0)


def fused_kernel(
    n,
    quarters,
    q_any,
    ff_any,
    fb_any,
    v_any,
    og_any,
    lbf_ref,
    lbb_ref,
    extra_ref,
    scale_ref,
    proj_any,
    resid_any,
    gain_ref,
    routes_ref,
    mix_ref,
    gate_any,
    up_any,
    down_any,
    mixed_ref,
    routed_ref,
    q_ref,
    ff_ref,
    fb_ref,
    v_ref,
    og_ref,
    proj_ref,
    resid_ref,
    meta_ref,
    meta_in,
    rows_ref,
    rows_in,
    chooser_ref,
    blend_ref,
    merge_blend,
    slots_ref,
    arrived_ref,
    passed_ref,
    gates_ref,
    ups_ref,
    downs_ref_narrow,
    downs_ref_wide,
    gated_ref,
    active_ref,
    lifted_ref,
    leaving_ref_narrow,
    leaving_ref_wide,
    returned_ref_narrow,
    returned_ref_wide,
    merge_in_narrow,
    merge_in_wide,
    merged_ref_narrow,
    merged_ref_wide,
    merged_in_narrow,
    merged_in_wide,
    total_ref,
    local_ref,
    reach_ref,
    part_ref,
    fade_ref,
    state_out,
    state_in,
    hidden_ref,
    partial_ref,
    summed_ref,
    pieces_ref,
    load_sem,
    rows_sem,
    pass_send,
    merge_recv,
    merged_send,
    merged_recv,
    slot_send,
    slot_recv,
    state_send,
    state_recv,
    weight_send,
    weight_recv,
    far_send,
    near_send,
    back_recv,
    piece_send,
    piece_recv,
):
    me = lax.axis_index("ep")
    place = lax.axis_index("tp")
    group_rows, width = q_ref.shape
    row_count, width_model = resid_ref.shape
    chunks = group_rows // CHUNK
    heads = extra_ref.shape[0]
    channels = width // heads
    slot_total = slots_ref.shape[0]
    slot_count = slot_total // n
    units = down_any.shape[1]
    depth_half = width_model // 2

    pieces, span = PIECES, width_model // SPANS

    def piece(refs, c):
        narrow, wide = refs
        return narrow.at[c // (pieces - 1)] if is_narrow(c) else wide.at[c - 1]

    def is_narrow(c):
        return c in (0, pieces - 1)

    def far_group(c):
        return 1 if is_narrow(c) else 2 if c == pieces - 2 else 0

    def columns(c):
        first = max(0, (2 * c - 1) * span)
        return slice(first, first + (span if is_narrow(c) else 2 * span))

    downs_refs = downs_ref_narrow, downs_ref_wide
    leaving_refs = leaving_ref_narrow, leaving_ref_wide
    returned_refs = returned_ref_narrow, returned_ref_wide
    merge_refs = merge_in_narrow, merge_in_wide
    merged_refs = merged_ref_narrow, merged_ref_wide
    merged_in_refs = merged_in_narrow, merged_in_wide
    beside, across = neighbours()

    half = n // 2
    side = half * slot_count
    relayed = half == PLANES
    base = me // half * half
    other = half - base
    partner = lax.rem(me + half, n)
    plane = me // 2
    at_end = (plane == 0) | (plane == n // 2 - 1)

    def when_end(act):
        if relayed:
            pl.when(at_end)(act)

    def when_middle(act):
        if relayed:
            pl.when(jnp.logical_not(at_end))(act)
        else:
            act()

    def when_passing(act):
        if relayed:
            pl.when(jnp.logical_not(at_end))(act)

    greet("ep", n)
    greet("tp", quarters)
    first_row = pl.multiple_of(place * row_count, row_count)
    loads = [
        pltpu.make_async_copy(source, target, load_sem.at[i])
        for i, (source, target) in enumerate(
            (
                (gate_any.at[0], gates_ref.at[3]),
                (up_any.at[0], ups_ref.at[3]),
                (resid_any.at[pl.ds(first_row, row_count)], resid_ref),
                (q_any, q_ref),
                (ff_any, ff_ref),
                (fb_any, fb_ref),
                (v_any, v_ref),
                (og_any, og_ref),
                (proj_any, proj_ref),
            )
        )
    ]
    down_loads = [
        pltpu.make_async_copy(
            down_any.at[0, :, columns(c)],
            piece(downs_refs, c).at[3 * units : 4 * units],
            load_sem.at[9 if is_narrow(c) else 10],
        )
        for c in range(pieces)
    ]
    for load in loads[:2] + down_loads + loads[2:]:
        load.start()

    pl.semaphore_wait(pltpu.get_barrier_semaphore(), n + quarters - 2)

    def weight_copy(i, hop):
        kind = min(i, 1)
        if i == 0:
            held = lambda slot: gates_ref.at[slot]
        elif i < 3:
            at = slice((i - 1) * depth_half, i * depth_half)
            held = lambda slot: ups_ref.at[slot, at]
        else:
            kind = 2 if is_narrow(i - 3) else 3
            held = lambda slot: piece(downs_refs, i - 3).at[slot * units : (slot + 1) * units]
        return pltpu.make_async_remote_copy(
            src_ref=held(1 if hop == 2 else 3),
            dst_ref=held(hop),
            send_sem=weight_send.at[kind, hop],
            recv_sem=weight_recv.at[kind if hop == 0 else i, hop],
            device_id={"tp": across if hop == 1 else beside},
            device_id_type=MESH,
        )

    loads[0].wait()
    weight_copy(0, 1).start()
    loads[1].wait()
    for i in (1, 2):
        weight_copy(i, 1).start()
    for kind in range(2):
        own_part = downs_refs[kind].at[:, 3 * units : 4 * units]
        pltpu.make_async_copy(own_part, own_part, load_sem.at[9 + kind]).wait()
    for c in range(pieces):
        weight_copy(3 + c, 1).start()

    lanes = pl.ds(first_row, row_count)
    expert = lax.broadcasted_iota(jnp.int32, (n, row_count), 0)
    hits = jnp.zeros((n, row_count), F32)
    shares = jnp.zeros((n, row_count), F32)
    for k in range(TOPK):
        chosen = routes_ref[k : k + 1, lanes] == expert
        hits = jnp.where(chosen, 1.0, hits)
        shares = jnp.where(chosen, mix_ref[k : k + 1], shares)
    before = lax.broadcasted_iota(jnp.int32, (row_count, row_count), 0)
    after = lax.broadcasted_iota(jnp.int32, (row_count, row_count), 1)
    earlier = (before < after).astype(BF16)
    ranks = jnp.dot(hits.astype(BF16), earlier, preferred_element_type=F32)
    meta_ref[0] = jnp.where(hits > 0.0, ranks, -1.0)
    meta_ref[1] = shares
    slot = lax.broadcasted_iota(jnp.int32, (slot_count, row_count), 0).astype(F32)

    def selection(ref, first, count, weighted):
        parts = []
        for j in range(count):
            match = slot == ref[0, pl.ds(first + j, 1)]
            parts.append(jnp.where(match, ref[1, pl.ds(first + j, 1)] if weighted else 1.0, 0.0))
        return jnp.concatenate(parts, axis=0)

    def split(weights):
        high = weights.astype(BF16)
        return high, (weights - high.astype(F32)).astype(BF16)

    loads[2].wait()
    rows_wide = resid_ref[...].astype(F32)
    mean_square = jnp.mean(rows_wide * rows_wide, axis=-1, keepdims=True)
    rows_ref[...] = (rows_wide * lax.rsqrt(mean_square + EPS) * gain_ref[...]).astype(BF16)

    def rows_copy(i):
        return pltpu.make_async_remote_copy(
            src_ref=(rows_ref, meta_ref)[i],
            dst_ref=(rows_in, meta_in)[i],
            send_sem=rows_sem.at[0, i],
            recv_sem=rows_sem.at[1, i],
            device_id={"ep": partner},
            device_id_type=MESH,
        )

    @when_end
    def _():
        rows_copy(1).start()
        rows_copy(0).start()

    chooser_ref[...] = selection(meta_ref, 0, n, False).astype(BF16)
    for g in range(slot_total // row_count):
        at = slice(g * row_count, (g + 1) * row_count)
        slots_ref[at] = jnp.dot(
            chooser_ref[at], rows_ref[...], preferred_element_type=F32
        ).astype(BF16)

    def block(ref, index):
        return ref.at[pl.ds(pl.multiple_of(index * slot_count, slot_count), slot_count)]

    def slot_copy(target, far):
        return pltpu.make_async_remote_copy(
            src_ref=block(slots_ref, target),
            dst_ref=block(arrived_ref, me),
            send_sem=slot_send,
            recv_sem=slot_recv.at[far],
            device_id={"ep": target},
            device_id_type=MESH,
        )

    def settle(ref, semaphore):
        return pltpu.make_async_remote_copy(
            src_ref=ref,
            dst_ref=ref,
            send_sem=semaphore,
            recv_sem=semaphore,
            device_id={"ep": partner},
            device_id_type=MESH,
        )

    def back_copy(c, target, far):
        return pltpu.make_async_remote_copy(
            src_ref=block(piece(leaving_refs, c), target),
            dst_ref=block(piece(returned_refs, c), me),
            send_sem=far_send.at[far_group(c)] if far else near_send.at[int(is_narrow(c))],
            recv_sem=back_recv.at[c, far],
            device_id={"ep": target},
            device_id_type=MESH,
        )

    def each_peer(act):
        def one(step, carry):
            act(lax.rem(me + step, n))
            return carry

        lax.fori_loop(1, n, one, 0)

    def each_near(act):
        def one(step, carry):
            act(base + lax.rem(me - base + step, half))
            return carry

        lax.fori_loop(1, half, one, 0)

    def each_far(act):
        def one(step, carry):
            act(other + lax.rem(me - base + step, half))
            return carry

        lax.fori_loop(0, half, one, 0)

    when_middle(lambda: each_far(lambda peer: slot_copy(peer, 1).start()))
    each_near(lambda peer: slot_copy(peer, 0).start())
    for i in range(3 + pieces):
        weight_copy(i, 0).start()
    here = pl.ds(pl.multiple_of(me * slot_count, slot_count), slot_count)
    arrived_ref[here] = slots_ref[here]
    for h in range(2):
        blend_ref[h, 0], blend_ref[h, 1] = split(selection(meta_ref, h * half, half, True).T)

    for load in loads[3:]:
        load.wait()
    rows = lax.broadcasted_iota(jnp.int32, (CHUNK, CHUNK), 0)
    cols = lax.broadcasted_iota(jnp.int32, (CHUNK, CHUNK), 1)

    def local(c, carry):
        at = pl.ds(pl.multiple_of(c * CHUNK, CHUNK), CHUNK)
        for h in range(heads):
            lanes = slice(h * channels, (h + 1) * channels)
            queries = q_ref[at, lanes].astype(F32)
            feature = queries / (1.0 + jnp.exp(-queries))
            value_rows = v_ref[at, lanes]
            extra = jnp.broadcast_to(extra_ref[h : h + 1, at], (channels, CHUNK)).T
            scores = jnp.zeros((CHUNK, CHUNK), F32)
            for way, (logit_ref, bound_ref) in enumerate(((ff_ref, lbf_ref), (fb_ref, lbb_ref))):
                key, decay = gates(logit_ref[at, lanes].astype(F32), bound_ref[:, lanes], extra)
                order = (rows <= cols) if way else (rows >= cols)
                total = jnp.dot(
                    order.astype(F32),
                    decay,
                    preferred_element_type=F32,
                    precision=lax.Precision.HIGHEST,
                )
                edge = total[0:1] if way else total[CHUNK - 1 : CHUNK]
                scores = scores + chunk_scores(feature, key, total, way == 1, rows, cols)
                reach_ref[way, h, c] = (feature * jnp.exp(total)).astype(BF16)
                faded = (key * jnp.exp(edge - total)).astype(BF16)
                part_ref[way, h, c] = lax.dot_general(
                    value_rows, faded, (((0,), (0,)), ((), ())), preferred_element_type=F32
                )
                fade_ref[way, h, c] = jnp.broadcast_to(jnp.exp(edge), (8, channels))
            local_ref[h, c] = jnp.dot(
                scores.astype(BF16), value_rows, preferred_element_type=F32
            )
        return carry

    lax.fori_loop(0, chunks, local, 0)
    for way in range(2):
        for h in range(heads):
            state = jnp.zeros(part_ref.shape[3:], F32)
            fade = jnp.ones((1, channels), F32)
            for c in range(chunks)[:: -1 if way else 1]:
                step = fade_ref[way, h, c, 0:1]
                state = state * step + part_ref[way, h, c]
                fade = fade * step
            state_out[way, h, : state.shape[0]] = state.astype(BF16)
            state_out[way, h, state.shape[0] :] = jnp.broadcast_to(
                fade, (DECAY_ROWS, channels)
            ).astype(BF16)

    def state_copy(target):
        way = jnp.where(target > me, 0, 1)
        return pltpu.make_async_remote_copy(
            src_ref=state_out.at[way],
            dst_ref=state_in.at[me],
            send_sem=state_send,
            recv_sem=state_recv,
            device_id={"ep": target},
            device_id_type=MESH,
        )

    each_peer(lambda peer: state_copy(peer).start())

    def pass_copy(target):
        return pltpu.make_async_remote_copy(
            src_ref=block(passed_ref, target - base),
            dst_ref=block(arrived_ref, partner),
            send_sem=pass_send,
            recv_sem=slot_recv.at[1],
            device_id={"ep": target},
            device_id_type=MESH,
        )

    @when_passing
    def _():
        rows_copy(1).wait_recv()
        rows_copy(0).wait_recv()
        chosen = selection(meta_in, base, half, False).astype(BF16)
        passed_ref[...] = jnp.dot(chosen, rows_in[...], preferred_element_type=F32).astype(BF16)
        each_near(lambda peer: pass_copy(peer).start())
        arrived_ref[pl.ds(pl.multiple_of(partner * slot_count, slot_count), slot_count)] = (
            passed_ref[pl.ds(pl.multiple_of((me - base) * slot_count, slot_count), slot_count)]
        )
        merge_blend[0], merge_blend[1] = split(selection(meta_in, base, half, True).T)

    near_rows = pl.ds(pl.multiple_of(base * slot_count, side), side)
    far_rows = pl.ds(pl.multiple_of(other * slot_count, side), side)

    def open_gate(i, at):
        gated = jnp.dot(arrived_ref[at], gates_ref[i], preferred_element_type=F32)
        gated_ref[at, i * units : (i + 1) * units] = gated / (1.0 + jnp.exp(-gated))

    def lift(i, part, at):
        rows_of = slice(part * depth_half, (part + 1) * depth_half)
        return jnp.dot(arrived_ref[at, rows_of], ups_ref[i, rows_of], preferred_element_type=F32)

    def activate(i, at, lifted):
        hidden = slice(i * units, (i + 1) * units)
        active_ref[at, hidden] = (gated_ref[at, hidden] * lifted).astype(BF16)

    def activate_whole(i, at):
        activate(i, at, jnp.dot(arrived_ref[at], ups_ref[i], preferred_element_type=F32))

    def finish_mixer():
        settle(state_in.at[: n - 1], state_recv).wait_recv()
        depth = part_ref.shape[3]
        for h in range(heads):
            for way in range(2):

                def one(hop, state, way=way, h=h):
                    source = n - 1 - hop if way else hop
                    step = state_in[source, h, depth : depth + DECAY_ROWS].astype(F32)[0:1]
                    return state * step + state_in[source, h, :depth].astype(F32)

                ahead = n - 1 - me if way else me
                state = lax.fori_loop(0, ahead, one, jnp.zeros(part_ref.shape[3:], F32))
                for c in range(chunks)[:: -1 if way else 1]:
                    local_ref[h, c] += dot_rows(reach_ref[way, h, c], state.astype(BF16))
                    state = state * fade_ref[way, h, c, 0:1] + part_ref[way, h, c]
            lanes = slice(h * channels, (h + 1) * channels)
            for c in range(chunks):
                at = slice(c * CHUNK, (c + 1) * CHUNK)
                combined = local_ref[h, c]
                mean_square = jnp.mean(combined * combined, axis=-1, keepdims=True)
                gate = og_ref[at, lanes].astype(F32)
                opened = combined * lax.rsqrt(mean_square + EPS) * scale_ref[:, lanes]
                hidden_ref[at, lanes] = (opened * (gate / (1.0 + jnp.exp(-gate)))).astype(BF16)

    every = slice(None)
    for kind in range(2):
        settle(downs_refs[kind].at[:, :units], weight_recv.at[2 + kind, 0]).wait_recv()
    weight_copy(0, 0).wait_recv()
    settle(ups_ref.at[0], weight_recv.at[1, 0]).wait_recv()
    settle(arrived_ref.at[: (half - 1) * slot_count], slot_recv.at[0]).wait_recv()
    for i in (3, 0):
        open_gate(i, near_rows)
        activate_whole(i, near_rows)
    weight_copy(0, 1).wait_recv()
    weight_copy(0, 2).start()
    open_gate(1, near_rows)
    weight_copy(0, 2).wait_recv()
    open_gate(2, near_rows)
    weight_copy(1, 1).wait_recv()
    weight_copy(1, 2).start()

    @when_end
    def _():
        settle(arrived_ref.at[: half * slot_count], slot_recv.at[1]).wait_recv()

    @when_middle
    def _():
        blocks = half - 1 if relayed else half
        settle(arrived_ref.at[: blocks * slot_count], slot_recv.at[1]).wait_recv()

    for i in (3, 0):
        open_gate(i, far_rows)
        activate_whole(i, far_rows)
    open_gate(1, far_rows)
    open_gate(2, far_rows)
    lifted_ref[0] = lift(1, 0, every)
    weight_copy(1, 2).wait_recv()
    lifted_ref[1] = lift(2, 0, every)
    weight_copy(2, 1).wait_recv()
    weight_copy(2, 2).start()
    activate(1, every, lifted_ref[0] + lift(1, 1, every))
    weight_copy(3, 1).wait_recv()
    weight_copy(3, 2).start()
    weight_copy(2, 2).wait_recv()
    activate(2, every, lifted_ref[1] + lift(2, 1, every))

    mine = pl.ds(pl.multiple_of((me - base) * slot_count, slot_count), slot_count)

    def merge_copy(c, dest):
        return pltpu.make_async_remote_copy(
            src_ref=block(piece(leaving_refs, c), dest),
            dst_ref=block(piece(merge_refs, c), me - base),
            send_sem=far_send.at[far_group(c)],
            recv_sem=merge_recv.at[c],
            device_id={"ep": lax.rem(dest + half, n)},
            device_id_type=MESH,
        )

    def ends(peer):
        return (peer // 2 == 0) | (peer // 2 == n // 2 - 1)

    def merged_copy(c):
        return pltpu.make_async_remote_copy(
            src_ref=piece(merged_refs, c),
            dst_ref=piece(merged_in_refs, c),
            send_sem=merged_send.at[int(is_narrow(c))],
            recv_sem=merged_recv.at[c],
            device_id={"ep": partner},
            device_id_type=MESH,
        )

    def blended(weights, values):
        total = jnp.dot(weights[0], values, preferred_element_type=F32)
        return total + jnp.dot(weights[1], values, preferred_element_type=F32)

    def merge(c):
        @when_passing
        def _():
            ready = piece(merge_refs, c).at[: (half - 1) * slot_count]
            settle(ready, merge_recv.at[c]).wait_recv()
            piece(merged_refs, c)[...] = blended(merge_blend, piece(merge_refs, c)[...]).astype(BF16)
            merged_copy(c).start()

    def results(c):
        if c > 0:
            weight_copy(3 + c, 1).wait_recv()
            weight_copy(3 + c, 2).start()
        weight_copy(3 + c, 2).wait_recv()
        leaving = piece(leaving_refs, c)
        leaving[...] = jnp.dot(
            active_ref[...], piece(downs_refs, c)[...], preferred_element_type=F32
        ).astype(BF16)

        @when_passing
        def _():
            piece(merge_refs, c)[mine] = leaving[
                pl.ds(pl.multiple_of(partner * slot_count, slot_count), slot_count)
            ]

        if relayed:

            @each_far
            def _(peer):
                pl.when(ends(peer) & (peer != partner))(lambda: merge_copy(c, peer).start())

    def far(c):
        @each_far
        def _(peer):
            if relayed:
                pl.when(jnp.logical_not(ends(peer)))(lambda: back_copy(c, peer, 1).start())
            else:
                back_copy(c, peer, 1).start()

    def near(c):
        each_near(lambda peer: back_copy(c, peer, 0).start())
        piece(returned_refs, c)[here] = piece(leaving_refs, c)[here]

    def collect(c):
        returned = piece(returned_refs, c)
        total = total_ref.at[:, : returned.shape[1]]
        settle(returned.at[: (half - 1) * slot_count], back_recv.at[c, 0]).wait_recv()
        total[...] = blended(blend_ref.at[base // half], returned[near_rows])

        @when_middle
        def _():
            settle(returned.at[: half * slot_count], back_recv.at[c, 1]).wait_recv()
            total[...] += blended(blend_ref.at[other // half], returned[far_rows])

        @when_end
        def _():
            merged_copy(c).wait_recv()
            total[...] += piece(merged_in_refs, c)[...].astype(F32)

        routed_ref[:, columns(c)] = total[...].astype(BF16)

    diagonal = lax.rem(beside + quarters // 2, quarters)

    def piece_copy(i):
        return pltpu.make_async_remote_copy(
            src_ref=(partial_ref.at[0], partial_ref.at[1], summed_ref)[i],
            dst_ref=pieces_ref.at[i],
            send_sem=piece_send.at[i],
            recv_sem=piece_recv.at[i],
            device_id={"tp": across if i == 2 else beside},
            device_id_type=MESH,
        )

    def project():
        for i, part in enumerate((diagonal, beside, across, place)):
            at = pl.ds(pl.multiple_of(part * row_count, row_count), row_count)
            partial_ref[i] = jnp.dot(
                hidden_ref[at], proj_ref[...], preferred_element_type=F32
            ).astype(BF16)
            if i < 2:
                piece_copy(i).start()

    def cross():
        piece_copy(0).wait_recv()
        summed_ref[...] = (partial_ref[2].astype(F32) + pieces_ref[0].astype(F32)).astype(BF16)
        piece_copy(2).start()

    def gather_mixed():
        piece_copy(1).wait_recv()
        piece_copy(2).wait_recv()
        total = partial_ref[3].astype(F32) + pieces_ref[1].astype(F32)
        mixed_ref[...] = (total + pieces_ref[2].astype(F32)).astype(BF16)

    early = 4
    for c in range(pieces):
        results(c)
        if c < early or not relayed:
            far(c)
        else:
            when_end(lambda: far(c))
        if c == 0:
            near(0)
        else:
            when_middle(lambda: near(c))
        if c == 4:
            when_end(lambda: near(1))
        if c == 1:
            finish_mixer()
        if 0 < c < 3:
            merge(c - 1)
        if c > 3:
            merge(c - 2)
        if c == 2:
            project()
        if c == 4:
            cross()

    def far_sent(group, blocks):
        narrow, wide = leaving_refs
        sent = (wide.at[: pieces - 3], narrow, wide.at[:1])[group]
        settle(sent.at[:, : blocks * slot_count], far_send.at[group]).wait_send()

    @when_end
    def _():
        far_sent(2, half)
        for c in range(2, pieces):
            near(c)

    for c in range(early, pieces - 3):
        when_passing(lambda: far(c))
    merge(pieces - 2)
    when_passing(lambda: far(pieces - 3))
    merge(pieces - 1)
    for c in range(pieces - 2, pieces):
        when_passing(lambda: far(c))
    for c in range(pieces):
        if c == pieces // 2:
            gather_mixed()
        collect(c)

    @when_end
    def _():
        rows_copy(0).wait_send()
        rows_copy(1).wait_send()
        settle(slots_ref.at[: (half - 1) * slot_count], slot_send).wait_send()
        for group in range(2):
            far_sent(group, half)

    @when_middle
    def _():
        settle(slots_ref.at[: (n - 1) * slot_count], slot_send).wait_send()
        for group in range(3):
            far_sent(group, half - 1 if relayed else half)

    @when_passing
    def _():
        settle(passed_ref.at[: (half - 1) * slot_count], pass_send).wait_send()
        for kind in range(2):
            settle(merged_refs[kind], merged_send.at[1 - kind]).wait_send()

    for kind in range(2):
        sent = leaving_refs[kind].at[:, : (half - 1) * slot_count]
        settle(sent, near_send.at[1 - kind]).wait_send()
    settle(state_in.at[: n - 1], state_send).wait_send()
    for i in range(3):
        piece_copy(i).wait_send()
    for hop in range(3):
        settle(gates_ref.at[0], weight_send.at[0, hop]).wait_send()
        settle(ups_ref.at[0], weight_send.at[1, hop]).wait_send()
        for kind in range(2):
            settle(downs_refs[kind].at[:, :units], weight_send.at[2 + kind, hop]).wait_send()


def shards(
    queries,
    forget_forward_logits,
    forget_backward_logits,
    values,
    output_gate_logits,
    lower_bound_forward,
    lower_bound_backward,
    extra_log_decay,
    head_norm_scale,
    output_projection,
    second_residual,
    expert_norm_scale,
    routes,
    specialist_mixing_factor,
    expert_gate_matrix,
    expert_up_matrix,
    expert_down_matrix,
):
    group_rows, width_model = second_residual.shape
    quarters = lax.axis_size("tp")
    n = lax.axis_size("ep")
    row_count = group_rows // quarters
    slot_count = 2 * TOPK * row_count // n
    slot_total = n * slot_count
    width = queries.shape[1]
    heads = extra_log_decay.shape[1]
    channels = width // heads
    depth = values.shape[1] // heads
    chunks = group_rows // CHUNK
    units = expert_down_matrix.shape[1]
    span = width_model // SPANS
    vmem = pl.BlockSpec(memory_space=pltpu.VMEM)
    anywhere = pl.BlockSpec(memory_space=pl.ANY)
    state = (heads, depth + DECAY_ROWS, channels)
    block = (group_rows, width)
    out = jax.ShapeDtypeStruct((row_count, width_model), BF16)

    def narrow_and_wide(height):
        return [
            pltpu.VMEM((2, height, span), BF16),
            pltpu.VMEM((PIECES - 2, height, 2 * span), BF16),
        ]

    dma = pltpu.SemaphoreType.DMA
    return pl.pallas_call(
        functools.partial(fused_kernel, n, quarters),
        out_shape=(out, out),
        in_specs=[anywhere] * 5
        + [vmem] * 4
        + [anywhere] * 2
        + [vmem] * 3
        + [anywhere] * 3,
        out_specs=(vmem, vmem),
        scratch_shapes=[pltpu.VMEM(block, BF16)] * 5
        + [
            pltpu.VMEM((width, width_model), BF16),
            pltpu.VMEM((row_count, width_model), BF16),
            pltpu.VMEM((2, n, row_count), F32),
            pltpu.VMEM((2, n, row_count), F32),
            pltpu.VMEM((row_count, width_model), BF16),
            pltpu.VMEM((row_count, width_model), BF16),
            pltpu.VMEM((slot_total, row_count), BF16),
            pltpu.VMEM((2, 2, row_count, slot_total // 2), BF16),
            pltpu.VMEM((2, row_count, slot_total // 2), BF16),
            pltpu.VMEM((slot_total, width_model), BF16),
            pltpu.VMEM((slot_total, width_model), BF16),
            pltpu.VMEM((slot_total // 2, width_model), BF16),
            pltpu.VMEM((quarters,) + expert_gate_matrix.shape[1:], BF16),
            pltpu.VMEM((quarters,) + expert_up_matrix.shape[1:], BF16),
            *narrow_and_wide(quarters * units),
            pltpu.VMEM((slot_total, quarters * units), F32),
            pltpu.VMEM((slot_total, quarters * units), BF16),
            pltpu.VMEM((2, slot_total, units), F32),
            *narrow_and_wide(slot_total),
            *narrow_and_wide(slot_total),
            *narrow_and_wide(slot_total // 2),
            *narrow_and_wide(row_count),
            *narrow_and_wide(row_count),
            pltpu.VMEM((row_count, 2 * span), F32),
            pltpu.VMEM((heads, chunks, CHUNK, depth), F32),
            pltpu.VMEM((2, heads, chunks, CHUNK, channels), BF16),
            pltpu.VMEM((2, heads, chunks, depth, channels), F32),
            pltpu.VMEM((2, heads, chunks, 8, channels), F32),
            pltpu.VMEM((2,) + state, BF16),
            pltpu.VMEM((n,) + state, BF16),
            pltpu.VMEM(block, BF16),
            pltpu.VMEM((4, row_count, width_model), BF16),
            pltpu.VMEM((row_count, width_model), BF16),
            pltpu.VMEM((3, row_count, width_model), BF16),
            dma((11,)),
            dma((2, 2)),
            dma(()),
            dma((PIECES,)),
            dma((2,)),
            dma((PIECES,)),
            dma(()),
            dma((2,)),
            dma(()),
            dma(()),
            dma((4, 3)),
            dma((3 + PIECES, 3)),
            dma((3,)),
            dma((2,)),
            dma((PIECES, 2)),
            dma((3,)),
            dma((3,)),
        ],
        compiler_params=pltpu.CompilerParams(
            collective_id=0, has_side_effects=True, vmem_limit_bytes=48 * 2**20
        ),
        cost_estimate=pl.CostEstimate(
            flops=4 * 10**10, bytes_accessed=30 * 2**20, transcendentals=0
        ),
        name="mix_and_route",
    )(
        *(
            pltpu.with_memory_space_constraint(operand, pltpu.HBM)
            for operand in (
                queries,
                forget_forward_logits,
                forget_backward_logits,
                values,
                output_gate_logits,
                lower_bound_forward.reshape(1, -1),
                lower_bound_backward.reshape(1, -1),
                extra_log_decay.T,
                head_norm_scale.reshape(1, -1),
                output_projection,
                second_residual,
                expert_norm_scale.reshape(1, -1),
                routes.T,
                specialist_mixing_factor.T,
                expert_gate_matrix,
                expert_up_matrix,
                expert_down_matrix,
            )
        )
    )


def solution(mesh):
    in_specs = (
        P("ep", "tp"),
        P("ep", "tp"),
        P("ep", "tp"),
        P("ep", "tp"),
        P("ep", "tp"),
        P("tp"),
        P("tp"),
        P("ep", "tp"),
        P("tp"),
        P("tp", None),
        P("ep", None),
        P(),
        P("ep", None),
        P(("ep", "tp"), None),
        P("ep", None, "tp"),
        P("ep", None, "tp"),
        P("ep", "tp", None),
    )
    out_specs = (P(("ep", "tp"), None), P(("ep", "tp"), None))
    return jax.shard_map(shards, mesh=mesh, in_specs=in_specs, out_specs=out_specs, check_vma=False)
```

```python
import functools

import jax
import jax.numpy as jnp
from jax import lax
from jax.experimental import pallas as pl
from jax.experimental.pallas import tpu as pltpu
from jax.sharding import PartitionSpec as P

TOPK = 2
CHUNK = 128
LEAF = 16
DECAY_ROWS = 16
SPANS = 16
PIECES = SPANS // 2 + 1
PLANES = 4
EPS = 1e-06
MESH = pl.DeviceIdType.MESH
F32 = jnp.float32
BF16 = jnp.bfloat16


def neighbours():
    place, count = lax.axis_index("tp"), lax.axis_size("tp")
    return place + 1 - 2 * lax.rem(place, 2), lax.rem(place + count // 2, count)


def greet(axis, n):
    me = lax.axis_index(axis)
    barrier = pltpu.get_barrier_semaphore()

    def one(step, carry):
        peer = lax.rem(me + step, n)
        pl.semaphore_signal(barrier, inc=1, device_id={axis: peer}, device_id_type=MESH)
        return carry

    lax.fori_loop(1, n, one, 0)


def dot_rows(a, b):
    return lax.dot_general(a, b, (((1,), (1,)), ((), ())), preferred_element_type=F32)


def gates(logits, bound, extra):
    shrink = jnp.exp(-logits)
    opened = 1.0 / (1.0 + shrink)
    floor_part = 1.0 / (1.0 + jnp.exp(-bound))
    complement = 1.0 / (1.0 + jnp.exp(bound))
    decay = jnp.log(floor_part + complement * opened) + extra
    return complement * (shrink * opened), decay


def referenced(total, size, place):
    blocks = total.reshape(CHUNK // size, size, total.shape[-1])
    anchor = jnp.broadcast_to(blocks[:, place : place + 1, :], blocks.shape)
    return total - anchor.reshape(total.shape)


def chunk_scores(feature, key, total, backward, rows, cols):
    scores = jnp.zeros((CHUNK, CHUNK), F32)
    size = CHUNK
    while size > LEAF:
        half = size // 2
        reach = jnp.exp(-jnp.abs(referenced(total, size, half if backward else half - 1)))
        part = dot_rows((feature * reach).astype(BF16), (key * reach).astype(BF16))
        late, early = (cols, rows) if backward else (rows, cols)
        mask = (rows // size == cols // size) & (late % size >= half) & (early % size < half)
        scores = scores + jnp.where(mask, part, 0.0)
        size = half
    spread = referenced(total, LEAF, LEAF // 2 if backward else LEAF // 2 - 1)
    part = dot_rows(
        (feature * jnp.exp(spread)).astype(BF16), (key * jnp.exp(-spread)).astype(BF16)
    )
    mask = (rows // LEAF == cols // LEAF) & ((rows <= cols) if backward else (rows >= cols))
    return scores + jnp.where(mask, part, 0.0)


def fused_kernel(
    n,
    quarters,
    q_any,
    ff_any,
    fb_any,
    v_any,
    og_any,
    lbf_any,
    lbb_any,
    extra_any,
    scale_any,
    proj_any,
    resid_any,
    gain_any,
    routes_any,
    mix_any,
    gate_any,
    up_any,
    down_any,
    both_ref,
    lbf_ref,
    lbb_ref,
    extra_ref,
    scale_ref,
    gain_ref,
    routes_ref,
    mix_ref,
    q_ref,
    ff_ref,
    fb_ref,
    v_ref,
    og_ref,
    proj_ref,
    resid_ref,
    meta_ref,
    meta_in,
    rows_ref,
    rows_in,
    chooser_ref,
    blend_ref,
    merge_blend,
    slots_ref,
    arrived_ref,
    passed_ref,
    gates_ref,
    ups_ref,
    downs_ref_narrow,
    downs_ref_wide,
    gated_ref,
    active_ref,
    lifted_ref,
    leaving_ref_narrow,
    leaving_ref_wide,
    returned_ref_narrow,
    returned_ref_wide,
    merge_in_narrow,
    merge_in_wide,
    merged_ref_narrow,
    merged_ref_wide,
    merged_in_narrow,
    merged_in_wide,
    total_ref,
    local_ref,
    reach_ref,
    part_ref,
    fade_ref,
    state_out,
    state_in,
    hidden_ref,
    partial_ref,
    summed_ref,
    pieces_ref,
    load_sem,
    rows_sem,
    pass_send,
    merge_recv,
    merged_send,
    merged_recv,
    slot_send,
    slot_recv,
    state_send,
    state_recv,
    weight_send,
    weight_recv,
    far_send,
    near_send,
    back_recv,
    piece_send,
    piece_recv,
):
    mixed_ref, routed_ref = both_ref.at[0], both_ref.at[1]
    me = lax.axis_index("ep")
    place = lax.axis_index("tp")
    group_rows, width = q_ref.shape
    row_count, width_model = resid_ref.shape
    chunks = group_rows // CHUNK
    heads = extra_ref.shape[0]
    channels = width // heads
    slot_total = slots_ref.shape[0]
    slot_count = slot_total // n
    units = down_any.shape[1]
    depth_half = width_model // 2

    pieces, span = PIECES, width_model // SPANS

    def piece(refs, c):
        narrow, wide = refs
        return narrow.at[c // (pieces - 1)] if is_narrow(c) else wide.at[c - 1]

    def is_narrow(c):
        return c in (0, pieces - 1)

    def far_group(c):
        return 1 if is_narrow(c) else 2 if c == pieces - 2 else 0

    def columns(c):
        first = max(0, (2 * c - 1) * span)
        return slice(first, first + (span if is_narrow(c) else 2 * span))

    downs_refs = downs_ref_narrow, downs_ref_wide
    leaving_refs = leaving_ref_narrow, leaving_ref_wide
    returned_refs = returned_ref_narrow, returned_ref_wide
    merge_refs = merge_in_narrow, merge_in_wide
    merged_refs = merged_ref_narrow, merged_ref_wide
    merged_in_refs = merged_in_narrow, merged_in_wide
    beside, across = neighbours()

    half = n // 2
    side = half * slot_count
    relayed = half == PLANES
    base = me // half * half
    other = half - base
    partner = lax.rem(me + half, n)
    plane = me // 2
    at_end = (plane == 0) | (plane == n // 2 - 1)

    def when_end(act):
        if relayed:
            pl.when(at_end)(act)

    def when_middle(act):
        if relayed:
            pl.when(jnp.logical_not(at_end))(act)
        else:
            act()

    def when_passing(act):
        if relayed:
            pl.when(jnp.logical_not(at_end))(act)

    greet("ep", n)
    greet("tp", quarters)
    first_row = pl.multiple_of(place * row_count, row_count)
    loads = [
        pltpu.make_async_copy(source, target, load_sem.at[i])
        for i, (source, target) in enumerate(
            (
                (gate_any.at[0], gates_ref.at[3]),
                (up_any.at[0], ups_ref.at[3]),
                (resid_any.at[pl.ds(first_row, row_count)], resid_ref),
                (q_any, q_ref),
                (ff_any, ff_ref),
                (fb_any, fb_ref),
                (v_any, v_ref),
                (og_any, og_ref),
                (proj_any, proj_ref),
            )
        )
    ]
    down_loads = [
        pltpu.make_async_copy(
            down_any.at[0, :, columns(c)],
            piece(downs_refs, c).at[3 * units : 4 * units],
            load_sem.at[9 if is_narrow(c) else 10],
        )
        for c in range(pieces)
    ]
    small_loads = [
        pltpu.make_async_copy(source, target, load_sem.at[11 + i])
        for i, (source, target) in enumerate(
            (
                (routes_any, routes_ref),
                (mix_any, mix_ref),
                (gain_any, gain_ref),
                (extra_any, extra_ref),
                (lbf_any, lbf_ref),
                (lbb_any, lbb_ref),
                (scale_any, scale_ref),
            )
        )
    ]
    for load in loads[:2] + small_loads + loads[2:3] + down_loads + loads[3:]:
        load.start()

    pl.semaphore_wait(pltpu.get_barrier_semaphore(), n + quarters - 2)

    def weight_copy(i, hop):
        kind = min(i, 1)
        if i == 0:
            held = lambda slot: gates_ref.at[slot]
        elif i < 3:
            at = slice((i - 1) * depth_half, i * depth_half)
            held = lambda slot: ups_ref.at[slot, at]
        else:
            kind = 2 if is_narrow(i - 3) else 3
            held = lambda slot: piece(downs_refs, i - 3).at[slot * units : (slot + 1) * units]
        return pltpu.make_async_remote_copy(
            src_ref=held(1 if hop == 2 else 3),
            dst_ref=held(hop),
            send_sem=weight_send.at[kind, hop],
            recv_sem=weight_recv.at[kind if hop == 0 else i, hop],
            device_id={"tp": across if hop == 1 else beside},
            device_id_type=MESH,
        )

    loads[0].wait()
    weight_copy(0, 1).start()
    loads[1].wait()
    for i in (1, 2):
        weight_copy(i, 1).start()
    for kind in range(2):
        own_part = downs_refs[kind].at[:, 3 * units : 4 * units]
        pltpu.make_async_copy(own_part, own_part, load_sem.at[9 + kind]).wait()
    for c in range(pieces):
        weight_copy(3 + c, 1).start()

    for load in small_loads:
        load.wait()

    lanes = pl.ds(first_row, row_count)
    expert = lax.broadcasted_iota(jnp.int32, (n, row_count), 0)
    hits = jnp.zeros((n, row_count), F32)
    shares = jnp.zeros((n, row_count), F32)
    for k in range(TOPK):
        chosen = routes_ref[k : k + 1, lanes] == expert
        hits = jnp.where(chosen, 1.0, hits)
        shares = jnp.where(chosen, mix_ref[k : k + 1], shares)
    before = lax.broadcasted_iota(jnp.int32, (row_count, row_count), 0)
    after = lax.broadcasted_iota(jnp.int32, (row_count, row_count), 1)
    earlier = (before < after).astype(BF16)
    ranks = jnp.dot(hits.astype(BF16), earlier, preferred_element_type=F32)
    meta_ref[0] = jnp.where(hits > 0.0, ranks, -1.0)
    meta_ref[1] = shares
    slot = lax.broadcasted_iota(jnp.int32, (slot_count, row_count), 0).astype(F32)

    def selection(ref, first, count, weighted):
        parts = []
        for j in range(count):
            match = slot == ref[0, pl.ds(first + j, 1)]
            parts.append(jnp.where(match, ref[1, pl.ds(first + j, 1)] if weighted else 1.0, 0.0))
        return jnp.concatenate(parts, axis=0)

    def split(weights):
        high = weights.astype(BF16)
        return high, (weights - high.astype(F32)).astype(BF16)

    loads[2].wait()
    rows_wide = resid_ref[...].astype(F32)
    mean_square = jnp.mean(rows_wide * rows_wide, axis=-1, keepdims=True)
    rows_ref[...] = (rows_wide * lax.rsqrt(mean_square + EPS) * gain_ref[...]).astype(BF16)

    def rows_copy(i):
        return pltpu.make_async_remote_copy(
            src_ref=(rows_ref, meta_ref)[i],
            dst_ref=(rows_in, meta_in)[i],
            send_sem=rows_sem.at[0, i],
            recv_sem=rows_sem.at[1, i],
            device_id={"ep": partner},
            device_id_type=MESH,
        )

    @when_end
    def _():
        rows_copy(1).start()
        rows_copy(0).start()

    chooser_ref[...] = selection(meta_ref, 0, n, False).astype(BF16)
    for g in range(slot_total // row_count):
        at = slice(g * row_count, (g + 1) * row_count)
        slots_ref[at] = jnp.dot(
            chooser_ref[at], rows_ref[...], preferred_element_type=F32
        ).astype(BF16)

    def block(ref, index):
        return ref.at[pl.ds(pl.multiple_of(index * slot_count, slot_count), slot_count)]

    def slot_copy(target, far):
        return pltpu.make_async_remote_copy(
            src_ref=block(slots_ref, target),
            dst_ref=block(arrived_ref, me),
            send_sem=slot_send,
            recv_sem=slot_recv.at[far],
            device_id={"ep": target},
            device_id_type=MESH,
        )

    def settle(ref, semaphore):
        return pltpu.make_async_remote_copy(
            src_ref=ref,
            dst_ref=ref,
            send_sem=semaphore,
            recv_sem=semaphore,
            device_id={"ep": partner},
            device_id_type=MESH,
        )

    def back_copy(c, target, far):
        return pltpu.make_async_remote_copy(
            src_ref=block(piece(leaving_refs, c), target),
            dst_ref=block(piece(returned_refs, c), me),
            send_sem=far_send.at[far_group(c)] if far else near_send.at[int(is_narrow(c))],
            recv_sem=back_recv.at[c, far],
            device_id={"ep": target},
            device_id_type=MESH,
        )

    def each_peer(act):
        def one(step, carry):
            act(lax.rem(me + step, n))
            return carry

        lax.fori_loop(1, n, one, 0)

    def each_near(act):
        def one(step, carry):
            act(base + lax.rem(me - base + step, half))
            return carry

        lax.fori_loop(1, half, one, 0)

    def each_far(act):
        def one(step, carry):
            act(other + lax.rem(me - base + step, half))
            return carry

        lax.fori_loop(0, half, one, 0)

    when_middle(lambda: each_far(lambda peer: slot_copy(peer, 1).start()))
    each_near(lambda peer: slot_copy(peer, 0).start())
    for i in range(3 + pieces):
        weight_copy(i, 0).start()
    here = pl.ds(pl.multiple_of(me * slot_count, slot_count), slot_count)
    arrived_ref[here] = slots_ref[here]
    for h in range(2):
        blend_ref[h, 0], blend_ref[h, 1] = split(selection(meta_ref, h * half, half, True).T)

    for load in loads[3:]:
        load.wait()
    rows = lax.broadcasted_iota(jnp.int32, (CHUNK, CHUNK), 0)
    cols = lax.broadcasted_iota(jnp.int32, (CHUNK, CHUNK), 1)

    def local(c, carry):
        at = pl.ds(pl.multiple_of(c * CHUNK, CHUNK), CHUNK)
        for h in range(heads):
            lanes = slice(h * channels, (h + 1) * channels)
            queries = q_ref[at, lanes].astype(F32)
            feature = queries / (1.0 + jnp.exp(-queries))
            value_rows = v_ref[at, lanes]
            extra = jnp.broadcast_to(extra_ref[h : h + 1, at], (channels, CHUNK)).T
            scores = jnp.zeros((CHUNK, CHUNK), F32)
            for way, (logit_ref, bound_ref) in enumerate(((ff_ref, lbf_ref), (fb_ref, lbb_ref))):
                key, decay = gates(logit_ref[at, lanes].astype(F32), bound_ref[:, lanes], extra)
                order = (rows <= cols) if way else (rows >= cols)
                total = jnp.dot(
                    order.astype(F32),
                    decay,
                    preferred_element_type=F32,
                    precision=lax.Precision.HIGHEST,
                )
                edge = total[0:1] if way else total[CHUNK - 1 : CHUNK]
                scores = scores + chunk_scores(feature, key, total, way == 1, rows, cols)
                reach_ref[way, h, c] = (feature * jnp.exp(total)).astype(BF16)
                faded = (key * jnp.exp(edge - total)).astype(BF16)
                part_ref[way, h, c] = lax.dot_general(
                    value_rows, faded, (((0,), (0,)), ((), ())), preferred_element_type=F32
                )
                fade_ref[way, h, c] = jnp.broadcast_to(jnp.exp(edge), (8, channels))
            local_ref[h, c] = jnp.dot(
                scores.astype(BF16), value_rows, preferred_element_type=F32
            )
        return carry

    lax.fori_loop(0, chunks, local, 0)
    for way in range(2):
        for h in range(heads):
            state = jnp.zeros(part_ref.shape[3:], F32)
            fade = jnp.ones((1, channels), F32)
            for c in range(chunks)[:: -1 if way else 1]:
                step = fade_ref[way, h, c, 0:1]
                state = state * step + part_ref[way, h, c]
                fade = fade * step
            state_out[way, h, : state.shape[0]] = state.astype(BF16)
            state_out[way, h, state.shape[0] :] = jnp.broadcast_to(
                fade, (DECAY_ROWS, channels)
            ).astype(BF16)

    def state_copy(target):
        way = jnp.where(target > me, 0, 1)
        return pltpu.make_async_remote_copy(
            src_ref=state_out.at[way],
            dst_ref=state_in.at[me],
            send_sem=state_send,
            recv_sem=state_recv,
            device_id={"ep": target},
            device_id_type=MESH,
        )

    each_peer(lambda peer: state_copy(peer).start())

    def pass_copy(target):
        return pltpu.make_async_remote_copy(
            src_ref=block(passed_ref, target - base),
            dst_ref=block(arrived_ref, partner),
            send_sem=pass_send,
            recv_sem=slot_recv.at[1],
            device_id={"ep": target},
            device_id_type=MESH,
        )

    @when_passing
    def _():
        rows_copy(1).wait_recv()
        rows_copy(0).wait_recv()
        chosen = selection(meta_in, base, half, False).astype(BF16)
        passed_ref[...] = jnp.dot(chosen, rows_in[...], preferred_element_type=F32).astype(BF16)
        each_near(lambda peer: pass_copy(peer).start())
        arrived_ref[pl.ds(pl.multiple_of(partner * slot_count, slot_count), slot_count)] = (
            passed_ref[pl.ds(pl.multiple_of((me - base) * slot_count, slot_count), slot_count)]
        )
        merge_blend[0], merge_blend[1] = split(selection(meta_in, base, half, True).T)

    near_rows = pl.ds(pl.multiple_of(base * slot_count, side), side)
    far_rows = pl.ds(pl.multiple_of(other * slot_count, side), side)

    def open_gate(i, at):
        gated = jnp.dot(arrived_ref[at], gates_ref[i], preferred_element_type=F32)
        gated_ref[at, i * units : (i + 1) * units] = gated / (1.0 + jnp.exp(-gated))

    def lift(i, part, at):
        rows_of = slice(part * depth_half, (part + 1) * depth_half)
        return jnp.dot(arrived_ref[at, rows_of], ups_ref[i, rows_of], preferred_element_type=F32)

    def activate(i, at, lifted):
        hidden = slice(i * units, (i + 1) * units)
        active_ref[at, hidden] = (gated_ref[at, hidden] * lifted).astype(BF16)

    def activate_whole(i, at):
        activate(i, at, jnp.dot(arrived_ref[at], ups_ref[i], preferred_element_type=F32))

    def finish_mixer():
        settle(state_in.at[: n - 1], state_recv).wait_recv()
        depth = part_ref.shape[3]
        for h in range(heads):
            for way in range(2):

                def one(hop, state, way=way, h=h):
                    source = n - 1 - hop if way else hop
                    step = state_in[source, h, depth : depth + DECAY_ROWS].astype(F32)[0:1]
                    return state * step + state_in[source, h, :depth].astype(F32)

                ahead = n - 1 - me if way else me
                state = lax.fori_loop(0, ahead, one, jnp.zeros(part_ref.shape[3:], F32))
                for c in range(chunks)[:: -1 if way else 1]:
                    local_ref[h, c] += dot_rows(reach_ref[way, h, c], state.astype(BF16))
                    state = state * fade_ref[way, h, c, 0:1] + part_ref[way, h, c]
            lanes = slice(h * channels, (h + 1) * channels)
            for c in range(chunks):
                at = slice(c * CHUNK, (c + 1) * CHUNK)
                combined = local_ref[h, c]
                mean_square = jnp.mean(combined * combined, axis=-1, keepdims=True)
                gate = og_ref[at, lanes].astype(F32)
                opened = combined * lax.rsqrt(mean_square + EPS) * scale_ref[:, lanes]
                hidden_ref[at, lanes] = (opened * (gate / (1.0 + jnp.exp(-gate)))).astype(BF16)

    every = slice(None)
    for kind in range(2):
        settle(downs_refs[kind].at[:, :units], weight_recv.at[2 + kind, 0]).wait_recv()
    weight_copy(0, 0).wait_recv()
    settle(ups_ref.at[0], weight_recv.at[1, 0]).wait_recv()
    settle(arrived_ref.at[: (half - 1) * slot_count], slot_recv.at[0]).wait_recv()
    for i in (3, 0):
        open_gate(i, near_rows)
        activate_whole(i, near_rows)
    weight_copy(0, 1).wait_recv()
    weight_copy(0, 2).start()
    open_gate(1, near_rows)
    weight_copy(0, 2).wait_recv()
    open_gate(2, near_rows)
    weight_copy(1, 1).wait_recv()
    weight_copy(1, 2).start()

    @when_end
    def _():
        settle(arrived_ref.at[: half * slot_count], slot_recv.at[1]).wait_recv()

    @when_middle
    def _():
        blocks = half - 1 if relayed else half
        settle(arrived_ref.at[: blocks * slot_count], slot_recv.at[1]).wait_recv()

    for i in (3, 0):
        open_gate(i, far_rows)
        activate_whole(i, far_rows)
    open_gate(1, far_rows)
    open_gate(2, far_rows)
    lifted_ref[0] = lift(1, 0, every)
    weight_copy(1, 2).wait_recv()
    lifted_ref[1] = lift(2, 0, every)
    weight_copy(2, 1).wait_recv()
    weight_copy(2, 2).start()
    activate(1, every, lifted_ref[0] + lift(1, 1, every))
    weight_copy(3, 1).wait_recv()
    weight_copy(3, 2).start()
    weight_copy(2, 2).wait_recv()
    activate(2, every, lifted_ref[1] + lift(2, 1, every))

    mine = pl.ds(pl.multiple_of((me - base) * slot_count, slot_count), slot_count)

    def merge_copy(c, dest):
        return pltpu.make_async_remote_copy(
            src_ref=block(piece(leaving_refs, c), dest),
            dst_ref=block(piece(merge_refs, c), me - base),
            send_sem=far_send.at[far_group(c)],
            recv_sem=merge_recv.at[c],
            device_id={"ep": lax.rem(dest + half, n)},
            device_id_type=MESH,
        )

    def ends(peer):
        return (peer // 2 == 0) | (peer // 2 == n // 2 - 1)

    def merged_copy(c):
        return pltpu.make_async_remote_copy(
            src_ref=piece(merged_refs, c),
            dst_ref=piece(merged_in_refs, c),
            send_sem=merged_send.at[int(is_narrow(c))],
            recv_sem=merged_recv.at[c],
            device_id={"ep": partner},
            device_id_type=MESH,
        )

    def blended(weights, values):
        total = jnp.dot(weights[0], values, preferred_element_type=F32)
        return total + jnp.dot(weights[1], values, preferred_element_type=F32)

    def merge(c):
        @when_passing
        def _():
            ready = piece(merge_refs, c).at[: (half - 1) * slot_count]
            settle(ready, merge_recv.at[c]).wait_recv()
            piece(merged_refs, c)[...] = blended(merge_blend, piece(merge_refs, c)[...]).astype(BF16)
            merged_copy(c).start()

    def results(c):
        if c > 0:
            weight_copy(3 + c, 1).wait_recv()
            weight_copy(3 + c, 2).start()
        weight_copy(3 + c, 2).wait_recv()
        leaving = piece(leaving_refs, c)
        leaving[...] = jnp.dot(
            active_ref[...], piece(downs_refs, c)[...], preferred_element_type=F32
        ).astype(BF16)

        @when_passing
        def _():
            piece(merge_refs, c)[mine] = leaving[
                pl.ds(pl.multiple_of(partner * slot_count, slot_count), slot_count)
            ]

        if relayed:

            @each_far
            def _(peer):
                pl.when(ends(peer) & (peer != partner))(lambda: merge_copy(c, peer).start())

    def far(c):
        @each_far
        def _(peer):
            if relayed:
                pl.when(jnp.logical_not(ends(peer)))(lambda: back_copy(c, peer, 1).start())
            else:
                back_copy(c, peer, 1).start()

    def near(c):
        each_near(lambda peer: back_copy(c, peer, 0).start())
        piece(returned_refs, c)[here] = piece(leaving_refs, c)[here]

    def collect(c):
        returned = piece(returned_refs, c)
        total = total_ref.at[:, : returned.shape[1]]
        settle(returned.at[: (half - 1) * slot_count], back_recv.at[c, 0]).wait_recv()
        total[...] = blended(blend_ref.at[base // half], returned[near_rows])

        @when_middle
        def _():
            settle(returned.at[: half * slot_count], back_recv.at[c, 1]).wait_recv()
            total[...] += blended(blend_ref.at[other // half], returned[far_rows])

        @when_end
        def _():
            merged_copy(c).wait_recv()
            total[...] += piece(merged_in_refs, c)[...].astype(F32)

        routed_ref[:, columns(c)] = total[...].astype(BF16)

    diagonal = lax.rem(beside + quarters // 2, quarters)

    def piece_copy(i):
        return pltpu.make_async_remote_copy(
            src_ref=(partial_ref.at[0], partial_ref.at[1], summed_ref)[i],
            dst_ref=pieces_ref.at[i],
            send_sem=piece_send.at[i],
            recv_sem=piece_recv.at[i],
            device_id={"tp": across if i == 2 else beside},
            device_id_type=MESH,
        )

    def project():
        for i, part in enumerate((diagonal, beside, across, place)):
            at = pl.ds(pl.multiple_of(part * row_count, row_count), row_count)
            partial_ref[i] = jnp.dot(
                hidden_ref[at], proj_ref[...], preferred_element_type=F32
            ).astype(BF16)
            if i < 2:
                piece_copy(i).start()

    def cross():
        piece_copy(0).wait_recv()
        summed_ref[...] = (partial_ref[2].astype(F32) + pieces_ref[0].astype(F32)).astype(BF16)
        piece_copy(2).start()

    def gather_mixed():
        piece_copy(1).wait_recv()
        piece_copy(2).wait_recv()
        total = partial_ref[3].astype(F32) + pieces_ref[1].astype(F32)
        mixed_ref[...] = (total + pieces_ref[2].astype(F32)).astype(BF16)

    early = 4
    for c in range(pieces):
        results(c)
        if c < early or not relayed:
            far(c)
        else:
            when_end(lambda: far(c))
        if c == 0:
            near(0)
        else:
            when_middle(lambda: near(c))
        if c == 4:
            when_end(lambda: near(1))
        if c == 1:
            finish_mixer()
        if 0 < c < 3:
            merge(c - 1)
        if c > 3:
            merge(c - 2)
        if c == 2:
            project()
        if c == 4:
            cross()

    def far_sent(group, blocks):
        narrow, wide = leaving_refs
        sent = (wide.at[: pieces - 3], narrow, wide.at[:1])[group]
        settle(sent.at[:, : blocks * slot_count], far_send.at[group]).wait_send()

    @when_end
    def _():
        far_sent(2, half)
        for c in range(2, pieces):
            near(c)

    for c in range(early, pieces - 3):
        when_passing(lambda: far(c))
    merge(pieces - 2)
    when_passing(lambda: far(pieces - 3))
    merge(pieces - 1)
    for c in range(pieces - 2, pieces):
        when_passing(lambda: far(c))
    for c in range(pieces):
        if c == pieces // 2:
            gather_mixed()
        collect(c)

    @when_end
    def _():
        rows_copy(0).wait_send()
        rows_copy(1).wait_send()
        settle(slots_ref.at[: (half - 1) * slot_count], slot_send).wait_send()
        for group in range(2):
            far_sent(group, half)

    @when_middle
    def _():
        settle(slots_ref.at[: (n - 1) * slot_count], slot_send).wait_send()
        for group in range(3):
            far_sent(group, half - 1 if relayed else half)

    @when_passing
    def _():
        settle(passed_ref.at[: (half - 1) * slot_count], pass_send).wait_send()
        for kind in range(2):
            settle(merged_refs[kind], merged_send.at[1 - kind]).wait_send()

    for kind in range(2):
        sent = leaving_refs[kind].at[:, : (half - 1) * slot_count]
        settle(sent, near_send.at[1 - kind]).wait_send()
    settle(state_in.at[: n - 1], state_send).wait_send()
    for i in range(3):
        piece_copy(i).wait_send()
    for hop in range(3):
        settle(gates_ref.at[0], weight_send.at[0, hop]).wait_send()
        settle(ups_ref.at[0], weight_send.at[1, hop]).wait_send()
        for kind in range(2):
            settle(downs_refs[kind].at[:, :units], weight_send.at[2 + kind, hop]).wait_send()


def shards(
    queries,
    forget_forward_logits,
    forget_backward_logits,
    values,
    output_gate_logits,
    lower_bound_forward,
    lower_bound_backward,
    extra_log_decay,
    head_norm_scale,
    output_projection,
    second_residual,
    expert_norm_scale,
    routes,
    specialist_mixing_factor,
    expert_gate_matrix,
    expert_up_matrix,
    expert_down_matrix,
):
    group_rows, width_model = second_residual.shape
    quarters = lax.axis_size("tp")
    n = lax.axis_size("ep")
    row_count = group_rows // quarters
    slot_count = 2 * TOPK * row_count // n
    slot_total = n * slot_count
    width = queries.shape[1]
    heads = extra_log_decay.shape[1]
    channels = width // heads
    depth = values.shape[1] // heads
    chunks = group_rows // CHUNK
    units = expert_down_matrix.shape[1]
    span = width_model // SPANS
    vmem = pl.BlockSpec(memory_space=pltpu.VMEM)
    anywhere = pl.BlockSpec(memory_space=pl.ANY)
    state = (heads, depth + DECAY_ROWS, channels)
    block = (group_rows, width)
    out = jax.ShapeDtypeStruct((row_count, width_model), BF16)

    def narrow_and_wide(height):
        return [
            pltpu.VMEM((2, height, span), BF16),
            pltpu.VMEM((PIECES - 2, height, 2 * span), BF16),
        ]

    dma = pltpu.SemaphoreType.DMA
    both = pl.pallas_call(
        functools.partial(fused_kernel, n, quarters),
        out_shape=jax.ShapeDtypeStruct((2, row_count, width_model), BF16),
        in_specs=[anywhere] * 17,
        out_specs=vmem,
        scratch_shapes=[
            pltpu.VMEM((1, width), F32),
            pltpu.VMEM((1, width), F32),
            pltpu.VMEM((heads, group_rows), F32),
            pltpu.VMEM((1, width), F32),
            pltpu.VMEM((1, width_model), F32),
            pltpu.VMEM((TOPK, group_rows), jnp.int32),
            pltpu.VMEM((TOPK, row_count), F32),
        ]
        + [pltpu.VMEM(block, BF16)] * 5
        + [
            pltpu.VMEM((width, width_model), BF16),
            pltpu.VMEM((row_count, width_model), BF16),
            pltpu.VMEM((2, n, row_count), F32),
            pltpu.VMEM((2, n, row_count), F32),
            pltpu.VMEM((row_count, width_model), BF16),
            pltpu.VMEM((row_count, width_model), BF16),
            pltpu.VMEM((slot_total, row_count), BF16),
            pltpu.VMEM((2, 2, row_count, slot_total // 2), BF16),
            pltpu.VMEM((2, row_count, slot_total // 2), BF16),
            pltpu.VMEM((slot_total, width_model), BF16),
            pltpu.VMEM((slot_total, width_model), BF16),
            pltpu.VMEM((slot_total // 2, width_model), BF16),
            pltpu.VMEM((quarters,) + expert_gate_matrix.shape[1:], BF16),
            pltpu.VMEM((quarters,) + expert_up_matrix.shape[1:], BF16),
            *narrow_and_wide(quarters * units),
            pltpu.VMEM((slot_total, quarters * units), F32),
            pltpu.VMEM((slot_total, quarters * units), BF16),
            pltpu.VMEM((2, slot_total, units), F32),
            *narrow_and_wide(slot_total),
            *narrow_and_wide(slot_total),
            *narrow_and_wide(slot_total // 2),
            *narrow_and_wide(row_count),
            *narrow_and_wide(row_count),
            pltpu.VMEM((row_count, 2 * span), F32),
            pltpu.VMEM((heads, chunks, CHUNK, depth), F32),
            pltpu.VMEM((2, heads, chunks, CHUNK, channels), BF16),
            pltpu.VMEM((2, heads, chunks, depth, channels), F32),
            pltpu.VMEM((2, heads, chunks, 8, channels), F32),
            pltpu.VMEM((2,) + state, BF16),
            pltpu.VMEM((n,) + state, BF16),
            pltpu.VMEM(block, BF16),
            pltpu.VMEM((4, row_count, width_model), BF16),
            pltpu.VMEM((row_count, width_model), BF16),
            pltpu.VMEM((3, row_count, width_model), BF16),
            dma((18,)),
            dma((2, 2)),
            dma(()),
            dma((PIECES,)),
            dma((2,)),
            dma((PIECES,)),
            dma(()),
            dma((2,)),
            dma(()),
            dma(()),
            dma((4, 3)),
            dma((3 + PIECES, 3)),
            dma((3,)),
            dma((2,)),
            dma((PIECES, 2)),
            dma((3,)),
            dma((3,)),
        ],
        compiler_params=pltpu.CompilerParams(
            collective_id=0, has_side_effects=True, vmem_limit_bytes=48 * 2**20
        ),
        cost_estimate=pl.CostEstimate(
            flops=4 * 10**10, bytes_accessed=30 * 2**20, transcendentals=0
        ),
        name="mix_and_route",
    )(
        *(
            pltpu.with_memory_space_constraint(operand, pltpu.HBM)
            for operand in (
                queries,
                forget_forward_logits,
                forget_backward_logits,
                values,
                output_gate_logits,
                lower_bound_forward.reshape(1, -1),
                lower_bound_backward.reshape(1, -1),
                extra_log_decay.T,
                head_norm_scale.reshape(1, -1),
                output_projection,
                second_residual,
                expert_norm_scale.reshape(1, -1),
                routes.T,
                specialist_mixing_factor.T,
                expert_gate_matrix,
                expert_up_matrix,
                expert_down_matrix,
            )
        )
    )
    return both[0], both[1]


def solution(mesh):
    in_specs = (
        P("ep", "tp"),
        P("ep", "tp"),
        P("ep", "tp"),
        P("ep", "tp"),
        P("ep", "tp"),
        P("tp"),
        P("tp"),
        P("ep", "tp"),
        P("tp"),
        P("tp", None),
        P("ep", None),
        P(),
        P("ep", None),
        P(("ep", "tp"), None),
        P("ep", None, "tp"),
        P("ep", None, "tp"),
        P("ep", "tp", None),
    )
    out_specs = (P(("ep", "tp"), None), P(("ep", "tp"), None))
    return jax.shard_map(shards, mesh=mesh, in_specs=in_specs, out_specs=out_specs, check_vma=False)
```

```python
import functools

import jax
import jax.numpy as jnp
from jax import lax
from jax.experimental import pallas as pl
from jax.experimental.pallas import tpu as pltpu
from jax.sharding import PartitionSpec as P

TOPK = 2
CHUNK = 128
LEAF = 16
DECAY_ROWS = 16
SPANS = 16
PIECES = SPANS // 2 + 1
PLANES = 4
EPS = 1e-06
MESH = pl.DeviceIdType.MESH
F32 = jnp.float32
BF16 = jnp.bfloat16


def neighbours():
    place, count = lax.axis_index("tp"), lax.axis_size("tp")
    return place + 1 - 2 * lax.rem(place, 2), lax.rem(place + count // 2, count)


def greet(axis, n):
    me = lax.axis_index(axis)
    barrier = pltpu.get_barrier_semaphore()

    def one(step, carry):
        peer = lax.rem(me + step, n)
        pl.semaphore_signal(barrier, inc=1, device_id={axis: peer}, device_id_type=MESH)
        return carry

    lax.fori_loop(1, n, one, 0)


def dot_rows(a, b):
    return lax.dot_general(a, b, (((1,), (1,)), ((), ())), preferred_element_type=F32)


def gates(logits, bound, extra):
    shrink = jnp.exp(-logits)
    opened = 1.0 / (1.0 + shrink)
    floor_part = 1.0 / (1.0 + jnp.exp(-bound))
    complement = 1.0 / (1.0 + jnp.exp(bound))
    decay = jnp.log(floor_part + complement * opened) + extra
    return complement * (shrink * opened), decay


def referenced(total, size, place):
    blocks = total.reshape(CHUNK // size, size, total.shape[-1])
    anchor = jnp.broadcast_to(blocks[:, place : place + 1, :], blocks.shape)
    return total - anchor.reshape(total.shape)


def chunk_scores(feature, key, total, backward, rows, cols):
    scores = jnp.zeros((CHUNK, CHUNK), F32)
    size = CHUNK
    while size > LEAF:
        half = size // 2
        reach = jnp.exp(-jnp.abs(referenced(total, size, half if backward else half - 1)))
        part = dot_rows((feature * reach).astype(BF16), (key * reach).astype(BF16))
        late, early = (cols, rows) if backward else (rows, cols)
        mask = (rows // size == cols // size) & (late % size >= half) & (early % size < half)
        scores = scores + jnp.where(mask, part, 0.0)
        size = half
    spread = referenced(total, LEAF, LEAF // 2 if backward else LEAF // 2 - 1)
    part = dot_rows(
        (feature * jnp.exp(spread)).astype(BF16), (key * jnp.exp(-spread)).astype(BF16)
    )
    mask = (rows // LEAF == cols // LEAF) & ((rows <= cols) if backward else (rows >= cols))
    return scores + jnp.where(mask, part, 0.0)


def fused_kernel(
    n,
    quarters,
    q_any,
    ff_any,
    fb_any,
    v_any,
    og_any,
    lbf_any,
    lbb_any,
    extra_any,
    scale_any,
    proj_any,
    resid_any,
    gain_any,
    routes_any,
    mix_any,
    gate_any,
    up_any,
    down_any,
    both_ref,
    lbf_ref,
    lbb_ref,
    extra_ref,
    scale_ref,
    gain_ref,
    routes_ref,
    mix_ref,
    q_ref,
    ff_ref,
    fb_ref,
    v_ref,
    og_ref,
    proj_ref,
    resid_ref,
    meta_ref,
    meta_in,
    rows_ref,
    rows_in,
    chooser_ref,
    blend_ref,
    merge_blend,
    slots_ref,
    arrived_ref,
    passed_ref,
    gates_ref,
    ups_ref,
    downs_ref_narrow,
    downs_ref_wide,
    gated_ref,
    active_ref,
    lifted_ref,
    leaving_ref_narrow,
    leaving_ref_wide,
    returned_ref_narrow,
    returned_ref_wide,
    merge_in_narrow,
    merge_in_wide,
    merged_ref_narrow,
    merged_ref_wide,
    merged_in_narrow,
    merged_in_wide,
    total_ref,
    local_ref,
    reach_ref,
    part_ref,
    fade_ref,
    state_out,
    state_in,
    hidden_ref,
    partial_ref,
    summed_ref,
    pieces_ref,
    load_sem,
    rows_sem,
    pass_send,
    merge_recv,
    merged_send,
    merged_recv,
    slot_send,
    slot_recv,
    state_send,
    state_recv,
    weight_send,
    weight_recv,
    far_send,
    near_send,
    back_recv,
    piece_send,
    piece_recv,
):
    mixed_ref, routed_ref = both_ref.at[0], both_ref.at[1]
    me = lax.axis_index("ep")
    place = lax.axis_index("tp")
    group_rows, width = q_ref.shape
    row_count, width_model = resid_ref.shape
    chunks = group_rows // CHUNK
    heads = extra_ref.shape[0]
    channels = width // heads
    slot_total = slots_ref.shape[0]
    slot_count = slot_total // n
    units = down_any.shape[1]
    depth_half = width_model // 2

    pieces, span = PIECES, width_model // SPANS

    def piece(refs, c):
        narrow, wide = refs
        return narrow.at[c // (pieces - 1)] if is_narrow(c) else wide.at[c - 1]

    def is_narrow(c):
        return c in (0, pieces - 1)

    def far_group(c):
        return 1 if is_narrow(c) else 2 if c == pieces - 2 else 0

    def columns(c):
        first = max(0, (2 * c - 1) * span)
        return slice(first, first + (span if is_narrow(c) else 2 * span))

    downs_refs = downs_ref_narrow, downs_ref_wide
    leaving_refs = leaving_ref_narrow, leaving_ref_wide
    returned_refs = returned_ref_narrow, returned_ref_wide
    merge_refs = merge_in_narrow, merge_in_wide
    merged_refs = merged_ref_narrow, merged_ref_wide
    merged_in_refs = merged_in_narrow, merged_in_wide
    beside, across = neighbours()

    half = n // 2
    side = half * slot_count
    relayed = half == PLANES
    base = me // half * half
    other = half - base
    partner = lax.rem(me + half, n)
    plane = me // 2
    at_end = (plane == 0) | (plane == n // 2 - 1)

    def when_end(act):
        if relayed:
            pl.when(at_end)(act)

    def when_middle(act):
        if relayed:
            pl.when(jnp.logical_not(at_end))(act)
        else:
            act()

    def when_passing(act):
        if relayed:
            pl.when(jnp.logical_not(at_end))(act)

    greet("ep", n)
    greet("tp", quarters)
    first_row = pl.multiple_of(place * row_count, row_count)
    loads = [
        pltpu.make_async_copy(source, target, load_sem.at[i])
        for i, (source, target) in enumerate(
            (
                (gate_any.at[0], gates_ref.at[3]),
                (up_any.at[0], ups_ref.at[3]),
                (resid_any.at[pl.ds(first_row, row_count)], resid_ref),
                (q_any, q_ref),
                (ff_any, ff_ref),
                (fb_any, fb_ref),
                (v_any, v_ref),
                (og_any, og_ref),
                (proj_any, proj_ref),
            )
        )
    ]
    down_loads = [
        pltpu.make_async_copy(
            down_any.at[0, :, columns(c)],
            piece(downs_refs, c).at[3 * units : 4 * units],
            load_sem.at[9 if is_narrow(c) else 10],
        )
        for c in range(pieces)
    ]
    small_loads = [
        pltpu.make_async_copy(source, target, load_sem.at[11 + i])
        for i, (source, target) in enumerate(
            (
                (routes_any, routes_ref),
                (mix_any, mix_ref),
                (gain_any, gain_ref),
                (extra_any, extra_ref),
                (lbf_any, lbf_ref),
                (lbb_any, lbb_ref),
                (scale_any, scale_ref),
            )
        )
    ]
    for load in loads[:2] + small_loads + loads[2:3] + down_loads + loads[3:]:
        load.start()

    pl.semaphore_wait(pltpu.get_barrier_semaphore(), n + quarters - 2)

    def weight_copy(i, hop):
        kind = min(i, 1)
        if i == 0:
            held = lambda slot: gates_ref.at[slot]
        elif i < 3:
            at = slice((i - 1) * depth_half, i * depth_half)
            held = lambda slot: ups_ref.at[slot, at]
        else:
            kind = 2 if is_narrow(i - 3) else 3
            held = lambda slot: piece(downs_refs, i - 3).at[slot * units : (slot + 1) * units]
        return pltpu.make_async_remote_copy(
            src_ref=held(1 if hop == 2 else 3),
            dst_ref=held(hop),
            send_sem=weight_send.at[kind, hop],
            recv_sem=weight_recv.at[kind if hop == 0 else i, hop],
            device_id={"tp": across if hop == 1 else beside},
            device_id_type=MESH,
        )

    loads[0].wait()
    weight_copy(0, 1).start()
    loads[1].wait()
    for i in (1, 2):
        weight_copy(i, 1).start()
    for kind in range(2):
        own_part = downs_refs[kind].at[:, 3 * units : 4 * units]
        pltpu.make_async_copy(own_part, own_part, load_sem.at[9 + kind]).wait()
    for c in range(pieces):
        weight_copy(3 + c, 1).start()

    for load in small_loads:
        load.wait()

    lanes = pl.ds(first_row, row_count)
    expert = lax.broadcasted_iota(jnp.int32, (n, row_count), 0)
    hits = jnp.zeros((n, row_count), F32)
    shares = jnp.zeros((n, row_count), F32)
    for k in range(TOPK):
        chosen = routes_ref[k : k + 1, lanes] == expert
        hits = jnp.where(chosen, 1.0, hits)
        shares = jnp.where(chosen, mix_ref[k : k + 1], shares)
    before = lax.broadcasted_iota(jnp.int32, (row_count, row_count), 0)
    after = lax.broadcasted_iota(jnp.int32, (row_count, row_count), 1)
    earlier = (before < after).astype(BF16)
    ranks = jnp.dot(hits.astype(BF16), earlier, preferred_element_type=F32)
    meta_ref[0] = jnp.where(hits > 0.0, ranks, -1.0)
    meta_ref[1] = shares
    slot = lax.broadcasted_iota(jnp.int32, (slot_count, row_count), 0).astype(F32)

    def selection(ref, first, count, weighted):
        parts = []
        for j in range(count):
            match = slot == ref[0, pl.ds(first + j, 1)]
            parts.append(jnp.where(match, ref[1, pl.ds(first + j, 1)] if weighted else 1.0, 0.0))
        return jnp.concatenate(parts, axis=0)

    def split(weights):
        high = weights.astype(BF16)
        return high, (weights - high.astype(F32)).astype(BF16)

    loads[2].wait()
    rows_wide = resid_ref[...].astype(F32)
    mean_square = jnp.mean(rows_wide * rows_wide, axis=-1, keepdims=True)
    rows_ref[...] = (rows_wide * lax.rsqrt(mean_square + EPS) * gain_ref[...]).astype(BF16)

    def rows_copy(i):
        return pltpu.make_async_remote_copy(
            src_ref=(rows_ref, meta_ref)[i],
            dst_ref=(rows_in, meta_in)[i],
            send_sem=rows_sem.at[0, i],
            recv_sem=rows_sem.at[1, i],
            device_id={"ep": partner},
            device_id_type=MESH,
        )

    @when_end
    def _():
        rows_copy(1).start()
        rows_copy(0).start()

    chooser_ref[...] = selection(meta_ref, 0, n, False).astype(BF16)
    for g in range(slot_total // row_count):
        at = slice(g * row_count, (g + 1) * row_count)
        slots_ref[at] = jnp.dot(
            chooser_ref[at], rows_ref[...], preferred_element_type=F32
        ).astype(BF16)

    def block(ref, index):
        return ref.at[pl.ds(pl.multiple_of(index * slot_count, slot_count), slot_count)]

    def slot_copy(target, far):
        return pltpu.make_async_remote_copy(
            src_ref=block(slots_ref, target),
            dst_ref=block(arrived_ref, me),
            send_sem=slot_send,
            recv_sem=slot_recv.at[far],
            device_id={"ep": target},
            device_id_type=MESH,
        )

    def settle(ref, semaphore):
        return pltpu.make_async_remote_copy(
            src_ref=ref,
            dst_ref=ref,
            send_sem=semaphore,
            recv_sem=semaphore,
            device_id={"ep": partner},
            device_id_type=MESH,
        )

    def back_copy(c, target, far):
        return pltpu.make_async_remote_copy(
            src_ref=block(piece(leaving_refs, c), target),
            dst_ref=block(piece(returned_refs, c), me),
            send_sem=far_send.at[far_group(c)] if far else near_send.at[int(is_narrow(c))],
            recv_sem=back_recv.at[c, far],
            device_id={"ep": target},
            device_id_type=MESH,
        )

    def each_peer(act):
        def one(step, carry):
            act(lax.rem(me + step, n))
            return carry

        lax.fori_loop(1, n, one, 0)

    def each_near(act):
        def one(step, carry):
            act(base + lax.rem(me - base + step, half))
            return carry

        lax.fori_loop(1, half, one, 0)

    def each_far(act):
        def one(step, carry):
            act(other + lax.rem(me - base + step, half))
            return carry

        lax.fori_loop(0, half, one, 0)

    when_middle(lambda: each_far(lambda peer: slot_copy(peer, 1).start()))
    each_near(lambda peer: slot_copy(peer, 0).start())
    for i in range(3 + pieces):
        weight_copy(i, 0).start()
    here = pl.ds(pl.multiple_of(me * slot_count, slot_count), slot_count)
    arrived_ref[here] = slots_ref[here]
    for h in range(2):
        blend_ref[h, 0], blend_ref[h, 1] = split(selection(meta_ref, h * half, half, True).T)

    for load in loads[3:]:
        load.wait()
    rows = lax.broadcasted_iota(jnp.int32, (CHUNK, CHUNK), 0)
    cols = lax.broadcasted_iota(jnp.int32, (CHUNK, CHUNK), 1)

    def local(c, carry):
        at = pl.ds(pl.multiple_of(c * CHUNK, CHUNK), CHUNK)
        for h in range(heads):
            lanes = slice(h * channels, (h + 1) * channels)
            queries = q_ref[at, lanes].astype(F32)
            feature = queries / (1.0 + jnp.exp(-queries))
            value_rows = v_ref[at, lanes]
            extra = jnp.broadcast_to(extra_ref[h : h + 1, at], (channels, CHUNK)).T
            scores = jnp.zeros((CHUNK, CHUNK), F32)
            for way, (logit_ref, bound_ref) in enumerate(((ff_ref, lbf_ref), (fb_ref, lbb_ref))):
                key, decay = gates(logit_ref[at, lanes].astype(F32), bound_ref[:, lanes], extra)
                order = (rows <= cols) if way else (rows >= cols)
                total = jnp.dot(
                    order.astype(F32),
                    decay,
                    preferred_element_type=F32,
                    precision=lax.Precision.HIGHEST,
                )
                edge = total[0:1] if way else total[CHUNK - 1 : CHUNK]
                scores = scores + chunk_scores(feature, key, total, way == 1, rows, cols)
                reach_ref[way, h, c] = (feature * jnp.exp(total)).astype(BF16)
                faded = (key * jnp.exp(edge - total)).astype(BF16)
                part_ref[way, h, c] = lax.dot_general(
                    value_rows, faded, (((0,), (0,)), ((), ())), preferred_element_type=F32
                )
                fade_ref[way, h, c] = jnp.broadcast_to(jnp.exp(edge), (8, channels))
            local_ref[h, c] = jnp.dot(
                scores.astype(BF16), value_rows, preferred_element_type=F32
            )
        return carry

    lax.fori_loop(0, chunks, local, 0)
    for way in range(2):
        for h in range(heads):
            state = jnp.zeros(part_ref.shape[3:], F32)
            fade = jnp.ones((1, channels), F32)
            for c in range(chunks)[:: -1 if way else 1]:
                step = fade_ref[way, h, c, 0:1]
                state = state * step + part_ref[way, h, c]
                fade = fade * step
            state_out[way, h, : state.shape[0]] = state.astype(BF16)
            state_out[way, h, state.shape[0] :] = jnp.broadcast_to(
                fade, (DECAY_ROWS, channels)
            ).astype(BF16)

    def state_copy(target):
        way = jnp.where(target > me, 0, 1)
        return pltpu.make_async_remote_copy(
            src_ref=state_out.at[way],
            dst_ref=state_in.at[me],
            send_sem=state_send,
            recv_sem=state_recv,
            device_id={"ep": target},
            device_id_type=MESH,
        )

    each_peer(lambda peer: state_copy(peer).start())

    def pass_copy(target):
        return pltpu.make_async_remote_copy(
            src_ref=block(passed_ref, target - base),
            dst_ref=block(arrived_ref, partner),
            send_sem=pass_send,
            recv_sem=slot_recv.at[1],
            device_id={"ep": target},
            device_id_type=MESH,
        )

    @when_passing
    def _():
        rows_copy(1).wait_recv()
        rows_copy(0).wait_recv()
        chosen = selection(meta_in, base, half, False).astype(BF16)
        passed_ref[...] = jnp.dot(chosen, rows_in[...], preferred_element_type=F32).astype(BF16)
        each_near(lambda peer: pass_copy(peer).start())
        arrived_ref[pl.ds(pl.multiple_of(partner * slot_count, slot_count), slot_count)] = (
            passed_ref[pl.ds(pl.multiple_of((me - base) * slot_count, slot_count), slot_count)]
        )
        merge_blend[0], merge_blend[1] = split(selection(meta_in, base, half, True).T)

    near_rows = pl.ds(pl.multiple_of(base * slot_count, side), side)
    far_rows = pl.ds(pl.multiple_of(other * slot_count, side), side)

    def open_gate(i, at):
        gated = jnp.dot(arrived_ref[at], gates_ref[i], preferred_element_type=F32)
        gated_ref[at, i * units : (i + 1) * units] = gated / (1.0 + jnp.exp(-gated))

    def lift(i, part, at):
        rows_of = slice(part * depth_half, (part + 1) * depth_half)
        return jnp.dot(arrived_ref[at, rows_of], ups_ref[i, rows_of], preferred_element_type=F32)

    def activate(i, at, lifted):
        hidden = slice(i * units, (i + 1) * units)
        active_ref[at, hidden] = (gated_ref[at, hidden] * lifted).astype(BF16)

    def activate_whole(i, at):
        activate(i, at, jnp.dot(arrived_ref[at], ups_ref[i], preferred_element_type=F32))

    def finish_mixer():
        settle(state_in.at[: n - 1], state_recv).wait_recv()
        depth = part_ref.shape[3]
        for h in range(heads):
            for way in range(2):

                def one(hop, state, way=way, h=h):
                    source = n - 1 - hop if way else hop
                    step = state_in[source, h, depth : depth + DECAY_ROWS].astype(F32)[0:1]
                    return state * step + state_in[source, h, :depth].astype(F32)

                ahead = n - 1 - me if way else me
                state = lax.fori_loop(0, ahead, one, jnp.zeros(part_ref.shape[3:], F32))
                for c in range(chunks)[:: -1 if way else 1]:
                    local_ref[h, c] += dot_rows(reach_ref[way, h, c], state.astype(BF16))
                    state = state * fade_ref[way, h, c, 0:1] + part_ref[way, h, c]
            lanes = slice(h * channels, (h + 1) * channels)
            for c in range(chunks):
                at = slice(c * CHUNK, (c + 1) * CHUNK)
                combined = local_ref[h, c]
                mean_square = jnp.mean(combined * combined, axis=-1, keepdims=True)
                gate = og_ref[at, lanes].astype(F32)
                opened = combined * lax.rsqrt(mean_square + EPS) * scale_ref[:, lanes]
                hidden_ref[at, lanes] = (opened * (gate / (1.0 + jnp.exp(-gate)))).astype(BF16)

    every = slice(None)
    for kind in range(2):
        settle(downs_refs[kind].at[:, :units], weight_recv.at[2 + kind, 0]).wait_recv()
    weight_copy(0, 0).wait_recv()
    settle(ups_ref.at[0], weight_recv.at[1, 0]).wait_recv()
    settle(arrived_ref.at[: (half - 1) * slot_count], slot_recv.at[0]).wait_recv()
    for i in (3, 0):
        open_gate(i, near_rows)
        activate_whole(i, near_rows)
    weight_copy(0, 1).wait_recv()
    weight_copy(0, 2).start()
    open_gate(1, near_rows)
    weight_copy(0, 2).wait_recv()
    open_gate(2, near_rows)
    weight_copy(1, 1).wait_recv()
    weight_copy(1, 2).start()

    @when_end
    def _():
        settle(arrived_ref.at[: half * slot_count], slot_recv.at[1]).wait_recv()

    @when_middle
    def _():
        blocks = half - 1 if relayed else half
        settle(arrived_ref.at[: blocks * slot_count], slot_recv.at[1]).wait_recv()

    for i in (3, 0):
        open_gate(i, far_rows)
        activate_whole(i, far_rows)
    open_gate(1, far_rows)
    open_gate(2, far_rows)
    lifted_ref[0] = lift(1, 0, every)
    weight_copy(1, 2).wait_recv()
    lifted_ref[1] = lift(2, 0, every)
    weight_copy(2, 1).wait_recv()
    weight_copy(2, 2).start()
    activate(1, every, lifted_ref[0] + lift(1, 1, every))
    weight_copy(3, 1).wait_recv()
    weight_copy(3, 2).start()
    weight_copy(2, 2).wait_recv()
    activate(2, every, lifted_ref[1] + lift(2, 1, every))

    mine = pl.ds(pl.multiple_of((me - base) * slot_count, slot_count), slot_count)

    def merge_copy(c, dest):
        return pltpu.make_async_remote_copy(
            src_ref=block(piece(leaving_refs, c), dest),
            dst_ref=block(piece(merge_refs, c), me - base),
            send_sem=far_send.at[far_group(c)],
            recv_sem=merge_recv.at[c],
            device_id={"ep": lax.rem(dest + half, n)},
            device_id_type=MESH,
        )

    def ends(peer):
        return (peer // 2 == 0) | (peer // 2 == n // 2 - 1)

    def merged_copy(c):
        return pltpu.make_async_remote_copy(
            src_ref=piece(merged_refs, c),
            dst_ref=piece(merged_in_refs, c),
            send_sem=merged_send.at[int(is_narrow(c))],
            recv_sem=merged_recv.at[c],
            device_id={"ep": partner},
            device_id_type=MESH,
        )

    def blended(weights, values):
        total = jnp.dot(weights[0], values, preferred_element_type=F32)
        return total + jnp.dot(weights[1], values, preferred_element_type=F32)

    def merge(c):
        @when_passing
        def _():
            ready = piece(merge_refs, c).at[: (half - 1) * slot_count]
            settle(ready, merge_recv.at[c]).wait_recv()
            piece(merged_refs, c)[...] = blended(merge_blend, piece(merge_refs, c)[...]).astype(BF16)
            merged_copy(c).start()

    def results(c):
        if c > 0:
            weight_copy(3 + c, 1).wait_recv()
            weight_copy(3 + c, 2).start()
        weight_copy(3 + c, 2).wait_recv()
        leaving = piece(leaving_refs, c)
        leaving[...] = jnp.dot(
            active_ref[...], piece(downs_refs, c)[...], preferred_element_type=F32
        ).astype(BF16)

        @when_passing
        def _():
            piece(merge_refs, c)[mine] = leaving[
                pl.ds(pl.multiple_of(partner * slot_count, slot_count), slot_count)
            ]

        if relayed:

            @each_far
            def _(peer):
                pl.when(ends(peer) & (peer != partner))(lambda: merge_copy(c, peer).start())

    def far(c):
        @each_far
        def _(peer):
            if relayed:
                pl.when(jnp.logical_not(ends(peer)))(lambda: back_copy(c, peer, 1).start())
            else:
                back_copy(c, peer, 1).start()

    def near(c):
        each_near(lambda peer: back_copy(c, peer, 0).start())
        piece(returned_refs, c)[here] = piece(leaving_refs, c)[here]

    def collect(c):
        returned = piece(returned_refs, c)
        total = total_ref.at[:, : returned.shape[1]]
        settle(returned.at[: (half - 1) * slot_count], back_recv.at[c, 0]).wait_recv()
        total[...] = blended(blend_ref.at[base // half], returned[near_rows])

        @when_middle
        def _():
            settle(returned.at[: half * slot_count], back_recv.at[c, 1]).wait_recv()
            total[...] += blended(blend_ref.at[other // half], returned[far_rows])

        @when_end
        def _():
            merged_copy(c).wait_recv()
            total[...] += piece(merged_in_refs, c)[...].astype(F32)

        routed_ref[:, columns(c)] = total[...].astype(BF16)

    diagonal = lax.rem(beside + quarters // 2, quarters)

    def piece_copy(i):
        return pltpu.make_async_remote_copy(
            src_ref=(partial_ref.at[0], partial_ref.at[1], summed_ref)[i],
            dst_ref=pieces_ref.at[i],
            send_sem=piece_send.at[i],
            recv_sem=piece_recv.at[i],
            device_id={"tp": across if i == 2 else beside},
            device_id_type=MESH,
        )

    def project():
        for i, part in enumerate((diagonal, beside, across, place)):
            at = pl.ds(pl.multiple_of(part * row_count, row_count), row_count)
            partial_ref[i] = jnp.dot(
                hidden_ref[at], proj_ref[...], preferred_element_type=F32
            ).astype(BF16)
            if i < 2:
                piece_copy(i).start()

    def cross():
        piece_copy(0).wait_recv()
        summed_ref[...] = (partial_ref[2].astype(F32) + pieces_ref[0].astype(F32)).astype(BF16)
        piece_copy(2).start()

    def gather_mixed():
        piece_copy(1).wait_recv()
        piece_copy(2).wait_recv()
        total = partial_ref[3].astype(F32) + pieces_ref[1].astype(F32)
        mixed_ref[...] = (total + pieces_ref[2].astype(F32)).astype(BF16)

    early = 4
    for c in range(pieces):
        results(c)
        if c < early or not relayed:
            far(c)
        else:
            when_end(lambda: far(c))
        if c == 0:
            near(0)
        else:
            when_middle(lambda: near(c))
        if c in (4, 7):
            when_end(lambda: near(c // 3))
        if c == 1:
            finish_mixer()
        if 0 < c < 3:
            merge(c - 1)
        if c > 3:
            merge(c - 2)
        if c == 2:
            project()
        if c == 4:
            cross()

    def far_sent(group, blocks):
        narrow, wide = leaving_refs
        sent = (wide.at[: pieces - 3], narrow, wide.at[:1])[group]
        settle(sent.at[:, : blocks * slot_count], far_send.at[group]).wait_send()

    @when_end
    def _():
        far_sent(2, half)
        for c in range(3, pieces):
            near(c)

    for c in range(early, pieces - 3):
        when_passing(lambda: far(c))
    merge(pieces - 2)
    when_passing(lambda: far(pieces - 3))
    merge(pieces - 1)
    for c in range(pieces - 2, pieces):
        when_passing(lambda: far(c))
    for c in range(pieces):
        if c == pieces // 2:
            gather_mixed()
        collect(c)

    @when_end
    def _():
        rows_copy(0).wait_send()
        rows_copy(1).wait_send()
        settle(slots_ref.at[: (half - 1) * slot_count], slot_send).wait_send()
        for group in range(2):
            far_sent(group, half)

    @when_middle
    def _():
        settle(slots_ref.at[: (n - 1) * slot_count], slot_send).wait_send()
        for group in range(3):
            far_sent(group, half - 1 if relayed else half)

    @when_passing
    def _():
        settle(passed_ref.at[: (half - 1) * slot_count], pass_send).wait_send()
        for kind in range(2):
            settle(merged_refs[kind], merged_send.at[1 - kind]).wait_send()

    for kind in range(2):
        sent = leaving_refs[kind].at[:, : (half - 1) * slot_count]
        settle(sent, near_send.at[1 - kind]).wait_send()
    settle(state_in.at[: n - 1], state_send).wait_send()
    for i in range(3):
        piece_copy(i).wait_send()
    for hop in range(3):
        settle(gates_ref.at[0], weight_send.at[0, hop]).wait_send()
        settle(ups_ref.at[0], weight_send.at[1, hop]).wait_send()
        for kind in range(2):
            settle(downs_refs[kind].at[:, :units], weight_send.at[2 + kind, hop]).wait_send()


def shards(
    queries,
    forget_forward_logits,
    forget_backward_logits,
    values,
    output_gate_logits,
    lower_bound_forward,
    lower_bound_backward,
    extra_log_decay,
    head_norm_scale,
    output_projection,
    second_residual,
    expert_norm_scale,
    routes,
    specialist_mixing_factor,
    expert_gate_matrix,
    expert_up_matrix,
    expert_down_matrix,
):
    group_rows, width_model = second_residual.shape
    quarters = lax.axis_size("tp")
    n = lax.axis_size("ep")
    row_count = group_rows // quarters
    slot_count = 2 * TOPK * row_count // n
    slot_total = n * slot_count
    width = queries.shape[1]
    heads = extra_log_decay.shape[1]
    channels = width // heads
    depth = values.shape[1] // heads
    chunks = group_rows // CHUNK
    units = expert_down_matrix.shape[1]
    span = width_model // SPANS
    vmem = pl.BlockSpec(memory_space=pltpu.VMEM)
    anywhere = pl.BlockSpec(memory_space=pl.ANY)
    state = (heads, depth + DECAY_ROWS, channels)
    block = (group_rows, width)
    out = jax.ShapeDtypeStruct((row_count, width_model), BF16)

    def narrow_and_wide(height):
        return [
            pltpu.VMEM((2, height, span), BF16),
            pltpu.VMEM((PIECES - 2, height, 2 * span), BF16),
        ]

    dma = pltpu.SemaphoreType.DMA
    both = pl.pallas_call(
        functools.partial(fused_kernel, n, quarters),
        out_shape=jax.ShapeDtypeStruct((2, row_count, width_model), BF16),
        in_specs=[anywhere] * 17,
        out_specs=vmem,
        scratch_shapes=[
            pltpu.VMEM((1, width), F32),
            pltpu.VMEM((1, width), F32),
            pltpu.VMEM((heads, group_rows), F32),
            pltpu.VMEM((1, width), F32),
            pltpu.VMEM((1, width_model), F32),
            pltpu.VMEM((TOPK, group_rows), jnp.int32),
            pltpu.VMEM((TOPK, row_count), F32),
        ]
        + [pltpu.VMEM(block, BF16)] * 5
        + [
            pltpu.VMEM((width, width_model), BF16),
            pltpu.VMEM((row_count, width_model), BF16),
            pltpu.VMEM((2, n, row_count), F32),
            pltpu.VMEM((2, n, row_count), F32),
            pltpu.VMEM((row_count, width_model), BF16),
            pltpu.VMEM((row_count, width_model), BF16),
            pltpu.VMEM((slot_total, row_count), BF16),
            pltpu.VMEM((2, 2, row_count, slot_total // 2), BF16),
            pltpu.VMEM((2, row_count, slot_total // 2), BF16),
            pltpu.VMEM((slot_total, width_model), BF16),
            pltpu.VMEM((slot_total, width_model), BF16),
            pltpu.VMEM((slot_total // 2, width_model), BF16),
            pltpu.VMEM((quarters,) + expert_gate_matrix.shape[1:], BF16),
            pltpu.VMEM((quarters,) + expert_up_matrix.shape[1:], BF16),
            *narrow_and_wide(quarters * units),
            pltpu.VMEM((slot_total, quarters * units), F32),
            pltpu.VMEM((slot_total, quarters * units), BF16),
            pltpu.VMEM((2, slot_total, units), F32),
            *narrow_and_wide(slot_total),
            *narrow_and_wide(slot_total),
            *narrow_and_wide(slot_total // 2),
            *narrow_and_wide(row_count),
            *narrow_and_wide(row_count),
            pltpu.VMEM((row_count, 2 * span), F32),
            pltpu.VMEM((heads, chunks, CHUNK, depth), F32),
            pltpu.VMEM((2, heads, chunks, CHUNK, channels), BF16),
            pltpu.VMEM((2, heads, chunks, depth, channels), F32),
            pltpu.VMEM((2, heads, chunks, 8, channels), F32),
            pltpu.VMEM((2,) + state, BF16),
            pltpu.VMEM((n,) + state, BF16),
            pltpu.VMEM(block, BF16),
            pltpu.VMEM((4, row_count, width_model), BF16),
            pltpu.VMEM((row_count, width_model), BF16),
            pltpu.VMEM((3, row_count, width_model), BF16),
            dma((18,)),
            dma((2, 2)),
            dma(()),
            dma((PIECES,)),
            dma((2,)),
            dma((PIECES,)),
            dma(()),
            dma((2,)),
            dma(()),
            dma(()),
            dma((4, 3)),
            dma((3 + PIECES, 3)),
            dma((3,)),
            dma((2,)),
            dma((PIECES, 2)),
            dma((3,)),
            dma((3,)),
        ],
        compiler_params=pltpu.CompilerParams(
            collective_id=0, has_side_effects=True, vmem_limit_bytes=48 * 2**20
        ),
        cost_estimate=pl.CostEstimate(
            flops=4 * 10**10, bytes_accessed=30 * 2**20, transcendentals=0
        ),
        name="mix_and_route",
    )(
        *(
            pltpu.with_memory_space_constraint(operand, pltpu.HBM)
            for operand in (
                queries,
                forget_forward_logits,
                forget_backward_logits,
                values,
                output_gate_logits,
                lower_bound_forward.reshape(1, -1),
                lower_bound_backward.reshape(1, -1),
                extra_log_decay.T,
                head_norm_scale.reshape(1, -1),
                output_projection,
                second_residual,
                expert_norm_scale.reshape(1, -1),
                routes.T,
                specialist_mixing_factor.T,
                expert_gate_matrix,
                expert_up_matrix,
                expert_down_matrix,
            )
        )
    )
    return both[0], both[1]


def solution(mesh):
    in_specs = (
        P("ep", "tp"),
        P("ep", "tp"),
        P("ep", "tp"),
        P("ep", "tp"),
        P("ep", "tp"),
        P("tp"),
        P("tp"),
        P("ep", "tp"),
        P("tp"),
        P("tp", None),
        P("ep", None),
        P(),
        P("ep", None),
        P(("ep", "tp"), None),
        P("ep", None, "tp"),
        P("ep", None, "tp"),
        P("ep", "tp", None),
    )
    out_specs = (P(("ep", "tp"), None), P(("ep", "tp"), None))
    return jax.shard_map(shards, mesh=mesh, in_specs=in_specs, out_specs=out_specs, check_vma=False)
```
